32 devices in a mesh: sp: 4 (over z), fs: 4 (over y, x), tp: 2 (over core).
Axes of the slice: x: 2, y: 2, z: 4, core: 2. Of those that a mesh axis runs over, the one named last changes fastest.
Arguments:
- activations: bfloat16 [2048, 4096], P(('fs', 'sp'), 'tp'), parts along dimension 0, may hold values from -6 to 6
- input_norm_gain: float32 [4096], replicated, may hold values from 0.1 to 1.9
- window_query_weight: bfloat16 [4096, 2048], P('sp', 'tp'), may hold values from -0.09375 to 0.09375
- window_key_weight: bfloat16 [4096, 512], P('sp', 'tp'), may hold values from -0.09375 to 0.09375
- window_value_weight: bfloat16 [4096, 512], P('sp', 'tp'), may hold values from -0.09375 to 0.09375
- linear_query_weight: bfloat16 [4096, 1024], P('sp', 'tp'), may hold values from -0.09375 to 0.09375
- linear_key_weight: bfloat16 [4096, 1024], P('sp', 'tp'), may hold values from -0.09375 to 0.09375
- linear_value_weight: bfloat16 [4096, 2048], P('sp', 'tp'), may hold values from -0.09375 to 0.09375
- decay_down_factor: bfloat16 [4096, 16], replicated, may hold values from -0.09375 to 0.09375
- decay_up_factor: bfloat16 [16, 1024], P(None, 'tp'), may hold values from -1.5 to 1.5
- decay_offset_bias: float32 [1024], P('tp'), may hold values from -0.5 to 9
- extra_fading_exponent: float32 [2048, 8], P(('fs', 'sp'), 'tp'), parts along dimension 0, may hold values from -1.5 to 0
- starting_state: float32 [8, 128, 256], P('tp'), may hold values from -12 to 12
- head_sink_logit: float32 [32], P('tp'), may hold values from 1 to 5
- linear_head_gain: float32 [256], replicated, may hold values from 0.1 to 1.9
- window_output_weight: bfloat16 [2048, 4096], P('tp', 'sp'), may hold values from -0.09375 to 0.09375
- linear_output_weight: bfloat16 [2048, 4096], P('tp', 'sp'), may hold values from -0.09375 to 0.09375
Outputs:
- mixer_output: bfloat16 [2048, 4096], P(('fs', 'sp', 'tp')), parts along dimension 0
The draws below stay inside these ranges and needn't reach their ends.
There are 4 independent parts, one for each index of `fs`. The reference program is written for one: setup_inputs(seed, part) draws one part's arguments, and reference() takes and returns one part's arrays. A program takes and returns all parts, laid end to end along the dimension named above; an argument that names none is the same for every part. Nothing has to cross between parts.
All inputs are finite; a program needn't handle non-finite values.
Results may differ from the reference program's by a relative error of at most 0.019.
Values may be sent and summed in bfloat16 or wider, within the bound.
A program may use at most 128 MiB of HBM per device.

```python
import jax
import jax.numpy as jnp
from jax import lax

D = 4096
QH = 32
KVH = 8
HD = 64
WINDOW = 128
GATED_MIXERS = 8
LOOKUP_FEATURES = 128
DV = 256
RANK = 16
SPAN = 64
T_DEV = 128
TOKENS = 512
N_TP = 2


def draw_decay_offset_bias(key, part):
    key_flags, key_slow, key_quick = jax.random.split(key, 3)
    fast_share = 0.5
    is_quick = jax.random.uniform(key_flags, (GATED_MIXERS, 1)) < fast_share
    slow_values = jax.random.uniform(key_slow, (GATED_MIXERS, LOOKUP_FEATURES), minval=6.0, maxval=9.0)
    quick_values = jax.random.uniform(key_quick, (GATED_MIXERS, LOOKUP_FEATURES), minval=-0.5, maxval=1.0)
    return jnp.where(is_quick, quick_values, slow_values).reshape(GATED_MIXERS * LOOKUP_FEATURES).astype(jnp.float32)


def draw_extra_fading_exponent(key, part):
    key_rate, key_place, key_depth = jax.random.split(key, 3)
    block_count = TOKENS // T_DEV
    low_end = 0.25
    rates = jnp.exp(jax.random.uniform(key_rate, (block_count, GATED_MIXERS), minval=jnp.log(low_end), maxval=0.0))
    equilibrium_memory = jnp.repeat(-0.8 * rates / TOKENS, T_DEV, axis=0)
    element_indices = jax.random.randint(key_place, (2, GATED_MIXERS), 0, TOKENS)
    accrued_fading_totals = jnp.log(jax.random.uniform(key_depth, (2, GATED_MIXERS), minval=0.5, maxval=0.8))
    element_ordinals = jnp.arange(TOKENS, dtype=jnp.int32)[:, None, None]
    spike_contributions = jnp.sum(jnp.where(element_ordinals == element_indices[None], accrued_fading_totals[None], 0.0), axis=1)
    return (equilibrium_memory + spike_contributions).astype(jnp.float32)


def levels(rng, shape, shards, low, top_value):
    def one(axis_at, blocks):
        heights = jax.random.uniform(jax.random.fold_in(jax.random.fold_in(rng, 6), axis_at), (blocks,), jnp.float32, low / len(shards), top_value / len(shards))
        return jnp.repeat(jnp.exp(heights), shape[axis_at] // blocks).reshape((-1,) + (1,) * (len(shape) - axis_at - 1))

    factor_of = one(*shards[0])
    for cut in shards[1:]:
        factor_of = factor_of * one(*cut)
    return factor_of


def scatter_about(stream_key, dims, spread, bound, shards=(), kind=jnp.bfloat16):
    level = levels(stream_key, dims, shards, -0.22, 0.18) if shards else 1.0
    values = jax.random.normal(stream_key, dims, jnp.float32) * spread * level
    return jnp.minimum(jnp.maximum(values, -bound), bound).astype(kind)


def setup_inputs(seed: int = 0, part: int = 0) -> dict:
    seeds = jax.random.split(jax.random.key(seed), 18)
    part_splits = jax.random.split(jax.random.fold_in(seeds[17], part), 18)
    activations = scatter_about(part_splits[0], (TOKENS, D), 1.0, 6.0, ((0, 4), (1, 2)))
    input_norm_gain = jnp.clip(1.0 + 0.18 * jax.random.normal(seeds[1], (D,), jnp.float32), 0.1, 1.9)
    window_query_weight = scatter_about(seeds[2], (D, QH * HD), D ** -0.5, 0.09375, ((0, 4), (1, 2)))
    window_key_weight = scatter_about(seeds[3], (D, KVH * HD), D ** -0.5, 0.09375, ((0, 4), (1, 2)))
    window_value_weight = scatter_about(seeds[4], (D, KVH * HD), D ** -0.5, 0.09375, ((0, 4), (1, 2)))
    linear_query_weight = scatter_about(seeds[5], (D, GATED_MIXERS * LOOKUP_FEATURES), D ** -0.5, 0.09375, ((0, 4), (1, 2)))
    linear_key_weight = scatter_about(seeds[6], (D, GATED_MIXERS * LOOKUP_FEATURES), D ** -0.5, 0.09375, ((0, 4), (1, 2)))
    linear_value_weight = scatter_about(seeds[7], (D, GATED_MIXERS * DV), D ** -0.5, 0.09375, ((0, 4), (1, 2)))
    decay_down_factor = scatter_about(seeds[8], (D, RANK), D ** -0.5, 0.09375)
    decay_up_factor = scatter_about(seeds[9], (RANK, GATED_MIXERS * LOOKUP_FEATURES), RANK ** -0.5, 1.5, ((1, 2),))
    decay_offset_bias = draw_decay_offset_bias(jax.random.fold_in(seeds[17], 71), part)
    extra_fading_exponent = draw_extra_fading_exponent(jax.random.fold_in(jax.random.fold_in(seeds[17], part), 71), part)
    starting_state = scatter_about(seeds[12], (GATED_MIXERS, LOOKUP_FEATURES, DV), 2.0, 12.0, ((0, 2),), jnp.float32)
    head_sink_logit = jnp.clip(1.0 + 4.0 * jax.random.uniform(seeds[13], (QH,), jnp.float32) ** levels(seeds[13], (QH,), ((0, 2),), -0.2, 0.2), 1.0, 5.0)
    linear_head_gain = jnp.clip(1.0 + 0.18 * jax.random.normal(seeds[14], (DV,), jnp.float32), 0.1, 1.9)
    window_output_weight = scatter_about(seeds[15], (QH * HD, D), (QH * HD + GATED_MIXERS * DV) ** -0.5, 0.09375, ((0, 2), (1, 4)))
    linear_output_weight = scatter_about(seeds[16], (GATED_MIXERS * DV, D), (QH * HD + GATED_MIXERS * DV) ** -0.5, 0.09375, ((0, 2), (1, 4)))
    return {"activations": activations, "input_norm_gain": input_norm_gain, "window_query_weight": window_query_weight, "window_key_weight": window_key_weight, "window_value_weight": window_value_weight, "linear_query_weight": linear_query_weight, "linear_key_weight": linear_key_weight, "linear_value_weight": linear_value_weight, "decay_down_factor": decay_down_factor, "decay_up_factor": decay_up_factor, "decay_offset_bias": decay_offset_bias, "extra_fading_exponent": extra_fading_exponent, "starting_state": starting_state, "head_sink_logit": head_sink_logit, "linear_head_gain": linear_head_gain, "window_output_weight": window_output_weight, "linear_output_weight": linear_output_weight}


EPS = 1e-05
FADING_SOFTNESS = 16.0
HIGH_PRECISION = lax.Precision.HIGHEST

def window_reference(near_query, near_keys, near_values, head_sink_logit):
    stream_extent = near_query.shape[0]
    blocks = stream_extent // WINDOW
    groups = QH // KVH
    zeros_front = jnp.zeros((WINDOW, KVH * HD), jnp.float32)

    def banded(current):
        extended = jnp.concatenate([zeros_front, current.astype(jnp.float32)], axis=0)
        earlier = extended[:stream_extent].reshape(blocks, WINDOW, KVH, HD)
        present = extended[WINDOW:].reshape(blocks, WINDOW, KVH, HD)
        return jnp.concatenate([earlier, present], axis=1)
    key_band = banded(near_keys)
    value_band = banded(near_values)
    queries = near_query.astype(jnp.float32).reshape(blocks, WINDOW, KVH, groups, HD)
    scores = jnp.einsum('nqhgd,nkhd->hgnqk', queries, key_band, precision=HIGH_PRECISION) * HD ** (-0.5)
    head_ids = jnp.arange(QH, dtype=jnp.int32)
    slopes = jnp.exp2(-8.0 * (head_ids + 1).astype(jnp.float32) / QH).reshape(KVH, groups)
    query_pos = jnp.arange(WINDOW, dtype=jnp.int32)
    key_pos = jnp.arange(2 * WINDOW, dtype=jnp.int32)
    distance = query_pos[:, None] - key_pos[None, :] + WINDOW
    start_pos = (jnp.arange(blocks, dtype=jnp.int32) - 1) * WINDOW
    absolute = start_pos[:, None] + key_pos[None, :]
    allowed = ((distance >= 0) & (distance < WINDOW))[None] & (absolute >= 0)[:, None, :]
    biased = scores - slopes[:, :, None, None, None] * distance.astype(jnp.float32)
    weights = jnp.where(allowed, jnp.exp(biased), 0.0)
    denominator = lax.optimization_barrier(jnp.sum(weights, axis=-1, keepdims=True)) + jnp.exp(head_sink_logit.reshape(KVH, groups))[:, :, None, None, None]
    attention = (weights / denominator).astype(jnp.bfloat16)
    attended = jnp.einsum('hgnqk,nkhd->nqhgd', attention.astype(jnp.float32), value_band, precision=HIGH_PRECISION)
    return attended.reshape(stream_extent, QH * HD).astype(jnp.bfloat16)

def linear_reference(gated_query, gated_keys, gated_values, fading_exponent, linear_head_gain, starting_state):
    stream_extent = gated_query.shape[0]
    span_count = stream_extent // SPAN
    scaled_query = gated_query.astype(jnp.float32).reshape(span_count, SPAN, GATED_MIXERS, LOOKUP_FEATURES) * LOOKUP_FEATURES ** (-0.5)
    keys_wide = gated_keys.astype(jnp.float32).reshape(span_count, SPAN, GATED_MIXERS, LOOKUP_FEATURES)
    values_wide = gated_values.astype(jnp.float32).reshape(span_count, SPAN, GATED_MIXERS, DV)
    running = jnp.cumsum(fading_exponent.reshape(span_count, SPAN, GATED_MIXERS, LOOKUP_FEATURES), axis=1)
    span_end = running[:, -1]
    query_with_decay = scaled_query * jnp.exp(running)
    inverse_keys = keys_wide * jnp.exp(-running)
    ending_keys = keys_wide * jnp.exp(span_end[:, None] - running)
    inner = jnp.einsum('nchk,nshk->nhcs', query_with_decay, inverse_keys, precision=HIGH_PRECISION)
    lower = jnp.tril(jnp.ones((SPAN, SPAN), dtype=bool))
    inner = jnp.where(lower, inner, 0.0)
    within = jnp.einsum('nhcs,nshv->nchv', inner, values_wide, precision=HIGH_PRECISION)

    def advance(running_state, inputs):
        query_portion, key_portion, value_portion, scale_factor = inputs
        layer_output = jnp.einsum('fmy,mys->fms', query_portion, running_state, precision=HIGH_PRECISION)
        running_state = running_state * scale_factor[..., None] + jnp.einsum('gxp,gxz->xpz', key_portion, value_portion, precision=HIGH_PRECISION)
        return (running_state, layer_output)
    start_state = starting_state.astype(jnp.float32)
    final_state, carried = lax.scan(advance, start_state, (query_with_decay, ending_keys, values_wide, jnp.exp(span_end)))
    flat = (within + carried).reshape(stream_extent, GATED_MIXERS, DV)
    normal = flat * lax.rsqrt(lax.optimization_barrier(jnp.mean(flat * flat, axis=-1, keepdims=True)) + EPS) * linear_head_gain
    return normal.reshape(stream_extent, GATED_MIXERS * DV).astype(jnp.bfloat16)

def reference(activations, input_norm_gain, window_query_weight, window_key_weight, window_value_weight, linear_query_weight, linear_key_weight, linear_value_weight, decay_down_factor, decay_up_factor, decay_offset_bias, extra_fading_exponent, starting_state, head_sink_logit, linear_head_gain, window_output_weight, linear_output_weight):
    widened = activations.astype(jnp.float32)
    normed = (widened * lax.rsqrt(lax.optimization_barrier(jnp.mean(widened * widened, axis=1, keepdims=True)) + EPS) * input_norm_gain).astype(jnp.bfloat16)

    def project(matrix):
        return jnp.dot(normed, matrix, preferred_element_type=jnp.float32).astype(jnp.bfloat16)
    near_query = project(window_query_weight)
    near_keys = project(window_key_weight)
    near_values = project(window_value_weight)
    gated_query = project(linear_query_weight)
    gated_keys = project(linear_key_weight)
    gated_values = project(linear_value_weight)
    low_rank = project(decay_down_factor)
    attention_energies = jnp.dot(low_rank, decay_up_factor, preferred_element_type=jnp.float32) + decay_offset_bias
    stream_extent = normed.shape[0]
    fading_exponent = (jax.nn.log_sigmoid(attention_energies) / FADING_SOFTNESS).reshape(stream_extent, GATED_MIXERS, LOOKUP_FEATURES) + extra_fading_exponent[:, :, None]
    near_out = window_reference(near_query, near_keys, near_values, head_sink_logit)
    gated_out = linear_reference(gated_query, gated_keys, gated_values, fading_exponent, linear_head_gain, starting_state)
    window_cols = QH * HD // N_TP
    linear_cols = GATED_MIXERS * DV // N_TP
    accumulated = jnp.zeros((stream_extent, D), jnp.float32)
    for member in range(N_TP):
        first_w = member * window_cols
        first_l = member * linear_cols
        partial_value = jnp.dot(near_out[:, first_w:first_w + window_cols], window_output_weight[first_w:first_w + window_cols], preferred_element_type=jnp.float32)
        partial_value = partial_value + jnp.dot(gated_out[:, first_l:first_l + linear_cols], linear_output_weight[first_l:first_l + linear_cols], preferred_element_type=jnp.float32)
        rounded = lax.optimization_barrier(partial_value.astype(jnp.bfloat16))
        accumulated = accumulated + rounded.astype(jnp.float32)
    return accumulated.astype(jnp.bfloat16)
```

```python
import functools

import jax
import jax.numpy as jnp
from jax import lax
from jax.experimental import pallas as pl
from jax.experimental.pallas import tpu as pltpu
from jax.sharding import PartitionSpec as P

QH = 32
HD = 64
WINDOW = 128
LOOKUP_FEATURES = 128
DV = 256
SPAN = 64
KVH = 8
GATED_MIXERS = 8


EPS = 1e-05
FADING_SOFTNESS = 16.0
HIGH_PRECISION = lax.Precision.HIGHEST


def passed_along(value, axis, steps):
    count = lax.axis_size(axis)
    leading, last = (max(0, -steps), min(count, count - steps))
    return lax.ppermute(value, axis, [(source, source + steps) for source in range(leading, last)])


def prefix(x, axis, combine, identity):
    peers, place = (lax.axis_size(axis), lax.axis_index(axis))
    everything = jax.tree.map(
        lambda part, kind: lax.all_gather(part.astype(kind), axis), x, (jnp.bfloat16, jnp.bfloat16)
    )
    start = jax.tree.map(
        lambda part, zero: jnp.broadcast_to(jnp.asarray(zero, part.dtype), part.shape), x, identity
    )

    def hop(k, before):
        reached = k < place
        new = combine(
            before, jax.tree.map(lambda part, own: part[k].astype(own.dtype), everything, x)
        )
        return jax.tree.map(lambda a, b: jnp.where(reached, a, b), new, before)

    return lax.fori_loop(0, peers, hop, start)


def window_attention(near_query, near_keys, near_values, head_sink_logit):
    stream_extent = near_query.shape[0]
    key_heads = near_keys.shape[1] // HD
    heads_here = near_query.shape[1] // HD
    groups = heads_here // key_heads
    blocks = stream_extent // WINDOW
    tail_rows = jnp.stack([near_keys, near_values])
    before = passed_along(tail_rows, "sp", 1)

    def banded(previous, current):
        extended = jnp.concatenate([previous, current], axis=0)
        earlier = extended[:stream_extent].reshape(blocks, WINDOW, key_heads, HD)
        present = extended[WINDOW:].reshape(blocks, WINDOW, key_heads, HD)
        return jnp.concatenate([earlier, present], axis=1)

    key_band = banded(before[0], near_keys)
    value_band = banded(before[1], near_values)
    queries = near_query.reshape(blocks, WINDOW, key_heads, groups, HD)
    scores = jnp.einsum(
        "nqhgd,nkhd->hgnqk", queries, key_band, preferred_element_type=jnp.float32
    ) * HD ** (-0.5)
    head_ids = lax.axis_index("tp") * heads_here + jnp.arange(heads_here, dtype=jnp.int32)
    slopes = jnp.exp2(-8.0 * (head_ids + 1).astype(jnp.float32) / QH).reshape(key_heads, groups)
    query_pos = jnp.arange(WINDOW, dtype=jnp.int32)
    key_pos = jnp.arange(2 * WINDOW, dtype=jnp.int32)
    distance = query_pos[:, None] - key_pos[None, :] + WINDOW
    start_pos = (
        lax.axis_index("sp") * stream_extent + (jnp.arange(blocks, dtype=jnp.int32) - 1) * WINDOW
    )
    absolute = start_pos[:, None] + key_pos[None, :]
    allowed = ((distance >= 0) & (distance < WINDOW))[None] & (absolute >= 0)[:, None, :]
    biased = scores - slopes[:, :, None, None, None] * distance.astype(jnp.float32)
    weights = jnp.where(allowed, jnp.exp(biased), 0.0)
    denominator = (
        jnp.sum(weights, axis=-1, keepdims=True)
        + jnp.exp(head_sink_logit.reshape(key_heads, groups))[:, :, None, None, None]
    )
    attention = (weights / denominator).astype(jnp.bfloat16)
    attended = jnp.einsum(
        "hgnqk,nkhd->nqhgd", attention, value_band, preferred_element_type=jnp.float32
    )
    return attended.reshape(stream_extent, heads_here * HD).astype(jnp.bfloat16)


def linear_attention(
    gated_query, gated_keys, gated_values, fading_exponent, linear_head_gain, starting_state
):
    stream_extent = gated_query.shape[0]
    head_total = gated_query.shape[1] // LOOKUP_FEATURES
    span_count = stream_extent // SPAN
    scaled_query = gated_query.astype(jnp.float32).reshape(
        span_count, SPAN, head_total, LOOKUP_FEATURES
    ) * LOOKUP_FEATURES ** (-0.5)
    keys_wide = gated_keys.astype(jnp.float32).reshape(
        span_count, SPAN, head_total, LOOKUP_FEATURES
    )
    values_wide = gated_values.astype(jnp.float32).reshape(span_count, SPAN, head_total, DV)
    running = jnp.cumsum(
        fading_exponent.reshape(span_count, SPAN, head_total, LOOKUP_FEATURES), axis=1
    )
    span_end = running[:, -1]
    query_with_decay = scaled_query * jnp.exp(running)
    inverse_keys = keys_wide * jnp.exp(-running)
    ending_keys = keys_wide * jnp.exp(span_end[:, None] - running)
    inner = jnp.einsum("nchk,nshk->nhcs", query_with_decay, inverse_keys, precision=HIGH_PRECISION)
    lower = jnp.tril(jnp.ones((SPAN, SPAN), dtype=bool))
    inner = jnp.where(lower, inner, 0.0)
    within = jnp.einsum("nhcs,nshv->nchv", inner, values_wide, precision=HIGH_PRECISION)

    def advance(running_state, inputs):
        query_portion, key_portion, value_portion, scale_factor = inputs
        layer_output = jnp.einsum(
            "fmy,mys->fms", query_portion, running_state, precision=HIGH_PRECISION
        )
        running_state = running_state * scale_factor[..., None] + jnp.einsum(
            "gxp,gxz->xpz", key_portion, value_portion, precision=HIGH_PRECISION
        )
        return (running_state, layer_output)

    start_state = jnp.zeros((head_total, LOOKUP_FEATURES, DV), jnp.float32)
    state_end, carried = lax.scan(
        advance, start_state, (query_with_decay, ending_keys, values_wide, jnp.exp(span_end))
    )
    device_decay = jnp.exp(jnp.sum(span_end, axis=0))
    prefix_sums = jnp.cumsum(span_end, axis=0) - span_end

    def combine(earlier, later):
        return (earlier[0] * later[0], later[0][..., None] * earlier[1] + later[1])

    decay_before, state_before = prefix(
        (device_decay, state_end),
        "sp",
        combine,
        (jnp.ones_like(device_decay), jnp.zeros_like(state_end)),
    )
    incoming_rows = state_before + decay_before[..., None] * starting_state
    crossing = jnp.einsum(
        "qwso,soz->qwsz",
        query_with_decay * jnp.exp(prefix_sums)[:, None],
        incoming_rows,
        precision=HIGH_PRECISION,
    )
    flat = (within + carried + crossing).reshape(stream_extent, head_total, DV)
    normal = (
        flat * lax.rsqrt(jnp.mean(flat * flat, axis=-1, keepdims=True) + EPS) * linear_head_gain
    )
    return normal.reshape(stream_extent, head_total * DV).astype(jnp.bfloat16)


def local(
    activations,
    input_norm_gain,
    window_query_weight,
    window_key_weight,
    window_value_weight,
    linear_query_weight,
    linear_key_weight,
    linear_value_weight,
    decay_down_factor,
    decay_up_factor,
    decay_offset_bias,
    extra_fading_exponent,
    starting_state,
    head_sink_logit,
    linear_head_gain,
    window_output_weight,
    linear_output_weight,
):
    gathered = lax.all_gather(activations, "tp", axis=1, tiled=True)
    widened = gathered.astype(jnp.float32)
    normed = (
        widened
        * lax.rsqrt(jnp.mean(widened * widened, axis=1, keepdims=True) + EPS)
        * input_norm_gain
    ).astype(jnp.bfloat16)
    row_total = normed.shape[0]
    matrices = (
        window_query_weight,
        window_key_weight,
        window_value_weight,
        linear_query_weight,
        linear_key_weight,
        linear_value_weight,
    )
    segments = (
        lax.all_gather(matrices[0], "sp", axis=0, tiled=True),
        lax.all_gather(matrices[1], "sp", axis=0, tiled=True),
        lax.all_gather(matrices[2], "sp", axis=0, tiled=True),
        lax.all_gather(matrices[3], "sp", axis=0, tiled=True),
        lax.all_gather(matrices[4], "sp", axis=0, tiled=True),
        lax.all_gather(matrices[5], "sp", axis=0, tiled=True),
    )
    projected = tuple(
        (jnp.dot(normed, segment, preferred_element_type=jnp.float32) for segment in segments)
    )
    near_query, near_keys, near_values, gated_query, gated_keys, gated_values = [
        product.astype(jnp.bfloat16) for product in projected
    ]
    low_rank = jnp.dot(normed, decay_down_factor, preferred_element_type=jnp.float32).astype(
        jnp.bfloat16
    )
    attention_energies = (
        jnp.dot(low_rank, decay_up_factor, preferred_element_type=jnp.float32) + decay_offset_bias
    )
    head_total = extra_fading_exponent.shape[1]
    fading_exponent = (jax.nn.log_sigmoid(attention_energies) / FADING_SOFTNESS).reshape(
        row_total, head_total, LOOKUP_FEATURES
    ) + extra_fading_exponent[:, :, None]
    near_out = window_attention(near_query, near_keys, near_values, head_sink_logit)
    gated_out = linear_attention(
        gated_query, gated_keys, gated_values, fading_exponent, linear_head_gain, starting_state
    )
    window_full, linear_full = (
        lax.all_gather(window_output_weight, "sp", axis=1, tiled=True),
        lax.all_gather(linear_output_weight, "sp", axis=1, tiled=True),
    )
    return lax.psum_scatter(
        (
            jnp.dot(near_out, window_full, preferred_element_type=jnp.float32)
            + jnp.dot(gated_out, linear_full, preferred_element_type=jnp.float32)
        ).astype(jnp.bfloat16),
        "tp",
        scatter_dimension=0,
        tiled=True,
    )


MESH = pl.DeviceIdType.MESH
BF = jnp.bfloat16
F32 = jnp.float32


def dot(a, b):
    return jnp.dot(a, b, preferred_element_type=F32)


def remote(src, dst, send_sem, recv_sem, **where):
    return pltpu.make_async_remote_copy(
        src_ref=src,
        dst_ref=dst,
        send_sem=send_sem,
        recv_sem=recv_sem,
        device_id=where,
        device_id_type=MESH,
    )


def greet(sp, tp):
    s, t = lax.axis_index("sp"), lax.axis_index("tp")
    barrier = pltpu.get_barrier_semaphore()
    for ds in range(sp):
        for dt in range(tp):
            if ds or dt:
                where = {"sp": lax.rem(s + ds, sp), "tp": lax.rem(t + dt, tp)}
                pl.semaphore_signal(barrier, inc=1, device_id=where, device_id_type=MESH)
    pl.semaphore_wait(barrier, sp * tp - 1)


def columns_dot(a, b):
    return lax.dot_general(a, b, (((1,), (1,)), ((), ())), preferred_element_type=F32)


def mixer_kernel(sp, tp, *refs):
    x, gain, bias, sink, head_gain, up, fade = refs[:7]
    sources, state_in, down_in, out = refs[7:15], refs[15], refs[16], refs[17]
    weights, start, down = refs[18:26], refs[26], refs[27]
    squares, normed, blocks, note, term, away, landed = refs[28:35]
    lin_own, win_own, lin_in, win_in, held_g, held_n = refs[35:41]
    w_sem, sq_sem, a_send, a_recv, f_send, l_sem, n_send, n_recv = refs[41:49]
    r_send, r_recv, g_send, g_recv, t_send, t_recv, o_send, o_recv, y_sem = refs[49:58]
    s, t = lax.axis_index("sp"), lax.axis_index("tp")
    other = 1 - t
    last = sp - 1
    e = jnp.where(s >= sp // 2, 1, 0)
    at_end = jnp.logical_or(s == 0, s == last)
    inside = jnp.logical_not(at_end)
    per_half = sp // tp
    rows, half = x.shape
    width = half // per_half
    rank = down.shape[1]
    lk = LOOKUP_FEATURES
    mine = lin_own.shape[2]
    lane_of = {i: weights[i].shape[1] // 2 for i in range(6)}
    loads = [
        pltpu.make_async_copy(a, b, w_sem.at[i]) for i, (a, b) in enumerate(zip(sources, weights))
    ]
    loads.append(pltpu.make_async_copy(state_in.at[pl.ds(e * mine, mine)], start, w_sem.at[8]))
    loads.append(
        pltpu.make_async_copy(
            down_in.at[pl.ds(pl.multiple_of(t * half, half), half)], down, w_sem.at[9]
        )
    )
    for i in (9, 3, 4, 5, 0, 1, 2, 8, 6, 7):
        loads[i].start()
    wide = x[...].astype(F32)
    own = jnp.sum(wide * wide, axis=1, keepdims=True)
    squares[0] = jnp.broadcast_to(own, (rows, 128))
    greet(sp, tp)
    swap_squares = remote(squares.at[0], squares.at[1], sq_sem.at[0], sq_sem.at[1], tp=other)
    swap_squares.start()
    swap_squares.wait()
    total = own + squares[1][:, :1]
    scale = lax.rsqrt(total / (half * tp) + EPS)
    home = lax.div(s, per_half) == t

    def slice_send(i):
        j = t * per_half + i
        return remote(normed.at[i], blocks.at[s], a_send.at[i], a_recv.at[s], sp=j)

    for i in range(per_half):
        cols = slice(i * width, (i + 1) * width)
        normed[i] = (x[:, cols].astype(F32) * scale * gain[t, :, cols]).astype(BF)

        @pl.when(t * per_half + i != s)
        def _():
            slice_send(i).start()

        @pl.when(t * per_half + i == s)
        def _():
            keep = pltpu.make_async_copy(normed.at[i], blocks.at[s], l_sem)
            keep.start()
            keep.wait()

    def forward(b):
        return remote(blocks.at[b], blocks.at[b], f_send.at[b], a_recv.at[b], tp=other)

    @pl.when(home)
    def _():
        forward(s).start()

    loads[9].wait()
    low = jnp.zeros((rows, rank), F32)
    for i in range(per_half):
        low += dot(normed[i], down[i * width : (i + 1) * width])
    fades = fade.shape[1]
    noted = note.shape[2]
    wide_note = jnp.concatenate(
        [low, fade[...], jnp.zeros((rows, rows - rank - fades), F32)], axis=1
    )
    note[s, t] = wide_note.T[:noted]

    def note_send(n):
        place, core = (0 if n < tp else last), lax.rem(t + n % tp, tp)
        ref = note.at[s, t]
        return remote(ref, ref, n_send.at[n], n_recv.at[s, t], sp=place, tp=core), jnp.logical_or(
            s != place, core != t
        )

    for n in range(2 * tp):
        send, away_from_here = note_send(n)

        @pl.when(away_from_here)
        def _():
            send.start()

    def step(way, b, i):
        src = lin_own.at[b, 1 - way, i] if i < mine else win_own.at[b, 1 - way]
        dst = lin_in.at[way, b, i] if i < mine else win_in.at[way, b]
        return remote(
            src, dst, r_send.at[way, b, i], r_recv.at[way, b, i], sp=jnp.clip(s + 1 - 2 * way, 0, last)
        )

    def relay(way, b):
        for i in range(mine + 1):
            step(way, b, i).wait_recv()
            if i < mine:
                lin_own[b, 1 - way, i] = (
                    lin_own[b, 1 - way, i].astype(F32) + lin_in[way, b, i].astype(F32)
                ).astype(BF)
            else:
                win_own[b, 1 - way] = (
                    win_own[b, 1 - way].astype(F32) + win_in[way, b].astype(F32)
                ).astype(BF)
            step(way, b, i).start()

    for i in range(6):
        loads[i].wait()
    qw, kw = lane_of[0], lane_of[1]

    def project(b, carry):
        @pl.when(jnp.logical_or(jnp.logical_not(home), b != s))
        def _():
            forward(b).wait_recv()

        @pl.when(jnp.logical_and(home, b != s))
        def _():
            forward(b).start()

        block = blocks[b]

        def part(i, h):
            w = lane_of[i]
            return dot(block, weights[i][:, pl.ds(pl.multiple_of(h * w, w), w)]).astype(BF)

        for n in range(2):
            h = e if n else 1 - e
            query, key, value = part(3, h), part(4, h), part(5, h)
            for i in range(mine):
                lin_own[b, h, i, :, :lk] = query[:, i * lk : (i + 1) * lk]
                lin_own[b, h, i, :, lk : 2 * lk] = key[:, i * lk : (i + 1) * lk]
                lin_own[b, h, i, :, 2 * lk :] = value[:, i * DV : (i + 1) * DV]
            if n == 0:

                @pl.when(at_end)
                def _():
                    for i in range(mine):
                        step(e, b, i).start()

            win_own[b, h, :, :qw] = part(0, h)
            win_own[b, h, :, qw : qw + kw] = part(1, h)
            win_own[b, h, :, qw + kw :] = part(2, h)
            if n == 0:

                @pl.when(at_end)
                def _():
                    step(e, b, mine).start()

        @pl.when(jnp.logical_and(inside, b >= 1))
        def _():
            relay(0, b - 1)

        @pl.when(jnp.logical_and(inside, b >= 2))
        def _():
            relay(1, b - 2)

        return carry

    lax.fori_loop(0, sp, project, 0)

    def gather(way, b, i):
        ref = (held_g if i == 0 else held_n).at[b, way]
        return remote(
            ref, ref, g_send.at[way, b, i], g_recv.at[way, b, i], sp=jnp.clip(s + 1 - 2 * way, 0, last)
        )

    part_rows = rows // tp
    cols_g, cols_n = held_g.shape[3], held_n.shape[3]

    def swap(b):
        return remote(term.at[b, other], away.at[b], t_send.at[b], t_recv.at[b], tp=other)

    def deliver(b):
        return remote(term.at[b, t], landed.at[s], o_send.at[b], o_recv.at[s], sp=b)

    def close(b):
        swap(b).wait()
        term[b, t] = (term[b, t].astype(F32) + away[b].astype(F32)).astype(BF)

        @pl.when(s != b)
        def _():
            deliver(b).start()

        @pl.when(s == b)
        def _():
            landed[b] = term[b, t]

    def multiply(b):
        total = None
        for src in range(2):
            piece = dot(held_g[b, src], weights[7][src * cols_g : (src + 1) * cols_g]) + dot(
                held_n[b, src], weights[6][src * cols_n : (src + 1) * cols_n]
            )
            total = piece if total is None else total + piece
        for h in range(tp):
            term[b, h] = total[h * part_rows : (h + 1) * part_rows].astype(BF)
        swap(b).start()

    def pass_on(b):
        for i in range(2):
            for way in range(2):
                gather(way, b, i).wait_recv()
                gather(way, b, i).start()

    @pl.when(inside)
    def _():
        loads[8].wait()
        relay(1, sp - 2)
        pass_on(0)
        relay(0, last)
        relay(1, last)
        pass_on(1)
        loads[6].wait()
        loads[7].wait()
        for b in range(sp):
            multiply(b)
            if b + 2 < sp:
                pass_on(b + 2)
            if b:
                close(b - 1)
        close(last)

    @pl.when(at_end)
    def _():
        loads[8].wait()
        for ps in range(sp):
            for pt in range(tp):

                @pl.when(jnp.logical_or(s != ps, t != pt))
                def _():
                    ref = note.at[ps, pt]
                    remote(ref, ref, n_send.at[0], n_recv.at[ps, pt], tp=other).wait_recv()

        span = mine * lk
        lane = pl.ds(pl.multiple_of(e * span, span), span)
        up_own = jnp.concatenate([up[:, lane], jnp.zeros((rows - rank, span), BF)], axis=0)
        bias_own = bias[:, lane]
        row_at = lax.broadcasted_iota(jnp.int32, (rows, rows), 0)
        col_at = lax.broadcasted_iota(jnp.int32, (rows, rows), 1)
        span_low = jnp.logical_and(row_at >= col_at, row_at // SPAN == col_at // SPAN)
        ones_low = jnp.where(span_low, 1.0, 0.0).astype(BF)
        query_at = lax.broadcasted_iota(jnp.int32, (rows, 2 * rows), 0)
        key_at = lax.broadcasted_iota(jnp.int32, (rows, 2 * rows), 1)
        distance = query_at - key_at + rows
        near_by = jnp.logical_and(distance >= 0, distance < WINDOW)
        far = distance.astype(F32)
        heads = qw // HD // mine

        def linear(b, states):
            rank_rows = note[b, 0, :rank] + note[b, 1, :rank]
            tall = jnp.concatenate(
                [rank_rows, note[b, t, rank:], jnp.zeros((rows - noted, rows), F32)], axis=0
            ).T
            energies = dot(tall.astype(BF), up_own) + bias_own
            soft = jnp.minimum(energies, 0.0) - jnp.log1p(jnp.exp(-jnp.abs(energies)))
            soft = soft / FADING_SOFTNESS
            fading = []
            for i in range(mine):
                extra = jnp.sum(
                    jnp.where(col_at == rank + e * mine + i, tall, 0.0), axis=1, keepdims=True
                )
                fading.append(soft[:, i * lk : (i + 1) * lk] + extra)
            fading = jnp.concatenate(fading, axis=1)
            top = fading.astype(BF)
            rest = fading - top.astype(F32)
            middle = rest.astype(BF)
            bottom = (rest - middle.astype(F32)).astype(BF)
            summed = dot(ones_low, jnp.concatenate([top, middle, bottom], axis=1))
            running_all = summed[:, :span] + (summed[:, span : 2 * span] + summed[:, 2 * span :])
            new_states = []
            for i in range(mine):
                step(1 - e, b, i).wait_recv()
                here = (lin_own[b, e, i].astype(F32) + lin_in[1 - e, b, i].astype(F32)).astype(BF)
                running = running_all[:, i * lk : (i + 1) * lk]
                state = states[i]
                query = here[:, :lk].astype(F32) * lk ** (-0.5)
                key = here[:, lk : 2 * lk].astype(F32)
                value = here[:, 2 * lk :]
                decayed = (query * jnp.exp(running)).astype(BF)
                inner = columns_dot(decayed, (key * jnp.exp(-running)).astype(BF))
                inner = jnp.where(span_low, inner, 0.0).astype(BF)
                within = dot(inner, value)
                carried = []
                for j in range(rows // SPAN):
                    cut = slice(j * SPAN, (j + 1) * SPAN)
                    end = running[(j + 1) * SPAN - 1 : (j + 1) * SPAN]
                    ending = (key[cut] * jnp.exp(end - running[cut])).astype(BF)
                    carried.append(columns_dot(decayed[cut], state.astype(BF)))
                    state = state * jnp.exp(end) + lax.dot_general(
                        value[cut], ending, (((0,), (0,)), ((), ())), preferred_element_type=F32
                    )
                flat = within + jnp.concatenate(carried, axis=0)
                normal = (
                    flat
                    * lax.rsqrt(jnp.mean(flat * flat, axis=-1, keepdims=True) + EPS)
                    * head_gain[...]
                )
                held_g[b, e, :, i * DV : (i + 1) * DV] = normal.astype(BF)
                new_states.append(state)
            gather(e, b, 0).start()
            return new_states

        def window(b):
            step(1 - e, b, mine).wait_recv()
            win_own[b, e] = (win_own[b, e].astype(F32) + win_in[1 - e, b].astype(F32)).astype(BF)
            present = win_own[b, e]
            earlier = win_own[max(b - 1, 0), e]
            allowed = near_by if b else jnp.logical_and(near_by, key_at >= rows)
            for g in range(mine):
                ka, va = qw + g * HD, qw + kw + g * HD
                keys = jnp.concatenate([earlier[:, ka : ka + HD], present[:, ka : ka + HD]], axis=0)
                vals = jnp.concatenate([earlier[:, va : va + HD], present[:, va : va + HD]], axis=0)
                results = []
                for h in range(heads):
                    local = (e * mine + g) * heads + h
                    number = (t * (2 * mine * heads) + local + 1).astype(F32)
                    slope = jnp.exp2(jnp.full((rows, 1), -8.0 / QH, F32) * number)
                    at = (g * heads + h) * HD
                    score = (
                        columns_dot(present[:, at : at + HD], keys) * HD ** (-0.5) - slope * far
                    )
                    weight = jnp.where(allowed, jnp.exp(score), 0.0)
                    floor = jnp.exp(jnp.full((rows, 1), sink[local], F32))
                    probs = (weight / (jnp.sum(weight, axis=1, keepdims=True) + floor)).astype(BF)
                    results.append(dot(probs, vals))
                wide_to = heads * HD
                held_n[b, e, :, g * wide_to : (g + 1) * wide_to] = jnp.concatenate(
                    results, axis=1
                ).astype(BF)
            gather(e, b, 1).start()

        def collect(b):
            for i in range(2):
                gather(1 - e, b, i).wait_recv()

        states = [start[i].T for i in range(mine)]
        for b in range(sp):
            states = linear(b, states)
            window(b)
            if b == 1:
                loads[6].wait()
                loads[7].wait()
            if b:
                if b > 1:
                    close(b - 2)
                collect(b - 1)
                multiply(b - 1)
        close(sp - 2)
        collect(last)
        multiply(last)
        close(last)

    def drain(b, carry):
        for i in range(mine + 1):
            for way in range(2):

                @pl.when(s != last * (1 - way))
                def _():
                    step(way, b, i).wait_send()

        for i in range(2):
            for way in range(2):

                @pl.when(s != last * (1 - way))
                def _():
                    gather(way, b, i).wait_send()

        @pl.when(home)
        def _():
            forward(b).wait_send()

        return carry

    lax.fori_loop(0, sp, drain, 0)
    for i in range(per_half):

        @pl.when(t * per_half + i != s)
        def _():
            slice_send(i).wait_send()

    for n in range(2 * tp):
        send, away_from_here = note_send(n)

        @pl.when(away_from_here)
        def _():
            send.wait_send()

    columns = landed.shape[2]

    def leave(b):
        return pltpu.make_async_copy(
            landed.at[b], out.at[:, pl.ds(b * columns, columns)], y_sem.at[b]
        )

    for b in range(sp):

        @pl.when(s != b)
        def _():
            deliver(b).wait_send()
            remote(landed.at[b], landed.at[b], o_send.at[b], o_recv.at[b], tp=other).wait_recv()

        leave(b).start()
    for b in range(sp):
        leave(b).wait()


def stationary(
    activations,
    input_norm_gain,
    window_query_weight,
    window_key_weight,
    window_value_weight,
    linear_query_weight,
    linear_key_weight,
    linear_value_weight,
    decay_down_factor,
    decay_up_factor,
    decay_offset_bias,
    extra_fading_exponent,
    starting_state,
    head_sink_logit,
    linear_head_gain,
    window_output_weight,
    linear_output_weight,
):
    sp, tp = lax.axis_size("sp"), lax.axis_size("tp")
    rows, half = activations.shape
    matrices = (
        window_query_weight,
        window_key_weight,
        window_value_weight,
        linear_query_weight,
        linear_key_weight,
        linear_value_weight,
        window_output_weight,
        linear_output_weight,
    )
    rank = decay_down_factor.shape[1]
    heads_tp = extra_fading_exponent.shape[1]
    mine = heads_tp // 2
    noted = rank + heads_tp + -(rank + heads_tp) % 8
    columns = window_output_weight.shape[1]
    vmem = pl.BlockSpec(memory_space=pltpu.VMEM)
    hbm = pl.BlockSpec(memory_space=pltpu.HBM)
    dma = pltpu.SemaphoreType.DMA
    slice_width = half * tp // sp
    lin_cols = sum(m.shape[1] for m in matrices[3:6]) // heads_tp
    win_cols = sum(m.shape[1] for m in matrices[:3]) // 2
    return pl.pallas_call(
        functools.partial(mixer_kernel, sp, tp),
        out_shape=jax.ShapeDtypeStruct((rows // tp, columns * sp), BF),
        in_specs=[vmem] * 3
        + [pl.BlockSpec(memory_space=pltpu.SMEM)]
        + [vmem] * 3
        + [hbm] * 10,
        out_specs=hbm,
        scratch_shapes=[pltpu.VMEM(m.shape, BF) for m in matrices]
        + [
            pltpu.VMEM((mine,) + starting_state.shape[1:], F32),
            pltpu.VMEM((half, rank), BF),
            pltpu.VMEM((2, rows, 128), F32),
            pltpu.VMEM((sp // tp, rows, slice_width), BF),
            pltpu.VMEM((sp, rows, slice_width), BF),
            pltpu.VMEM((sp, tp, noted, rows), F32),
            pltpu.VMEM((sp, tp, rows // tp, columns), BF),
            pltpu.VMEM((sp, rows // tp, columns), BF),
            pltpu.VMEM((sp, rows // tp, columns), BF),
            pltpu.VMEM((sp, 2, mine, rows, lin_cols), BF),
            pltpu.VMEM((sp, 2, rows, win_cols), BF),
            pltpu.VMEM((2, sp, mine, rows, lin_cols), BF),
            pltpu.VMEM((2, sp, rows, win_cols), BF),
            pltpu.VMEM((sp, 2, rows, linear_output_weight.shape[0] // 2), BF),
            pltpu.VMEM((sp, 2, rows, window_output_weight.shape[0] // 2), BF),
            dma((10,)),
            dma((2,)),
            dma((sp // tp,)),
            dma((sp,)),
            dma((sp,)),
            dma,
            dma((2 * tp,)),
            dma((sp, tp)),
        ]
        + [dma((2, sp, mine + 1))] * 2
        + [dma((2, sp, 2))] * 2
        + [dma((sp,))] * 5,
        compiler_params=pltpu.CompilerParams(
            collective_id=0, has_side_effects=True, vmem_limit_bytes=56 * 2**20
        ),
    )(
        activations,
        input_norm_gain.reshape(tp, 1, half),
        decay_offset_bias.reshape(1, -1),
        head_sink_logit,
        linear_head_gain.reshape(1, -1),
        decay_up_factor,
        extra_fading_exponent,
        *matrices,
        starting_state,
        decay_down_factor,
    )


def mixer(*arrays):
    sp, tp = lax.axis_size("sp"), lax.axis_size("tp")
    rows = arrays[0].shape[0]
    one_each = KVH == GATED_MIXERS == sp * tp and QH % KVH == 0
    if tp == 2 and sp % tp == 0 and sp > 2 and one_each and rows == WINDOW and rows % SPAN == 0:
        return stationary(*arrays)
    return local(*arrays)


def solution(mesh):
    placed = (
        P(("fs", "sp"), "tp"),
        P(),
        P("sp", "tp"),
        P("sp", "tp"),
        P("sp", "tp"),
        P("sp", "tp"),
        P("sp", "tp"),
        P("sp", "tp"),
        P(),
        P(None, "tp"),
        P("tp"),
        P(("fs", "sp"), "tp"),
        P("tp", None, None),
        P("tp"),
        P(),
        P("tp", "sp"),
        P("tp", "sp"),
    )
    return jax.shard_map(
        mixer, mesh=mesh, in_specs=placed, out_specs=P(("fs", "sp", "tp"), None), check_vma=False
    )
```

```python
import functools

import jax
import jax.numpy as jnp
from jax import lax
from jax.experimental import pallas as pl
from jax.experimental.pallas import tpu as pltpu
from jax.sharding import PartitionSpec as P

QH = 32
HD = 64
WINDOW = 128
LOOKUP_FEATURES = 128
DV = 256
SPAN = 64
KVH = 8
GATED_MIXERS = 8


EPS = 1e-05
FADING_SOFTNESS = 16.0
HIGH_PRECISION = lax.Precision.HIGHEST


def passed_along(value, axis, steps):
    count = lax.axis_size(axis)
    leading, last = (max(0, -steps), min(count, count - steps))
    return lax.ppermute(value, axis, [(source, source + steps) for source in range(leading, last)])


def prefix(x, axis, combine, identity):
    peers, place = (lax.axis_size(axis), lax.axis_index(axis))
    everything = jax.tree.map(
        lambda part, kind: lax.all_gather(part.astype(kind), axis), x, (jnp.bfloat16, jnp.bfloat16)
    )
    start = jax.tree.map(
        lambda part, zero: jnp.broadcast_to(jnp.asarray(zero, part.dtype), part.shape), x, identity
    )

    def hop(k, before):
        reached = k < place
        new = combine(
            before, jax.tree.map(lambda part, own: part[k].astype(own.dtype), everything, x)
        )
        return jax.tree.map(lambda a, b: jnp.where(reached, a, b), new, before)

    return lax.fori_loop(0, peers, hop, start)


def window_attention(near_query, near_keys, near_values, head_sink_logit):
    stream_extent = near_query.shape[0]
    key_heads = near_keys.shape[1] // HD
    heads_here = near_query.shape[1] // HD
    groups = heads_here // key_heads
    blocks = stream_extent // WINDOW
    tail_rows = jnp.stack([near_keys, near_values])
    before = passed_along(tail_rows, "sp", 1)

    def banded(previous, current):
        extended = jnp.concatenate([previous, current], axis=0)
        earlier = extended[:stream_extent].reshape(blocks, WINDOW, key_heads, HD)
        present = extended[WINDOW:].reshape(blocks, WINDOW, key_heads, HD)
        return jnp.concatenate([earlier, present], axis=1)

    key_band = banded(before[0], near_keys)
    value_band = banded(before[1], near_values)
    queries = near_query.reshape(blocks, WINDOW, key_heads, groups, HD)
    scores = jnp.einsum(
        "nqhgd,nkhd->hgnqk", queries, key_band, preferred_element_type=jnp.float32
    ) * HD ** (-0.5)
    head_ids = lax.axis_index("tp") * heads_here + jnp.arange(heads_here, dtype=jnp.int32)
    slopes = jnp.exp2(-8.0 * (head_ids + 1).astype(jnp.float32) / QH).reshape(key_heads, groups)
    query_pos = jnp.arange(WINDOW, dtype=jnp.int32)
    key_pos = jnp.arange(2 * WINDOW, dtype=jnp.int32)
    distance = query_pos[:, None] - key_pos[None, :] + WINDOW
    start_pos = (
        lax.axis_index("sp") * stream_extent + (jnp.arange(blocks, dtype=jnp.int32) - 1) * WINDOW
    )
    absolute = start_pos[:, None] + key_pos[None, :]
    allowed = ((distance >= 0) & (distance < WINDOW))[None] & (absolute >= 0)[:, None, :]
    biased = scores - slopes[:, :, None, None, None] * distance.astype(jnp.float32)
    weights = jnp.where(allowed, jnp.exp(biased), 0.0)
    denominator = (
        jnp.sum(weights, axis=-1, keepdims=True)
        + jnp.exp(head_sink_logit.reshape(key_heads, groups))[:, :, None, None, None]
    )
    attention = (weights / denominator).astype(jnp.bfloat16)
    attended = jnp.einsum(
        "hgnqk,nkhd->nqhgd", attention, value_band, preferred_element_type=jnp.float32
    )
    return attended.reshape(stream_extent, heads_here * HD).astype(jnp.bfloat16)


def linear_attention(
    gated_query, gated_keys, gated_values, fading_exponent, linear_head_gain, starting_state
):
    stream_extent = gated_query.shape[0]
    head_total = gated_query.shape[1] // LOOKUP_FEATURES
    span_count = stream_extent // SPAN
    scaled_query = gated_query.astype(jnp.float32).reshape(
        span_count, SPAN, head_total, LOOKUP_FEATURES
    ) * LOOKUP_FEATURES ** (-0.5)
    keys_wide = gated_keys.astype(jnp.float32).reshape(
        span_count, SPAN, head_total, LOOKUP_FEATURES
    )
    values_wide = gated_values.astype(jnp.float32).reshape(span_count, SPAN, head_total, DV)
    running = jnp.cumsum(
        fading_exponent.reshape(span_count, SPAN, head_total, LOOKUP_FEATURES), axis=1
    )
    span_end = running[:, -1]
    query_with_decay = scaled_query * jnp.exp(running)
    inverse_keys = keys_wide * jnp.exp(-running)
    ending_keys = keys_wide * jnp.exp(span_end[:, None] - running)
    inner = jnp.einsum("nchk,nshk->nhcs", query_with_decay, inverse_keys, precision=HIGH_PRECISION)
    lower = jnp.tril(jnp.ones((SPAN, SPAN), dtype=bool))
    inner = jnp.where(lower, inner, 0.0)
    within = jnp.einsum("nhcs,nshv->nchv", inner, values_wide, precision=HIGH_PRECISION)

    def advance(running_state, inputs):
        query_portion, key_portion, value_portion, scale_factor = inputs
        layer_output = jnp.einsum(
            "fmy,mys->fms", query_portion, running_state, precision=HIGH_PRECISION
        )
        running_state = running_state * scale_factor[..., None] + jnp.einsum(
            "gxp,gxz->xpz", key_portion, value_portion, precision=HIGH_PRECISION
        )
        return (running_state, layer_output)

    start_state = jnp.zeros((head_total, LOOKUP_FEATURES, DV), jnp.float32)
    state_end, carried = lax.scan(
        advance, start_state, (query_with_decay, ending_keys, values_wide, jnp.exp(span_end))
    )
    device_decay = jnp.exp(jnp.sum(span_end, axis=0))
    prefix_sums = jnp.cumsum(span_end, axis=0) - span_end

    def combine(earlier, later):
        return (earlier[0] * later[0], later[0][..., None] * earlier[1] + later[1])

    decay_before, state_before = prefix(
        (device_decay, state_end),
        "sp",
        combine,
        (jnp.ones_like(device_decay), jnp.zeros_like(state_end)),
    )
    incoming_rows = state_before + decay_before[..., None] * starting_state
    crossing = jnp.einsum(
        "qwso,soz->qwsz",
        query_with_decay * jnp.exp(prefix_sums)[:, None],
        incoming_rows,
        precision=HIGH_PRECISION,
    )
    flat = (within + carried + crossing).reshape(stream_extent, head_total, DV)
    normal = (
        flat * lax.rsqrt(jnp.mean(flat * flat, axis=-1, keepdims=True) + EPS) * linear_head_gain
    )
    return normal.reshape(stream_extent, head_total * DV).astype(jnp.bfloat16)


def local(
    activations,
    input_norm_gain,
    window_query_weight,
    window_key_weight,
    window_value_weight,
    linear_query_weight,
    linear_key_weight,
    linear_value_weight,
    decay_down_factor,
    decay_up_factor,
    decay_offset_bias,
    extra_fading_exponent,
    starting_state,
    head_sink_logit,
    linear_head_gain,
    window_output_weight,
    linear_output_weight,
):
    gathered = lax.all_gather(activations, "tp", axis=1, tiled=True)
    widened = gathered.astype(jnp.float32)
    normed = (
        widened
        * lax.rsqrt(jnp.mean(widened * widened, axis=1, keepdims=True) + EPS)
        * input_norm_gain
    ).astype(jnp.bfloat16)
    row_total = normed.shape[0]
    matrices = (
        window_query_weight,
        window_key_weight,
        window_value_weight,
        linear_query_weight,
        linear_key_weight,
        linear_value_weight,
    )
    segments = (
        lax.all_gather(matrices[0], "sp", axis=0, tiled=True),
        lax.all_gather(matrices[1], "sp", axis=0, tiled=True),
        lax.all_gather(matrices[2], "sp", axis=0, tiled=True),
        lax.all_gather(matrices[3], "sp", axis=0, tiled=True),
        lax.all_gather(matrices[4], "sp", axis=0, tiled=True),
        lax.all_gather(matrices[5], "sp", axis=0, tiled=True),
    )
    projected = tuple(
        (jnp.dot(normed, segment, preferred_element_type=jnp.float32) for segment in segments)
    )
    near_query, near_keys, near_values, gated_query, gated_keys, gated_values = [
        product.astype(jnp.bfloat16) for product in projected
    ]
    low_rank = jnp.dot(normed, decay_down_factor, preferred_element_type=jnp.float32).astype(
        jnp.bfloat16
    )
    attention_energies = (
        jnp.dot(low_rank, decay_up_factor, preferred_element_type=jnp.float32) + decay_offset_bias
    )
    head_total = extra_fading_exponent.shape[1]
    fading_exponent = (jax.nn.log_sigmoid(attention_energies) / FADING_SOFTNESS).reshape(
        row_total, head_total, LOOKUP_FEATURES
    ) + extra_fading_exponent[:, :, None]
    near_out = window_attention(near_query, near_keys, near_values, head_sink_logit)
    gated_out = linear_attention(
        gated_query, gated_keys, gated_values, fading_exponent, linear_head_gain, starting_state
    )
    window_full, linear_full = (
        lax.all_gather(window_output_weight, "sp", axis=1, tiled=True),
        lax.all_gather(linear_output_weight, "sp", axis=1, tiled=True),
    )
    return lax.psum_scatter(
        (
            jnp.dot(near_out, window_full, preferred_element_type=jnp.float32)
            + jnp.dot(gated_out, linear_full, preferred_element_type=jnp.float32)
        ).astype(jnp.bfloat16),
        "tp",
        scatter_dimension=0,
        tiled=True,
    )


MESH = pl.DeviceIdType.MESH
BF = jnp.bfloat16
F32 = jnp.float32
LAG = 2


def dot(a, b):
    return jnp.dot(a, b, preferred_element_type=F32)


def remote(src, dst, send_sem, recv_sem, **where):
    return pltpu.make_async_remote_copy(
        src_ref=src,
        dst_ref=dst,
        send_sem=send_sem,
        recv_sem=recv_sem,
        device_id=where,
        device_id_type=MESH,
    )


def greet(sp, tp):
    s, t = lax.axis_index("sp"), lax.axis_index("tp")
    barrier = pltpu.get_barrier_semaphore()
    for ds in range(sp):
        for dt in range(tp):
            if ds or dt:
                where = {"sp": lax.rem(s + ds, sp), "tp": lax.rem(t + dt, tp)}
                pl.semaphore_signal(barrier, inc=1, device_id=where, device_id_type=MESH)


def greeted(sp, tp):
    pl.semaphore_wait(pltpu.get_barrier_semaphore(), sp * tp - 1)


def columns_dot(a, b):
    return lax.dot_general(a, b, (((1,), (1,)), ((), ())), preferred_element_type=F32)


def mixer_kernel(sp, tp, *refs):
    x, gain, bias, sink, head_gain, up, fade = refs[:7]
    sources, state_in, down_in, out = refs[7:15], refs[15], refs[16], refs[17]
    weights, start, down = refs[18:26], refs[26], refs[27]
    squares, blocks, note, term, away, landed = refs[28:34]
    lin_own, win_own, lin_in, win_in, held_g, held_n = refs[34:40]
    w_sem, sq_send, sq_recv, a_send, a_recv, f_send, l_sem, n_send, n_recv = refs[40:49]
    r_send, r_recv, g_send, g_recv, t_send, t_recv, o_send, o_recv, y_sem = refs[49:58]
    s, t = lax.axis_index("sp"), lax.axis_index("tp")
    other = 1 - t
    last = sp - 1
    e = jnp.where(s >= sp // 2, 1, 0)
    at_end = jnp.logical_or(s == 0, s == last)
    inside = jnp.logical_not(at_end)
    per_half = sp // tp
    rows, half = x.shape
    width = half // per_half
    rank = down.shape[1]
    lk = LOOKUP_FEATURES
    mine = lin_own.shape[2]
    lane_of = {i: weights[i].shape[1] // 2 for i in range(6)}
    greet(sp, tp)
    loads = [
        pltpu.make_async_copy(a, b, w_sem.at[i]) for i, (a, b) in enumerate(zip(sources, weights))
    ]
    loads.append(pltpu.make_async_copy(state_in.at[pl.ds(e * mine, mine)], start, w_sem.at[8]))
    loads.append(
        pltpu.make_async_copy(
            down_in.at[pl.ds(pl.multiple_of(t * half, half), half)], down, w_sem.at[9]
        )
    )
    for i in (9, 3, 4, 5, 0, 1, 2, 8, 6, 7):
        loads[i].start()
    wide = x[...].astype(F32)
    own = jnp.sum(wide * wide, axis=1, keepdims=True)
    squares[s, t] = jnp.broadcast_to(own, (rows, rows)).T[:8]
    home = lax.div(s, per_half) == t

    def slice_send(i):
        src = x.at[:, i * width : (i + 1) * width]
        return remote(src, blocks.at[s], a_send.at[i], a_recv.at[s], sp=t * per_half + i)

    def forward(b):
        return remote(blocks.at[b], blocks.at[b], f_send.at[b], a_recv.at[b], tp=other)

    def squares_send(n):
        where = {"sp": lax.rem(s + n // tp, sp), "tp": lax.rem(t + n % tp, tp)}
        ref = squares.at[s, t]
        return remote(ref, ref, sq_send.at[n], sq_recv.at[s, t], **where)

    def keep(i):
        return pltpu.make_async_copy(x.at[:, i * width : (i + 1) * width], blocks.at[s], l_sem)

    def share(i):
        src = x.at[:, i * width : (i + 1) * width]
        return remote(src, blocks.at[s], f_send.at[s], a_recv.at[s], tp=other)

    greeted(sp, tp)
    for n in range(1, sp * tp):
        squares_send(n).start()
    for i in range(per_half):

        @pl.when(t * per_half + i != s)
        def _():
            slice_send(i).start()

        @pl.when(t * per_half + i == s)
        def _():
            share(i).start()
            keep(i).start()

    def squares_wait(ps, pt):
        ref = squares.at[ps, pt]
        remote(ref, ref, sq_send.at[0], sq_recv.at[ps, pt], tp=other).wait_recv()

    def scale_of(b):
        total = jnp.sum(squares[b], axis=0) / (half * tp)
        tall = jnp.concatenate([lax.rsqrt(total + EPS), jnp.zeros((rows - 8, rows), F32)], axis=0)
        return tall.T[:, :1]

    squares_wait(s, other)
    scale = scale_of(s)
    loads[9].wait()
    low = jnp.zeros((rows, rank), F32)
    for i in range(per_half):
        cols = slice(i * width, (i + 1) * width)
        shaped = (x[:, cols].astype(F32) * scale * gain[t, :, cols]).astype(BF)
        low += dot(shaped, down[cols])
    fades = fade.shape[1]
    noted = note.shape[2]
    wide_note = jnp.concatenate(
        [low, fade[...], jnp.zeros((rows, rows - rank - fades), F32)], axis=1
    )
    note[s, t] = wide_note.T[:noted]

    def note_send(n):
        place, core = (0 if n < tp else last), lax.rem(t + n % tp, tp)
        ref = note.at[s, t]
        return remote(ref, ref, n_send.at[n], n_recv.at[s, t], sp=place, tp=core), jnp.logical_or(
            s != place, core != t
        )

    for n in range(2 * tp):
        send, away_from_here = note_send(n)

        @pl.when(away_from_here)
        def _():
            send.start()

    def step(way, b, i):
        src = lin_own.at[b, 1 - way, i] if i < mine else win_own.at[b, 1 - way]
        dst = lin_in.at[way, b, i] if i < mine else win_in.at[way, b]
        return remote(
            src, dst, r_send.at[way, b, i], r_recv.at[way, b, i], sp=jnp.clip(s + 1 - 2 * way, 0, last)
        )

    def relay(way, b, i):
        step(way, b, i).wait_recv()
        if i < mine:
            lin_own[b, 1 - way, i] = (
                lin_own[b, 1 - way, i].astype(F32) + lin_in[way, b, i].astype(F32)
            ).astype(BF)
        else:
            win_own[b, 1 - way] = (
                win_own[b, 1 - way].astype(F32) + win_in[way, b].astype(F32)
            ).astype(BF)
        step(way, b, i).start()

    for i in range(6):
        loads[i].wait()
    qw, kw = lane_of[0], lane_of[1]
    gain_here = gain[lax.div(s, per_half), :, pl.ds(pl.multiple_of(lax.rem(s, per_half) * width, width), width)]

    def project(b, carry):
        @pl.when(jnp.logical_or(jnp.logical_not(home), b != s))
        def _():
            forward(b).wait_recv()

        @pl.when(jnp.logical_and(home, b != s))
        def _():
            forward(b).start()

        @pl.when(jnp.logical_and(home, b == s))
        def _():
            keep(0).wait()

        @pl.when(b != s)
        def _():
            for pt in range(tp):
                squares_wait(b, pt)

        block = (blocks[b].astype(F32) * scale_of(b) * gain_here).astype(BF)

        def part(i, h):
            w = lane_of[i]
            return dot(block, weights[i][:, pl.ds(pl.multiple_of(h * w, w), w)]).astype(BF)

        for n in range(2):
            h = e if n else 1 - e
            query, key, value = part(3, h), part(4, h), part(5, h)
            for i in range(mine):
                lin_own[b, h, i, :, :lk] = query[:, i * lk : (i + 1) * lk]
                lin_own[b, h, i, :, lk : 2 * lk] = key[:, i * lk : (i + 1) * lk]
                lin_own[b, h, i, :, 2 * lk :] = value[:, i * DV : (i + 1) * DV]
            if n == 0:

                @pl.when(at_end)
                def _():
                    for i in range(mine):
                        step(e, b, i).start()

            win_own[b, h, :, :qw] = part(0, h)
            win_own[b, h, :, qw : qw + kw] = part(1, h)
            win_own[b, h, :, qw + kw :] = part(2, h)
            if n == 0:

                @pl.when(at_end)
                def _():
                    step(e, b, mine).start()

        return carry

    lax.fori_loop(0, sp, project, 0)

    def gather(way, b, i):
        ref = (held_g if i == 0 else held_n).at[b, way]
        return remote(
            ref, ref, g_send.at[way, b, i], g_recv.at[way, b, i], sp=jnp.clip(s + 1 - 2 * way, 0, last)
        )

    part_rows = rows // tp
    cols_g, cols_n = held_g.shape[3], held_n.shape[3]

    def swap(b):
        return remote(term.at[b, other], away.at[b], t_send.at[b], t_recv.at[b], tp=other)

    def deliver(b):
        return remote(term.at[b, t], landed.at[s], o_send.at[b], o_recv.at[s], sp=b)

    def close(b):
        swap(b).wait()
        term[b, t] = (term[b, t].astype(F32) + away[b].astype(F32)).astype(BF)

        @pl.when(s != b)
        def _():
            deliver(b).start()

        @pl.when(s == b)
        def _():
            landed[b] = term[b, t]

    def multiply(b):
        total = None
        for src in range(2):
            piece = dot(held_g[b, src], weights[7][src * cols_g : (src + 1) * cols_g]) + dot(
                held_n[b, src], weights[6][src * cols_n : (src + 1) * cols_n]
            )
            total = piece if total is None else total + piece
        for h in range(tp):
            term[b, h] = total[h * part_rows : (h + 1) * part_rows].astype(BF)
        swap(b).start()

    def pass_on(way, b, i):
        gather(way, b, i).wait_recv()
        gather(way, b, i).start()

    @pl.when(inside)
    def _():
        loads[8].wait()
        sums = [(b, i) for b in range(sp) for i in range(mine + 1)]
        for n in range(len(sums) + LAG):
            if n < len(sums):
                relay(e, *sums[n])
            if n >= LAG:
                relay(1 - e, *sums[n - LAG])
        loads[6].wait()
        loads[7].wait()
        outs = [(b, i) for b in range(sp) for i in range(2)]
        for n in range(len(outs) + LAG):
            if n < len(outs):
                pass_on(e, *outs[n])
            if n >= LAG:
                b, i = outs[n - LAG]
                pass_on(1 - e, b, i)
                if i == 1:
                    multiply(b)
                    if b:
                        close(b - 1)
        close(last)

    @pl.when(at_end)
    def _():
        loads[8].wait()
        for ps in range(sp):
            for pt in range(tp):

                @pl.when(jnp.logical_or(s != ps, t != pt))
                def _():
                    ref = note.at[ps, pt]
                    remote(ref, ref, n_send.at[0], n_recv.at[ps, pt], tp=other).wait_recv()

        span = mine * lk
        lane = pl.ds(pl.multiple_of(e * span, span), span)
        up_own = jnp.concatenate([up[:, lane], jnp.zeros((rows - rank, span), BF)], axis=0)
        bias_own = bias[:, lane]
        row_at = lax.broadcasted_iota(jnp.int32, (rows, rows), 0)
        col_at = lax.broadcasted_iota(jnp.int32, (rows, rows), 1)
        span_low = jnp.logical_and(row_at >= col_at, row_at // SPAN == col_at // SPAN)
        ones_low = jnp.where(span_low, 1.0, 0.0).astype(BF)
        query_at = lax.broadcasted_iota(jnp.int32, (rows, 2 * rows), 0)
        key_at = lax.broadcasted_iota(jnp.int32, (rows, 2 * rows), 1)
        distance = query_at - key_at + rows
        near_by = jnp.logical_and(distance >= 0, distance < WINDOW)
        far = distance.astype(F32)
        heads = qw // HD // mine

        def linear(b, states):
            rank_rows = note[b, 0, :rank] + note[b, 1, :rank]
            tall = jnp.concatenate(
                [rank_rows, note[b, t, rank:], jnp.zeros((rows - noted, rows), F32)], axis=0
            ).T
            energies = dot(tall.astype(BF), up_own) + bias_own
            soft = jnp.minimum(energies, 0.0) - jnp.log1p(jnp.exp(-jnp.abs(energies)))
            soft = soft / FADING_SOFTNESS
            fading = []
            for i in range(mine):
                extra = jnp.sum(
                    jnp.where(col_at == rank + e * mine + i, tall, 0.0), axis=1, keepdims=True
                )
                fading.append(soft[:, i * lk : (i + 1) * lk] + extra)
            fading = jnp.concatenate(fading, axis=1)
            top = fading.astype(BF)
            rest = fading - top.astype(F32)
            middle = rest.astype(BF)
            bottom = (rest - middle.astype(F32)).astype(BF)
            summed = dot(ones_low, jnp.concatenate([top, middle, bottom], axis=1))
            running_all = summed[:, :span] + (summed[:, span : 2 * span] + summed[:, 2 * span :])
            new_states = []
            for i in range(mine):
                step(1 - e, b, i).wait_recv()
                here = (lin_own[b, e, i].astype(F32) + lin_in[1 - e, b, i].astype(F32)).astype(BF)
                running = running_all[:, i * lk : (i + 1) * lk]
                state = states[i]
                query = here[:, :lk].astype(F32) * lk ** (-0.5)
                key = here[:, lk : 2 * lk].astype(F32)
                value = here[:, 2 * lk :]
                decayed = (query * jnp.exp(running)).astype(BF)
                inner = columns_dot(decayed, (key * jnp.exp(-running)).astype(BF))
                inner = jnp.where(span_low, inner, 0.0).astype(BF)
                within = dot(inner, value)
                carried = []
                for j in range(rows // SPAN):
                    cut = slice(j * SPAN, (j + 1) * SPAN)
                    end = running[(j + 1) * SPAN - 1 : (j + 1) * SPAN]
                    ending = (key[cut] * jnp.exp(end - running[cut])).astype(BF)
                    carried.append(columns_dot(decayed[cut], state.astype(BF)))
                    state = state * jnp.exp(end) + lax.dot_general(
                        value[cut], ending, (((0,), (0,)), ((), ())), preferred_element_type=F32
                    )
                flat = within + jnp.concatenate(carried, axis=0)
                normal = (
                    flat
                    * lax.rsqrt(jnp.mean(flat * flat, axis=-1, keepdims=True) + EPS)
                    * head_gain[...]
                )
                held_g[b, e, :, i * DV : (i + 1) * DV] = normal.astype(BF)
                new_states.append(state)
            gather(e, b, 0).start()
            return new_states

        def window(b):
            step(1 - e, b, mine).wait_recv()
            win_own[b, e] = (win_own[b, e].astype(F32) + win_in[1 - e, b].astype(F32)).astype(BF)
            present = win_own[b, e]
            earlier = win_own[max(b - 1, 0), e]
            allowed = near_by if b else jnp.logical_and(near_by, key_at >= rows)
            for g in range(mine):
                ka, va = qw + g * HD, qw + kw + g * HD
                keys = jnp.concatenate([earlier[:, ka : ka + HD], present[:, ka : ka + HD]], axis=0)
                vals = jnp.concatenate([earlier[:, va : va + HD], present[:, va : va + HD]], axis=0)
                results = []
                for h in range(heads):
                    local = (e * mine + g) * heads + h
                    number = (t * (2 * mine * heads) + local + 1).astype(F32)
                    slope = jnp.exp2(jnp.full((rows, 1), -8.0 / QH, F32) * number)
                    at = (g * heads + h) * HD
                    score = (
                        columns_dot(present[:, at : at + HD], keys) * HD ** (-0.5) - slope * far
                    )
                    weight = jnp.where(allowed, jnp.exp(score), 0.0)
                    floor = jnp.exp(jnp.full((rows, 1), sink[local], F32))
                    probs = (weight / (jnp.sum(weight, axis=1, keepdims=True) + floor)).astype(BF)
                    results.append(dot(probs, vals))
                wide_to = heads * HD
                held_n[b, e, :, g * wide_to : (g + 1) * wide_to] = jnp.concatenate(
                    results, axis=1
                ).astype(BF)
            gather(e, b, 1).start()

        def collect(b):
            for i in range(2):
                gather(1 - e, b, i).wait_recv()

        states = [start[i].T for i in range(mine)]
        for b in range(sp):
            states = linear(b, states)
            window(b)
        loads[6].wait()
        loads[7].wait()
        for b in range(sp):
            collect(b)
            multiply(b)
            if b:
                close(b - 1)
        close(last)

    def drain(b, carry):
        for i in range(mine + 1):
            for way in range(2):

                @pl.when(s != last * (1 - way))
                def _():
                    step(way, b, i).wait_send()

        for i in range(2):
            for way in range(2):

                @pl.when(s != last * (1 - way))
                def _():
                    gather(way, b, i).wait_send()

        @pl.when(home)
        def _():
            forward(b).wait_send()

        return carry

    lax.fori_loop(0, sp, drain, 0)
    for i in range(per_half):

        @pl.when(t * per_half + i != s)
        def _():
            slice_send(i).wait_send()

    for n in range(2 * tp):
        send, away_from_here = note_send(n)

        @pl.when(away_from_here)
        def _():
            send.wait_send()

    for n in range(1, sp * tp):
        squares_send(n).wait_send()

    columns = landed.shape[2]

    def leave(b):
        return pltpu.make_async_copy(
            landed.at[b], out.at[:, pl.ds(b * columns, columns)], y_sem.at[b]
        )

    for b in range(sp):

        @pl.when(s != b)
        def _():
            deliver(b).wait_send()
            remote(landed.at[b], landed.at[b], o_send.at[b], o_recv.at[b], tp=other).wait_recv()

        leave(b).start()
    for b in range(sp):
        leave(b).wait()


def stationary(
    activations,
    input_norm_gain,
    window_query_weight,
    window_key_weight,
    window_value_weight,
    linear_query_weight,
    linear_key_weight,
    linear_value_weight,
    decay_down_factor,
    decay_up_factor,
    decay_offset_bias,
    extra_fading_exponent,
    starting_state,
    head_sink_logit,
    linear_head_gain,
    window_output_weight,
    linear_output_weight,
):
    sp, tp = lax.axis_size("sp"), lax.axis_size("tp")
    rows, half = activations.shape
    matrices = (
        window_query_weight,
        window_key_weight,
        window_value_weight,
        linear_query_weight,
        linear_key_weight,
        linear_value_weight,
        window_output_weight,
        linear_output_weight,
    )
    rank = decay_down_factor.shape[1]
    heads_tp = extra_fading_exponent.shape[1]
    mine = heads_tp // 2
    noted = rank + heads_tp + -(rank + heads_tp) % 8
    columns = window_output_weight.shape[1]
    vmem = pl.BlockSpec(memory_space=pltpu.VMEM)
    hbm = pl.BlockSpec(memory_space=pltpu.HBM)
    dma = pltpu.SemaphoreType.DMA
    slice_width = half * tp // sp
    lin_cols = sum(m.shape[1] for m in matrices[3:6]) // heads_tp
    win_cols = sum(m.shape[1] for m in matrices[:3]) // 2
    return pl.pallas_call(
        functools.partial(mixer_kernel, sp, tp),
        out_shape=jax.ShapeDtypeStruct((rows // tp, columns * sp), BF),
        in_specs=[vmem] * 3
        + [pl.BlockSpec(memory_space=pltpu.SMEM)]
        + [vmem] * 3
        + [hbm] * 10,
        out_specs=hbm,
        scratch_shapes=[pltpu.VMEM(m.shape, BF) for m in matrices]
        + [
            pltpu.VMEM((mine,) + starting_state.shape[1:], F32),
            pltpu.VMEM((half, rank), BF),
            pltpu.VMEM((sp, tp, 8, rows), F32),
            pltpu.VMEM((sp, rows, slice_width), BF),
            pltpu.VMEM((sp, tp, noted, rows), F32),
            pltpu.VMEM((sp, tp, rows // tp, columns), BF),
            pltpu.VMEM((sp, rows // tp, columns), BF),
            pltpu.VMEM((sp, rows // tp, columns), BF),
            pltpu.VMEM((sp, 2, mine, rows, lin_cols), BF),
            pltpu.VMEM((sp, 2, rows, win_cols), BF),
            pltpu.VMEM((2, sp, mine, rows, lin_cols), BF),
            pltpu.VMEM((2, sp, rows, win_cols), BF),
            pltpu.VMEM((sp, 2, rows, linear_output_weight.shape[0] // 2), BF),
            pltpu.VMEM((sp, 2, rows, window_output_weight.shape[0] // 2), BF),
            dma((10,)),
            dma((sp * tp,)),
            dma((sp, tp)),
            dma((sp // tp,)),
            dma((sp,)),
            dma((sp,)),
            dma,
            dma((2 * tp,)),
            dma((sp, tp)),
        ]
        + [dma((2, sp, mine + 1))] * 2
        + [dma((2, sp, 2))] * 2
        + [dma((sp,))] * 5,
        compiler_params=pltpu.CompilerParams(
            collective_id=0, has_side_effects=True, vmem_limit_bytes=56 * 2**20
        ),
    )(
        activations,
        input_norm_gain.reshape(tp, 1, half),
        decay_offset_bias.reshape(1, -1),
        head_sink_logit,
        linear_head_gain.reshape(1, -1),
        decay_up_factor,
        extra_fading_exponent,
        *matrices,
        starting_state,
        decay_down_factor,
    )


def mixer(*arrays):
    sp, tp = lax.axis_size("sp"), lax.axis_size("tp")
    rows = arrays[0].shape[0]
    one_each = KVH == GATED_MIXERS == sp * tp and QH % KVH == 0
    if tp == 2 and sp % tp == 0 and sp > 2 and one_each and rows == WINDOW and rows % SPAN == 0:
        return stationary(*arrays)
    return local(*arrays)


def solution(mesh):
    placed = (
        P(("fs", "sp"), "tp"),
        P(),
        P("sp", "tp"),
        P("sp", "tp"),
        P("sp", "tp"),
        P("sp", "tp"),
        P("sp", "tp"),
        P("sp", "tp"),
        P(),
        P(None, "tp"),
        P("tp"),
        P(("fs", "sp"), "tp"),
        P("tp", None, None),
        P("tp"),
        P(),
        P("tp", "sp"),
        P("tp", "sp"),
    )
    return jax.shard_map(
        mixer, mesh=mesh, in_specs=placed, out_specs=P(("fs", "sp", "tp"), None), check_vma=False
    )
```

```python
import functools

import jax
import jax.numpy as jnp
from jax import lax
from jax.experimental import pallas as pl
from jax.experimental.pallas import tpu as pltpu
from jax.sharding import PartitionSpec as P

QH = 32
HD = 64
WINDOW = 128
LOOKUP_FEATURES = 128
DV = 256
SPAN = 64
KVH = 8
GATED_MIXERS = 8


EPS = 1e-05
FADING_SOFTNESS = 16.0
HIGH_PRECISION = lax.Precision.HIGHEST


def passed_along(value, axis, steps):
    count = lax.axis_size(axis)
    leading, last = (max(0, -steps), min(count, count - steps))
    return lax.ppermute(value, axis, [(source, source + steps) for source in range(leading, last)])


def prefix(x, axis, combine, identity):
    peers, place = (lax.axis_size(axis), lax.axis_index(axis))
    everything = jax.tree.map(
        lambda part, kind: lax.all_gather(part.astype(kind), axis), x, (jnp.bfloat16, jnp.bfloat16)
    )
    start = jax.tree.map(
        lambda part, zero: jnp.broadcast_to(jnp.asarray(zero, part.dtype), part.shape), x, identity
    )

    def hop(k, before):
        reached = k < place
        new = combine(
            before, jax.tree.map(lambda part, own: part[k].astype(own.dtype), everything, x)
        )
        return jax.tree.map(lambda a, b: jnp.where(reached, a, b), new, before)

    return lax.fori_loop(0, peers, hop, start)


def window_attention(near_query, near_keys, near_values, head_sink_logit):
    stream_extent = near_query.shape[0]
    key_heads = near_keys.shape[1] // HD
    heads_here = near_query.shape[1] // HD
    groups = heads_here // key_heads
    blocks = stream_extent // WINDOW
    tail_rows = jnp.stack([near_keys, near_values])
    before = passed_along(tail_rows, "sp", 1)

    def banded(previous, current):
        extended = jnp.concatenate([previous, current], axis=0)
        earlier = extended[:stream_extent].reshape(blocks, WINDOW, key_heads, HD)
        present = extended[WINDOW:].reshape(blocks, WINDOW, key_heads, HD)
        return jnp.concatenate([earlier, present], axis=1)

    key_band = banded(before[0], near_keys)
    value_band = banded(before[1], near_values)
    queries = near_query.reshape(blocks, WINDOW, key_heads, groups, HD)
    scores = jnp.einsum(
        "nqhgd,nkhd->hgnqk", queries, key_band, preferred_element_type=jnp.float32
    ) * HD ** (-0.5)
    head_ids = lax.axis_index("tp") * heads_here + jnp.arange(heads_here, dtype=jnp.int32)
    slopes = jnp.exp2(-8.0 * (head_ids + 1).astype(jnp.float32) / QH).reshape(key_heads, groups)
    query_pos = jnp.arange(WINDOW, dtype=jnp.int32)
    key_pos = jnp.arange(2 * WINDOW, dtype=jnp.int32)
    distance = query_pos[:, None] - key_pos[None, :] + WINDOW
    start_pos = (
        lax.axis_index("sp") * stream_extent + (jnp.arange(blocks, dtype=jnp.int32) - 1) * WINDOW
    )
    absolute = start_pos[:, None] + key_pos[None, :]
    allowed = ((distance >= 0) & (distance < WINDOW))[None] & (absolute >= 0)[:, None, :]
    biased = scores - slopes[:, :, None, None, None] * distance.astype(jnp.float32)
    weights = jnp.where(allowed, jnp.exp(biased), 0.0)
    denominator = (
        jnp.sum(weights, axis=-1, keepdims=True)
        + jnp.exp(head_sink_logit.reshape(key_heads, groups))[:, :, None, None, None]
    )
    attention = (weights / denominator).astype(jnp.bfloat16)
    attended = jnp.einsum(
        "hgnqk,nkhd->nqhgd", attention, value_band, preferred_element_type=jnp.float32
    )
    return attended.reshape(stream_extent, heads_here * HD).astype(jnp.bfloat16)


def linear_attention(
    gated_query, gated_keys, gated_values, fading_exponent, linear_head_gain, starting_state
):
    stream_extent = gated_query.shape[0]
    head_total = gated_query.shape[1] // LOOKUP_FEATURES
    span_count = stream_extent // SPAN
    scaled_query = gated_query.astype(jnp.float32).reshape(
        span_count, SPAN, head_total, LOOKUP_FEATURES
    ) * LOOKUP_FEATURES ** (-0.5)
    keys_wide = gated_keys.astype(jnp.float32).reshape(
        span_count, SPAN, head_total, LOOKUP_FEATURES
    )
    values_wide = gated_values.astype(jnp.float32).reshape(span_count, SPAN, head_total, DV)
    running = jnp.cumsum(
        fading_exponent.reshape(span_count, SPAN, head_total, LOOKUP_FEATURES), axis=1
    )
    span_end = running[:, -1]
    query_with_decay = scaled_query * jnp.exp(running)
    inverse_keys = keys_wide * jnp.exp(-running)
    ending_keys = keys_wide * jnp.exp(span_end[:, None] - running)
    inner = jnp.einsum("nchk,nshk->nhcs", query_with_decay, inverse_keys, precision=HIGH_PRECISION)
    lower = jnp.tril(jnp.ones((SPAN, SPAN), dtype=bool))
    inner = jnp.where(lower, inner, 0.0)
    within = jnp.einsum("nhcs,nshv->nchv", inner, values_wide, precision=HIGH_PRECISION)

    def advance(running_state, inputs):
        query_portion, key_portion, value_portion, scale_factor = inputs
        layer_output = jnp.einsum(
            "fmy,mys->fms", query_portion, running_state, precision=HIGH_PRECISION
        )
        running_state = running_state * scale_factor[..., None] + jnp.einsum(
            "gxp,gxz->xpz", key_portion, value_portion, precision=HIGH_PRECISION
        )
        return (running_state, layer_output)

    start_state = jnp.zeros((head_total, LOOKUP_FEATURES, DV), jnp.float32)
    state_end, carried = lax.scan(
        advance, start_state, (query_with_decay, ending_keys, values_wide, jnp.exp(span_end))
    )
    device_decay = jnp.exp(jnp.sum(span_end, axis=0))
    prefix_sums = jnp.cumsum(span_end, axis=0) - span_end

    def combine(earlier, later):
        return (earlier[0] * later[0], later[0][..., None] * earlier[1] + later[1])

    decay_before, state_before = prefix(
        (device_decay, state_end),
        "sp",
        combine,
        (jnp.ones_like(device_decay), jnp.zeros_like(state_end)),
    )
    incoming_rows = state_before + decay_before[..., None] * starting_state
    crossing = jnp.einsum(
        "qwso,soz->qwsz",
        query_with_decay * jnp.exp(prefix_sums)[:, None],
        incoming_rows,
        precision=HIGH_PRECISION,
    )
    flat = (within + carried + crossing).reshape(stream_extent, head_total, DV)
    normal = (
        flat * lax.rsqrt(jnp.mean(flat * flat, axis=-1, keepdims=True) + EPS) * linear_head_gain
    )
    return normal.reshape(stream_extent, head_total * DV).astype(jnp.bfloat16)


def local(
    activations,
    input_norm_gain,
    window_query_weight,
    window_key_weight,
    window_value_weight,
    linear_query_weight,
    linear_key_weight,
    linear_value_weight,
    decay_down_factor,
    decay_up_factor,
    decay_offset_bias,
    extra_fading_exponent,
    starting_state,
    head_sink_logit,
    linear_head_gain,
    window_output_weight,
    linear_output_weight,
):
    gathered = lax.all_gather(activations, "tp", axis=1, tiled=True)
    widened = gathered.astype(jnp.float32)
    normed = (
        widened
        * lax.rsqrt(jnp.mean(widened * widened, axis=1, keepdims=True) + EPS)
        * input_norm_gain
    ).astype(jnp.bfloat16)
    row_total = normed.shape[0]
    matrices = (
        window_query_weight,
        window_key_weight,
        window_value_weight,
        linear_query_weight,
        linear_key_weight,
        linear_value_weight,
    )
    segments = (
        lax.all_gather(matrices[0], "sp", axis=0, tiled=True),
        lax.all_gather(matrices[1], "sp", axis=0, tiled=True),
        lax.all_gather(matrices[2], "sp", axis=0, tiled=True),
        lax.all_gather(matrices[3], "sp", axis=0, tiled=True),
        lax.all_gather(matrices[4], "sp", axis=0, tiled=True),
        lax.all_gather(matrices[5], "sp", axis=0, tiled=True),
    )
    projected = tuple(
        (jnp.dot(normed, segment, preferred_element_type=jnp.float32) for segment in segments)
    )
    near_query, near_keys, near_values, gated_query, gated_keys, gated_values = [
        product.astype(jnp.bfloat16) for product in projected
    ]
    low_rank = jnp.dot(normed, decay_down_factor, preferred_element_type=jnp.float32).astype(
        jnp.bfloat16
    )
    attention_energies = (
        jnp.dot(low_rank, decay_up_factor, preferred_element_type=jnp.float32) + decay_offset_bias
    )
    head_total = extra_fading_exponent.shape[1]
    fading_exponent = (jax.nn.log_sigmoid(attention_energies) / FADING_SOFTNESS).reshape(
        row_total, head_total, LOOKUP_FEATURES
    ) + extra_fading_exponent[:, :, None]
    near_out = window_attention(near_query, near_keys, near_values, head_sink_logit)
    gated_out = linear_attention(
        gated_query, gated_keys, gated_values, fading_exponent, linear_head_gain, starting_state
    )
    window_full, linear_full = (
        lax.all_gather(window_output_weight, "sp", axis=1, tiled=True),
        lax.all_gather(linear_output_weight, "sp", axis=1, tiled=True),
    )
    return lax.psum_scatter(
        (
            jnp.dot(near_out, window_full, preferred_element_type=jnp.float32)
            + jnp.dot(gated_out, linear_full, preferred_element_type=jnp.float32)
        ).astype(jnp.bfloat16),
        "tp",
        scatter_dimension=0,
        tiled=True,
    )


MESH = pl.DeviceIdType.MESH
BF = jnp.bfloat16
F32 = jnp.float32
LAG = 2
CUTS = 2


def dot(a, b):
    return jnp.dot(a, b, preferred_element_type=F32)


def remote(src, dst, send_sem, recv_sem, **where):
    return pltpu.make_async_remote_copy(
        src_ref=src,
        dst_ref=dst,
        send_sem=send_sem,
        recv_sem=recv_sem,
        device_id=where,
        device_id_type=MESH,
    )


def greet(sp, tp):
    s, t = lax.axis_index("sp"), lax.axis_index("tp")
    barrier = pltpu.get_barrier_semaphore()
    for ds in range(sp):
        for dt in range(tp):
            if ds or dt:
                where = {"sp": lax.rem(s + ds, sp), "tp": lax.rem(t + dt, tp)}
                pl.semaphore_signal(barrier, inc=1, device_id=where, device_id_type=MESH)


def greeted(sp, tp):
    pl.semaphore_wait(pltpu.get_barrier_semaphore(), sp * tp - 1)


def columns_dot(a, b):
    return lax.dot_general(a, b, (((1,), (1,)), ((), ())), preferred_element_type=F32)


def mixer_kernel(sp, tp, *refs):
    gain, bias, sink, head_gain, up, fade = refs[:6]
    sources, state_in, down_in, x_in, out = refs[6:14], refs[14], refs[15], refs[16], refs[17]
    weights, start, down, x = refs[18:26], refs[26], refs[27], refs[28]
    squares, blocks, note, term, away, landed = refs[29:35]
    lin_own, win_own, lin_in, win_in, held_g, held_n = refs[35:41]
    w_sem, sq_send, sq_recv, a_send, a_recv, f_send, l_sem, n_send, n_recv = refs[41:50]
    r_send, r_recv, g_send, g_recv, t_send, t_recv, o_send, o_recv, y_sem, turn = refs[50:60]
    s, t = lax.axis_index("sp"), lax.axis_index("tp")
    other = 1 - t
    last = sp - 1
    e = jnp.where(s >= sp // 2, 1, 0)
    at_end = jnp.logical_or(s == 0, s == last)
    inside = jnp.logical_not(at_end)
    per_half = sp // tp
    rows, half = x.shape
    width = half // per_half
    rank = down.shape[0]
    lk = LOOKUP_FEATURES
    mine = lin_own.shape[2]
    lane_of = {i: weights[i].shape[1] // 2 for i in range(6)}
    greet(sp, tp)
    loads = [
        pltpu.make_async_copy(a, b, w_sem.at[i]) for i, (a, b) in enumerate(zip(sources, weights))
    ]
    loads.append(pltpu.make_async_copy(state_in.at[pl.ds(e * mine, mine)], start, w_sem.at[8]))
    loads.append(
        pltpu.make_async_copy(
            down_in.at[:, pl.ds(pl.multiple_of(t * half, half), half)], down, w_sem.at[9]
        )
    )
    loads.append(pltpu.make_async_copy(x_in, x, w_sem.at[10]))
    for i in (10, 9, 3, 4, 5, 0, 1, 2, 8, 6, 7):
        loads[i].start()
    loads[10].wait()
    wide = x[...].astype(F32)
    own = jnp.sum(wide * wide, axis=1, keepdims=True)
    squares[s, t] = jnp.broadcast_to(own, (rows, rows)).T[:8]
    home = lax.div(s, per_half) == t

    def slice_send(i):
        src = x.at[:, i * width : (i + 1) * width]
        return remote(src, blocks.at[s], a_send.at[i], a_recv.at[s], sp=t * per_half + i)

    def forward(b):
        return remote(blocks.at[b], blocks.at[b], f_send.at[b], a_recv.at[b], tp=other)

    def squares_send(n):
        where = {"sp": lax.rem(s + n // tp, sp), "tp": lax.rem(t + n % tp, tp)}
        ref = squares.at[s, t]
        return remote(ref, ref, sq_send.at[n], sq_recv.at[s, t], **where)

    def keep(i):
        return pltpu.make_async_copy(x.at[:, i * width : (i + 1) * width], blocks.at[s], l_sem)

    def share(i):
        src = x.at[:, i * width : (i + 1) * width]
        return remote(src, blocks.at[s], f_send.at[s], a_recv.at[s], tp=other)

    greeted(sp, tp)
    for n in range(1, sp * tp):
        squares_send(n).start()
    for i in reversed(range(per_half)):
        j = t * per_half + i

        @pl.when((j < s) | ((j > s) & (s == 0) & (t > 0)))
        def _():
            slice_send(i).start()

        @pl.when(j == s)
        def _():
            share(i).start()
            keep(i).start()

    def squares_wait(ps, pt):
        ref = squares.at[ps, pt]
        remote(ref, ref, sq_send.at[0], sq_recv.at[ps, pt], tp=other).wait_recv()

    def scale_of(b):
        total = jnp.sum(squares[b], axis=0) / (half * tp)
        tall = jnp.concatenate([lax.rsqrt(total + EPS), jnp.zeros((rows - 8, rows), F32)], axis=0)
        return tall.T[:, :1]

    squares_wait(s, other)
    scale = scale_of(s)
    loads[9].wait()
    low = jnp.zeros((rank, rows), F32)
    for i in range(per_half):
        cols = slice(i * width, (i + 1) * width)
        shaped = (x[:, cols].astype(F32) * scale * gain[t, :, cols]).astype(BF)
        low += columns_dot(down[:, cols], shaped)
    fades = fade.shape[0]
    noted = note.shape[2]
    note[s, t] = jnp.concatenate(
        [low, fade[...], jnp.zeros((noted - rank - fades, rows), F32)], axis=0
    )

    def note_send(n):
        place, core = (0 if n < tp else last), lax.rem(t + n % tp, tp)
        ref = note.at[s, t]
        return remote(ref, ref, n_send.at[n], n_recv.at[s, t], sp=place, tp=core), jnp.logical_or(
            s != place, core != t
        )

    for n in range(2 * tp):
        send, away_from_here = note_send(n)

        @pl.when(away_from_here)
        def _():
            send.start()

    cut_rows = rows // CUTS
    pieces = [(i, slice(r * cut_rows, (r + 1) * cut_rows)) for i in range(mine + 1) for r in range(CUTS)]

    def step(way, b, n):
        i, cut = pieces[n]
        src = lin_own.at[b, 1 - way, i, cut] if i < mine else win_own.at[b, 1 - way, cut]
        dst = lin_in.at[way, b, i, cut] if i < mine else win_in.at[way, b, cut]
        return remote(
            src, dst, r_send.at[way, b, n], r_recv.at[way, b, n], sp=jnp.clip(s + 1 - 2 * way, 0, last)
        )

    def relay(way, b, n):
        i, cut = pieces[n]
        step(way, b, n).wait_recv()
        if i < mine:
            lin_own[b, 1 - way, i, cut] = (
                lin_own[b, 1 - way, i, cut].astype(F32) + lin_in[way, b, i, cut].astype(F32)
            ).astype(BF)
        else:
            win_own[b, 1 - way, cut] = (
                win_own[b, 1 - way, cut].astype(F32) + win_in[way, b, cut].astype(F32)
            ).astype(BF)
        step(way, b, n).start()

    for i in range(6):
        loads[i].wait()
    qw, kw = lane_of[0], lane_of[1]
    gain_here = gain[lax.div(s, per_half), :, pl.ds(pl.multiple_of(lax.rem(s, per_half) * width, width), width)]

    def send_sums(b):
        for n in range(len(pieces)):
            step(e, b, n).start()

    def project(k, carry):
        b = lax.rem(s + k, sp)

        @pl.when((s > 1) & inside & (k == sp - 1))
        def _():
            relay(e, 0, 0)

        @pl.when(jnp.logical_or(jnp.logical_not(home), b != s))
        def _():
            forward(b).wait_recv()

        @pl.when(jnp.logical_and(home, b != s))
        def _():
            forward(b).start()

        @pl.when(jnp.logical_and(home, b == s))
        def _():
            keep(0).wait()

        @pl.when(b != s)
        def _():
            for pt in range(tp):
                squares_wait(b, pt)

        for i in reversed(range(per_half)):

            @pl.when((b == 0) & (s > 1) & (t * per_half + i > s))
            def _():
                slice_send(i).start()

        block = (blocks[b].astype(F32) * scale_of(b) * gain_here).astype(BF)

        def part(i, h):
            w = lane_of[i]
            return dot(block, weights[i][:, pl.ds(pl.multiple_of(h * w, w), w)]).astype(BF)

        for n in range(2):
            h = e if n else 1 - e
            query, key, value = part(3, h), part(4, h), part(5, h)
            for i in range(mine):
                lin_own[b, h, i, :, :lk] = query[:, i * lk : (i + 1) * lk]
                lin_own[b, h, i, :, lk : 2 * lk] = key[:, i * lk : (i + 1) * lk]
                lin_own[b, h, i, :, 2 * lk :] = value[:, i * DV : (i + 1) * DV]
            if n == 0:

                @pl.when((s == 0) & (t > 0) & (k == 0))
                def _():
                    slice_send(per_half - 1).wait_send()
                    pl.semaphore_signal(turn, inc=1, device_id={"tp": other}, device_id_type=MESH)

                @pl.when((s == 0) & (t == 0) & (k == 0))
                def _():
                    pl.semaphore_wait(turn, 1)
                    for i in range(1, per_half):
                        slice_send(i).start()

                for i in reversed(range(per_half)):

                    @pl.when((k == 0) & (s == 1) & (t * per_half + i > s))
                    def _():
                        slice_send(i).start()

                @pl.when(at_end & (k >= e))
                def _():
                    for m in range(mine * CUTS):
                        step(e, b, m).start()

            win_own[b, h, :, :qw] = part(0, h)
            win_own[b, h, :, qw : qw + kw] = part(1, h)
            win_own[b, h, :, qw + kw :] = part(2, h)
            if n == 0:

                @pl.when(at_end & (k >= e))
                def _():
                    for m in range(mine * CUTS, len(pieces)):
                        step(e, b, m).start()

        return carry

    lax.fori_loop(0, sp, project, 0)

    @pl.when(s == last)
    def _():
        send_sums(last)

    def gather(way, b, n):
        i, r = divmod(n, CUTS)
        ref = (held_n if i else held_g).at[b, way, slice(r * cut_rows, (r + 1) * cut_rows)]
        return remote(
            ref, ref, g_send.at[way, b, n], g_recv.at[way, b, n], sp=jnp.clip(s + 1 - 2 * way, 0, last)
        )

    part_rows = rows // tp
    cols_g, cols_n = held_g.shape[3], held_n.shape[3]

    def swap(b):
        return remote(term.at[b, other], away.at[b], t_send.at[b], t_recv.at[b], tp=other)

    def deliver(b):
        return remote(term.at[b, t], landed.at[s], o_send.at[b], o_recv.at[s], sp=b)

    def close(b):
        swap(b).wait()
        term[b, t] = (term[b, t].astype(F32) + away[b].astype(F32)).astype(BF)

        @pl.when(s != b)
        def _():
            deliver(b).start()

        @pl.when(s == b)
        def _():
            landed[b] = term[b, t]

    def multiply(b):
        total = None
        for src in range(2):
            piece = dot(held_g[b, src], weights[7][src * cols_g : (src + 1) * cols_g]) + dot(
                held_n[b, src], weights[6][src * cols_n : (src + 1) * cols_n]
            )
            total = piece if total is None else total + piece
        for h in range(tp):
            term[b, h] = total[h * part_rows : (h + 1) * part_rows].astype(BF)
        swap(b).start()

    def pass_on(way, b, i):
        gather(way, b, i).wait_recv()
        gather(way, b, i).start()

    @pl.when(inside)
    def _():
        loads[8].wait()
        items = [(relay, b, i) for b in range(sp) for i in range(len(pieces))]
        items += [(pass_on, b, i) for b in range(sp) for i in range(2 * CUTS)]
        for n in range(len(items) + LAG):
            if n == 0:

                @pl.when(s <= 1)
                def _():
                    relay(e, 0, 0)

            elif n < len(items):
                what, b, i = items[n]
                what(e, b, i)
            if n >= LAG:
                what, b, i = items[n - LAG]
                what(1 - e, b, i)
                if what is pass_on and i == 2 * CUTS - 1:
                    if b == 0:
                        loads[6].wait()
                        loads[7].wait()
                    if b == last:
                        for c in range(1, last):
                            close(c)
                    multiply(b)
        close(last)
        close(0)

    @pl.when(at_end)
    def _():
        loads[8].wait()
        for ps in range(sp):
            for pt in range(tp):

                @pl.when(jnp.logical_or(s != ps, t != pt))
                def _():
                    ref = note.at[ps, pt]
                    remote(ref, ref, n_send.at[0], n_recv.at[ps, pt], tp=other).wait_recv()

        span = mine * lk
        lane = pl.ds(pl.multiple_of(e * span, span), span)
        up_own = jnp.concatenate([up[:, lane], jnp.zeros((rows - rank, span), BF)], axis=0)
        bias_own = bias[:, lane]
        row_at = lax.broadcasted_iota(jnp.int32, (rows, rows), 0)
        col_at = lax.broadcasted_iota(jnp.int32, (rows, rows), 1)
        span_low = jnp.logical_and(row_at >= col_at, row_at // SPAN == col_at // SPAN)
        ones_low = jnp.where(span_low, 1.0, 0.0).astype(BF)
        query_at = lax.broadcasted_iota(jnp.int32, (rows, 2 * rows), 0)
        key_at = lax.broadcasted_iota(jnp.int32, (rows, 2 * rows), 1)
        distance = query_at - key_at + rows
        near_by = jnp.logical_and(distance >= 0, distance < WINDOW)
        far = distance.astype(F32)
        heads = qw // HD // mine

        def linear(b, states):
            rank_rows = note[b, 0, :rank] + note[b, 1, :rank]
            tall = jnp.concatenate(
                [rank_rows, note[b, t, rank:], jnp.zeros((rows - noted, rows), F32)], axis=0
            ).T
            energies = dot(tall.astype(BF), up_own) + bias_own
            soft = jnp.minimum(energies, 0.0) - jnp.log1p(jnp.exp(-jnp.abs(energies)))
            soft = soft / FADING_SOFTNESS
            fading = []
            for i in range(mine):
                extra = jnp.sum(
                    jnp.where(col_at == rank + e * mine + i, tall, 0.0), axis=1, keepdims=True
                )
                fading.append(soft[:, i * lk : (i + 1) * lk] + extra)
            fading = jnp.concatenate(fading, axis=1)
            top = fading.astype(BF)
            rest = fading - top.astype(F32)
            middle = rest.astype(BF)
            bottom = (rest - middle.astype(F32)).astype(BF)
            summed = dot(ones_low, jnp.concatenate([top, middle, bottom], axis=1))
            running_all = summed[:, :span] + (summed[:, span : 2 * span] + summed[:, 2 * span :])
            new_states = []
            for i in range(mine):
                for r in range(CUTS):
                    step(1 - e, b, i * CUTS + r).wait_recv()
                here = (lin_own[b, e, i].astype(F32) + lin_in[1 - e, b, i].astype(F32)).astype(BF)
                running = running_all[:, i * lk : (i + 1) * lk]
                state = states[i]
                query = here[:, :lk].astype(F32) * lk ** (-0.5)
                key = here[:, lk : 2 * lk].astype(F32)
                value = here[:, 2 * lk :]
                decayed = (query * jnp.exp(running)).astype(BF)
                inner = columns_dot(decayed, (key * jnp.exp(-running)).astype(BF))
                inner = jnp.where(span_low, inner, 0.0).astype(BF)
                within = dot(inner, value)
                carried = []
                for j in range(rows // SPAN):
                    cut = slice(j * SPAN, (j + 1) * SPAN)
                    end = running[(j + 1) * SPAN - 1 : (j + 1) * SPAN]
                    ending = (key[cut] * jnp.exp(end - running[cut])).astype(BF)
                    carried.append(columns_dot(decayed[cut], state.astype(BF)))
                    state = state * jnp.exp(end) + lax.dot_general(
                        value[cut], ending, (((0,), (0,)), ((), ())), preferred_element_type=F32
                    )
                flat = within + jnp.concatenate(carried, axis=0)
                normal = (
                    flat
                    * lax.rsqrt(jnp.mean(flat * flat, axis=-1, keepdims=True) + EPS)
                    * head_gain[...]
                )
                held_g[b, e, :, i * DV : (i + 1) * DV] = normal.astype(BF)
                new_states.append(state)
            for r in range(CUTS):
                gather(e, b, r).start()
            return new_states

        def window(b):
            for r in range(CUTS):
                step(1 - e, b, mine * CUTS + r).wait_recv()
            win_own[b, e] = (win_own[b, e].astype(F32) + win_in[1 - e, b].astype(F32)).astype(BF)
            present = win_own[b, e]
            earlier = win_own[max(b - 1, 0), e]
            allowed = near_by if b else jnp.logical_and(near_by, key_at >= rows)
            for g in range(mine):
                ka, va = qw + g * HD, qw + kw + g * HD
                keys = jnp.concatenate([earlier[:, ka : ka + HD], present[:, ka : ka + HD]], axis=0)
                vals = jnp.concatenate([earlier[:, va : va + HD], present[:, va : va + HD]], axis=0)
                results = []
                for h in range(heads):
                    local = (e * mine + g) * heads + h
                    number = (t * (2 * mine * heads) + local + 1).astype(F32)
                    slope = jnp.exp2(jnp.full((rows, 1), -8.0 / QH, F32) * number)
                    at = (g * heads + h) * HD
                    score = (
                        columns_dot(present[:, at : at + HD], keys) * HD ** (-0.5) - slope * far
                    )
                    weight = jnp.where(allowed, jnp.exp(score), 0.0)
                    floor = jnp.exp(jnp.full((rows, 1), sink[local], F32))
                    probs = (weight / (jnp.sum(weight, axis=1, keepdims=True) + floor)).astype(BF)
                    results.append(dot(probs, vals))
                wide_to = heads * HD
                held_n[b, e, :, g * wide_to : (g + 1) * wide_to] = jnp.concatenate(
                    results, axis=1
                ).astype(BF)
            for r in range(CUTS):
                gather(e, b, CUTS + r).start()

        def collect(b):
            for i in range(2 * CUTS):
                gather(1 - e, b, i).wait_recv()

        states = [start[i].T for i in range(mine)]
        for b in range(sp):
            states = linear(b, states)
            window(b)
        loads[6].wait()
        loads[7].wait()
        for b in range(sp):
            collect(b)
            multiply(b)
            if b == last - 1:
                for c in (*range(1, last), 0):
                    close(c)
        close(last)

    def drain(b, carry):
        for i in range(len(pieces)):
            for way in range(2):

                @pl.when(s != last * (1 - way))
                def _():
                    step(way, b, i).wait_send()

        for i in range(2 * CUTS):
            for way in range(2):

                @pl.when(s != last * (1 - way))
                def _():
                    gather(way, b, i).wait_send()

        @pl.when(home)
        def _():
            forward(b).wait_send()

        return carry

    lax.fori_loop(0, sp, drain, 0)
    for i in range(per_half):

        @pl.when((t * per_half + i != s) & ((s > 0) | (t == 0) | (i < per_half - 1)))
        def _():
            slice_send(i).wait_send()

    for n in range(2 * tp):
        send, away_from_here = note_send(n)

        @pl.when(away_from_here)
        def _():
            send.wait_send()

    for n in range(1, sp * tp):
        squares_send(n).wait_send()

    columns = landed.shape[2]

    def leave(b):
        return pltpu.make_async_copy(
            landed.at[b], out.at[:, pl.ds(b * columns, columns)], y_sem.at[b]
        )

    for b in range(sp):

        @pl.when(s != b)
        def _():
            deliver(b).wait_send()
            remote(landed.at[b], landed.at[b], o_send.at[b], o_recv.at[b], tp=other).wait_recv()

        leave(b).start()
    for b in range(sp):
        leave(b).wait()


def stationary(
    activations,
    input_norm_gain,
    window_query_weight,
    window_key_weight,
    window_value_weight,
    linear_query_weight,
    linear_key_weight,
    linear_value_weight,
    decay_down_factor,
    decay_up_factor,
    decay_offset_bias,
    extra_fading_exponent,
    starting_state,
    head_sink_logit,
    linear_head_gain,
    window_output_weight,
    linear_output_weight,
):
    sp, tp = lax.axis_size("sp"), lax.axis_size("tp")
    rows, half = activations.shape
    matrices = (
        window_query_weight,
        window_key_weight,
        window_value_weight,
        linear_query_weight,
        linear_key_weight,
        linear_value_weight,
        window_output_weight,
        linear_output_weight,
    )
    rank = decay_down_factor.shape[1]
    heads_tp = extra_fading_exponent.shape[1]
    mine = heads_tp // 2
    noted = rank + heads_tp + -(rank + heads_tp) % 8
    columns = window_output_weight.shape[1]
    vmem = pl.BlockSpec(memory_space=pltpu.VMEM)
    hbm = pl.BlockSpec(memory_space=pltpu.HBM)
    dma = pltpu.SemaphoreType.DMA
    slice_width = half * tp // sp
    lin_cols = sum(m.shape[1] for m in matrices[3:6]) // heads_tp
    win_cols = sum(m.shape[1] for m in matrices[:3]) // 2
    return pl.pallas_call(
        functools.partial(mixer_kernel, sp, tp),
        out_shape=jax.ShapeDtypeStruct((rows // tp, columns * sp), BF),
        in_specs=[vmem] * 2
        + [pl.BlockSpec(memory_space=pltpu.SMEM)]
        + [vmem] * 3
        + [hbm] * 11,
        out_specs=hbm,
        scratch_shapes=[pltpu.VMEM(m.shape, BF) for m in matrices]
        + [
            pltpu.VMEM((mine,) + starting_state.shape[1:], F32),
            pltpu.VMEM((rank, half), BF),
            pltpu.VMEM((rows, half), BF),
            pltpu.VMEM((sp, tp, 8, rows), F32),
            pltpu.VMEM((sp, rows, slice_width), BF),
            pltpu.VMEM((sp, tp, noted, rows), F32),
            pltpu.VMEM((sp, tp, rows // tp, columns), BF),
            pltpu.VMEM((sp, rows // tp, columns), BF),
            pltpu.VMEM((sp, rows // tp, columns), BF),
            pltpu.VMEM((sp, 2, mine, rows, lin_cols), BF),
            pltpu.VMEM((sp, 2, rows, win_cols), BF),
            pltpu.VMEM((2, sp, mine, rows, lin_cols), BF),
            pltpu.VMEM((2, sp, rows, win_cols), BF),
            pltpu.VMEM((sp, 2, rows, linear_output_weight.shape[0] // 2), BF),
            pltpu.VMEM((sp, 2, rows, window_output_weight.shape[0] // 2), BF),
            dma((11,)),
            dma((sp * tp,)),
            dma((sp, tp)),
            dma((sp // tp,)),
            dma((sp,)),
            dma((sp,)),
            dma,
            dma((2 * tp,)),
            dma((sp, tp)),
        ]
        + [dma((2, sp, (mine + 1) * CUTS))] * 2
        + [dma((2, sp, 2 * CUTS))] * 2
        + [dma((sp,))] * 5
        + [pltpu.SemaphoreType.REGULAR],
        compiler_params=pltpu.CompilerParams(
            collective_id=0, has_side_effects=True, vmem_limit_bytes=56 * 2**20
        ),
    )(
        input_norm_gain.reshape(tp, 1, half),
        decay_offset_bias.reshape(1, -1),
        head_sink_logit,
        linear_head_gain.reshape(1, -1),
        decay_up_factor,
        extra_fading_exponent.T,
        *matrices,
        starting_state,
        decay_down_factor.T,
        activations,
    )


def mixer(*arrays):
    sp, tp = lax.axis_size("sp"), lax.axis_size("tp")
    rows = arrays[0].shape[0]
    one_each = KVH == GATED_MIXERS == sp * tp and QH % KVH == 0
    if tp == 2 and sp % tp == 0 and sp > 2 and one_each and rows == WINDOW and rows % SPAN == 0:
        return stationary(*arrays)
    return local(*arrays)


def solution(mesh):
    placed = (
        P(("fs", "sp"), "tp"),
        P(),
        P("sp", "tp"),
        P("sp", "tp"),
        P("sp", "tp"),
        P("sp", "tp"),
        P("sp", "tp"),
        P("sp", "tp"),
        P(),
        P(None, "tp"),
        P("tp"),
        P(("fs", "sp"), "tp"),
        P("tp", None, None),
        P("tp"),
        P(),
        P("tp", "sp"),
        P("tp", "sp"),
    )
    return jax.shard_map(
        mixer, mesh=mesh, in_specs=placed, out_specs=P(("fs", "sp", "tp"), None), check_vma=False
    )
```

```python
import functools

import jax
import jax.numpy as jnp
from jax import lax
from jax.experimental import pallas as pl
from jax.experimental.pallas import tpu as pltpu
from jax.sharding import PartitionSpec as P

QH = 32
HD = 64
WINDOW = 128
LOOKUP_FEATURES = 128
DV = 256
SPAN = 64
KVH = 8
GATED_MIXERS = 8


EPS = 1e-05
FADING_SOFTNESS = 16.0
HIGH_PRECISION = lax.Precision.HIGHEST


def passed_along(value, axis, steps):
    count = lax.axis_size(axis)
    leading, last = (max(0, -steps), min(count, count - steps))
    return lax.ppermute(value, axis, [(source, source + steps) for source in range(leading, last)])


def prefix(x, axis, combine, identity):
    peers, place = (lax.axis_size(axis), lax.axis_index(axis))
    everything = jax.tree.map(
        lambda part, kind: lax.all_gather(part.astype(kind), axis), x, (jnp.bfloat16, jnp.bfloat16)
    )
    start = jax.tree.map(
        lambda part, zero: jnp.broadcast_to(jnp.asarray(zero, part.dtype), part.shape), x, identity
    )

    def hop(k, before):
        reached = k < place
        new = combine(
            before, jax.tree.map(lambda part, own: part[k].astype(own.dtype), everything, x)
        )
        return jax.tree.map(lambda a, b: jnp.where(reached, a, b), new, before)

    return lax.fori_loop(0, peers, hop, start)


def window_attention(near_query, near_keys, near_values, head_sink_logit):
    stream_extent = near_query.shape[0]
    key_heads = near_keys.shape[1] // HD
    heads_here = near_query.shape[1] // HD
    groups = heads_here // key_heads
    blocks = stream_extent // WINDOW
    tail_rows = jnp.stack([near_keys, near_values])
    before = passed_along(tail_rows, "sp", 1)

    def banded(previous, current):
        extended = jnp.concatenate([previous, current], axis=0)
        earlier = extended[:stream_extent].reshape(blocks, WINDOW, key_heads, HD)
        present = extended[WINDOW:].reshape(blocks, WINDOW, key_heads, HD)
        return jnp.concatenate([earlier, present], axis=1)

    key_band = banded(before[0], near_keys)
    value_band = banded(before[1], near_values)
    queries = near_query.reshape(blocks, WINDOW, key_heads, groups, HD)
    scores = jnp.einsum(
        "nqhgd,nkhd->hgnqk", queries, key_band, preferred_element_type=jnp.float32
    ) * HD ** (-0.5)
    head_ids = lax.axis_index("tp") * heads_here + jnp.arange(heads_here, dtype=jnp.int32)
    slopes = jnp.exp2(-8.0 * (head_ids + 1).astype(jnp.float32) / QH).reshape(key_heads, groups)
    query_pos = jnp.arange(WINDOW, dtype=jnp.int32)
    key_pos = jnp.arange(2 * WINDOW, dtype=jnp.int32)
    distance = query_pos[:, None] - key_pos[None, :] + WINDOW
    start_pos = (
        lax.axis_index("sp") * stream_extent + (jnp.arange(blocks, dtype=jnp.int32) - 1) * WINDOW
    )
    absolute = start_pos[:, None] + key_pos[None, :]
    allowed = ((distance >= 0) & (distance < WINDOW))[None] & (absolute >= 0)[:, None, :]
    biased = scores - slopes[:, :, None, None, None] * distance.astype(jnp.float32)
    weights = jnp.where(allowed, jnp.exp(biased), 0.0)
    denominator = (
        jnp.sum(weights, axis=-1, keepdims=True)
        + jnp.exp(head_sink_logit.reshape(key_heads, groups))[:, :, None, None, None]
    )
    attention = (weights / denominator).astype(jnp.bfloat16)
    attended = jnp.einsum(
        "hgnqk,nkhd->nqhgd", attention, value_band, preferred_element_type=jnp.float32
    )
    return attended.reshape(stream_extent, heads_here * HD).astype(jnp.bfloat16)


def linear_attention(
    gated_query, gated_keys, gated_values, fading_exponent, linear_head_gain, starting_state
):
    stream_extent = gated_query.shape[0]
    head_total = gated_query.shape[1] // LOOKUP_FEATURES
    span_count = stream_extent // SPAN
    scaled_query = gated_query.astype(jnp.float32).reshape(
        span_count, SPAN, head_total, LOOKUP_FEATURES
    ) * LOOKUP_FEATURES ** (-0.5)
    keys_wide = gated_keys.astype(jnp.float32).reshape(
        span_count, SPAN, head_total, LOOKUP_FEATURES
    )
    values_wide = gated_values.astype(jnp.float32).reshape(span_count, SPAN, head_total, DV)
    running = jnp.cumsum(
        fading_exponent.reshape(span_count, SPAN, head_total, LOOKUP_FEATURES), axis=1
    )
    span_end = running[:, -1]
    query_with_decay = scaled_query * jnp.exp(running)
    inverse_keys = keys_wide * jnp.exp(-running)
    ending_keys = keys_wide * jnp.exp(span_end[:, None] - running)
    inner = jnp.einsum("nchk,nshk->nhcs", query_with_decay, inverse_keys, precision=HIGH_PRECISION)
    lower = jnp.tril(jnp.ones((SPAN, SPAN), dtype=bool))
    inner = jnp.where(lower, inner, 0.0)
    within = jnp.einsum("nhcs,nshv->nchv", inner, values_wide, precision=HIGH_PRECISION)

    def advance(running_state, inputs):
        query_portion, key_portion, value_portion, scale_factor = inputs
        layer_output = jnp.einsum(
            "fmy,mys->fms", query_portion, running_state, precision=HIGH_PRECISION
        )
        running_state = running_state * scale_factor[..., None] + jnp.einsum(
            "gxp,gxz->xpz", key_portion, value_portion, precision=HIGH_PRECISION
        )
        return (running_state, layer_output)

    start_state = jnp.zeros((head_total, LOOKUP_FEATURES, DV), jnp.float32)
    state_end, carried = lax.scan(
        advance, start_state, (query_with_decay, ending_keys, values_wide, jnp.exp(span_end))
    )
    device_decay = jnp.exp(jnp.sum(span_end, axis=0))
    prefix_sums = jnp.cumsum(span_end, axis=0) - span_end

    def combine(earlier, later):
        return (earlier[0] * later[0], later[0][..., None] * earlier[1] + later[1])

    decay_before, state_before = prefix(
        (device_decay, state_end),
        "sp",
        combine,
        (jnp.ones_like(device_decay), jnp.zeros_like(state_end)),
    )
    incoming_rows = state_before + decay_before[..., None] * starting_state
    crossing = jnp.einsum(
        "qwso,soz->qwsz",
        query_with_decay * jnp.exp(prefix_sums)[:, None],
        incoming_rows,
        precision=HIGH_PRECISION,
    )
    flat = (within + carried + crossing).reshape(stream_extent, head_total, DV)
    normal = (
        flat * lax.rsqrt(jnp.mean(flat * flat, axis=-1, keepdims=True) + EPS) * linear_head_gain
    )
    return normal.reshape(stream_extent, head_total * DV).astype(jnp.bfloat16)


def local(
    activations,
    input_norm_gain,
    window_query_weight,
    window_key_weight,
    window_value_weight,
    linear_query_weight,
    linear_key_weight,
    linear_value_weight,
    decay_down_factor,
    decay_up_factor,
    decay_offset_bias,
    extra_fading_exponent,
    starting_state,
    head_sink_logit,
    linear_head_gain,
    window_output_weight,
    linear_output_weight,
):
    gathered = lax.all_gather(activations, "tp", axis=1, tiled=True)
    widened = gathered.astype(jnp.float32)
    normed = (
        widened
        * lax.rsqrt(jnp.mean(widened * widened, axis=1, keepdims=True) + EPS)
        * input_norm_gain
    ).astype(jnp.bfloat16)
    row_total = normed.shape[0]
    matrices = (
        window_query_weight,
        window_key_weight,
        window_value_weight,
        linear_query_weight,
        linear_key_weight,
        linear_value_weight,
    )
    segments = (
        lax.all_gather(matrices[0], "sp", axis=0, tiled=True),
        lax.all_gather(matrices[1], "sp", axis=0, tiled=True),
        lax.all_gather(matrices[2], "sp", axis=0, tiled=True),
        lax.all_gather(matrices[3], "sp", axis=0, tiled=True),
        lax.all_gather(matrices[4], "sp", axis=0, tiled=True),
        lax.all_gather(matrices[5], "sp", axis=0, tiled=True),
    )
    projected = tuple(
        (jnp.dot(normed, segment, preferred_element_type=jnp.float32) for segment in segments)
    )
    near_query, near_keys, near_values, gated_query, gated_keys, gated_values = [
        product.astype(jnp.bfloat16) for product in projected
    ]
    low_rank = jnp.dot(normed, decay_down_factor, preferred_element_type=jnp.float32).astype(
        jnp.bfloat16
    )
    attention_energies = (
        jnp.dot(low_rank, decay_up_factor, preferred_element_type=jnp.float32) + decay_offset_bias
    )
    head_total = extra_fading_exponent.shape[1]
    fading_exponent = (jax.nn.log_sigmoid(attention_energies) / FADING_SOFTNESS).reshape(
        row_total, head_total, LOOKUP_FEATURES
    ) + extra_fading_exponent[:, :, None]
    near_out = window_attention(near_query, near_keys, near_values, head_sink_logit)
    gated_out = linear_attention(
        gated_query, gated_keys, gated_values, fading_exponent, linear_head_gain, starting_state
    )
    window_full, linear_full = (
        lax.all_gather(window_output_weight, "sp", axis=1, tiled=True),
        lax.all_gather(linear_output_weight, "sp", axis=1, tiled=True),
    )
    return lax.psum_scatter(
        (
            jnp.dot(near_out, window_full, preferred_element_type=jnp.float32)
            + jnp.dot(gated_out, linear_full, preferred_element_type=jnp.float32)
        ).astype(jnp.bfloat16),
        "tp",
        scatter_dimension=0,
        tiled=True,
    )


MESH = pl.DeviceIdType.MESH
BF = jnp.bfloat16
F32 = jnp.float32
LAG = 2
CUTS = 2
EARLY = 3


def dot(a, b):
    return jnp.dot(a, b, preferred_element_type=F32)


def remote(src, dst, send_sem, recv_sem, **where):
    return pltpu.make_async_remote_copy(
        src_ref=src,
        dst_ref=dst,
        send_sem=send_sem,
        recv_sem=recv_sem,
        device_id=where,
        device_id_type=MESH,
    )


def greet(sp, tp):
    s, t = lax.axis_index("sp"), lax.axis_index("tp")
    barrier = pltpu.get_barrier_semaphore()
    for ds in range(sp):
        for dt in range(tp):
            if ds or dt:
                where = {"sp": lax.rem(s + ds, sp), "tp": lax.rem(t + dt, tp)}
                pl.semaphore_signal(barrier, inc=1, device_id=where, device_id_type=MESH)


def greeted(sp, tp):
    pl.semaphore_wait(pltpu.get_barrier_semaphore(), sp * tp - 1)


def columns_dot(a, b):
    return lax.dot_general(a, b, (((1,), (1,)), ((), ())), preferred_element_type=F32)


def mixer_kernel(sp, tp, *refs):
    small_in, sources, state_in, down_in, x_in = refs[:6], refs[6:14], refs[14], refs[15], refs[16]
    out = refs[17]
    weights, start, down, x = refs[18:26], refs[26], refs[27], refs[28]
    gain, bias, sink, head_gain, up, fade = refs[59:65]
    squares, blocks, note, term, away = refs[29:34]
    lin_own, win_own, lin_in, win_in, held_g, held_n = refs[34:40]
    w_sem, sq_send, sq_recv, a_send, a_recv, f_send, l_sem, n_send, n_recv = refs[40:49]
    r_send, r_recv, g_send, g_recv, t_send, t_recv, o_send, o_recv, turn, s_sem = refs[49:59]
    s, t = lax.axis_index("sp"), lax.axis_index("tp")
    other = 1 - t
    last = sp - 1
    e = jnp.where(s >= sp // 2, 1, 0)
    at_end = jnp.logical_or(s == 0, s == last)
    inside = jnp.logical_not(at_end)
    per_half = sp // tp
    rows, half = x.shape
    width = half // per_half
    rank = down.shape[0]
    lk = LOOKUP_FEATURES
    mine = lin_own.shape[2]
    lane_of = {i: weights[i].shape[1] // 2 for i in range(6)}
    greet(sp, tp)
    loads = [
        pltpu.make_async_copy(a, b, w_sem.at[i]) for i, (a, b) in enumerate(zip(sources, weights))
    ]
    loads.append(pltpu.make_async_copy(state_in.at[pl.ds(e * mine, mine)], start, w_sem.at[8]))
    loads.append(
        pltpu.make_async_copy(
            down_in.at[:, pl.ds(pl.multiple_of(t * half, half), half)], down, w_sem.at[9]
        )
    )
    loads.append(pltpu.make_async_copy(x_in, x, w_sem.at[10]))
    small = [
        pltpu.make_async_copy(a, b, s_sem.at[i]) for i, (a, b) in enumerate(zip(small_in, refs[59:65]))
    ]
    loads[10].start()
    for copy in small:
        copy.start()
    for i in (9, 3, 4, 5, 0, 1, 2, 8, 6, 7):
        loads[i].start()
    home = lax.div(s, per_half) == t

    def slice_send(i):
        src = x.at[:, i * width : (i + 1) * width]
        return remote(src, blocks.at[s], a_send.at[i], a_recv.at[s], sp=t * per_half + i)

    def forward(b):
        return remote(blocks.at[b], blocks.at[b], f_send, a_recv.at[b], tp=other)

    me = s * tp + t

    def squares_send(n):
        where = {"sp": lax.rem(s + n // tp, sp), "tp": lax.rem(t + n % tp, tp)}
        ref = squares.at[me]
        return remote(ref, ref, sq_send, sq_recv.at[0 if n // tp == 0 else 1], **where)

    def keep(i):
        return pltpu.make_async_copy(x.at[:, i * width : (i + 1) * width], blocks.at[s], l_sem)

    def share(i):
        src = x.at[:, i * width : (i + 1) * width]
        return remote(src, blocks.at[s], f_send, a_recv.at[s], tp=other)

    loads[10].wait()
    wide = x[...].astype(F32)
    own = jnp.sum(wide * wide, axis=1, keepdims=True)
    squares[me] = jnp.broadcast_to(own, (rows, rows)).T[:8]
    greeted(sp, tp)
    for n in range(1, sp * tp):
        squares_send(n).start()
    for i in reversed(range(per_half)):
        j = t * per_half + i

        @pl.when((j < s) | ((j > s) & (s == 0) & (t > 0)))
        def _():
            slice_send(i).start()

        @pl.when(j == s)
        def _():
            share(i).start()
            keep(i).start()

    def squares_wait(n, k):
        ref = squares.at[pl.ds(0, n)]
        remote(ref, ref, sq_send, sq_recv.at[k], tp=other).wait_recv()

    def scale_of(b):
        total = (squares[b * tp] + squares[b * tp + 1]) / (half * tp)
        tall = jnp.concatenate([lax.rsqrt(total + EPS), jnp.zeros((rows - 8, rows), F32)], axis=0)
        return tall.T[:, :1]

    for copy in small:
        copy.wait()
    squares_wait(tp - 1, 0)
    scale = scale_of(s)
    loads[9].wait()
    low = jnp.zeros((rank, rows), F32)
    for i in range(per_half):
        cols = slice(i * width, (i + 1) * width)
        shaped = (x[:, cols].astype(F32) * scale * gain[t, :, cols]).astype(BF)
        low += columns_dot(down[:, cols], shaped)
    fades = fade.shape[0]
    noted = note.shape[1]
    note[me] = jnp.concatenate(
        [low, fade[...], jnp.zeros((noted - rank - fades, rows), F32)], axis=0
    )

    def note_send(n):
        place, core = (0 if n < tp else last), lax.rem(t + n % tp, tp)
        ref = note.at[me]
        return remote(ref, ref, n_send, n_recv, sp=place, tp=core), (s != place) | (core != t)

    for n in range(2 * tp):
        send, away_from_here = note_send(n)

        @pl.when(away_from_here)
        def _():
            send.start()

    cut_rows = rows // CUTS
    pieces = [(i, slice(r * cut_rows, (r + 1) * cut_rows)) for i in range(mine + 1) for r in range(CUTS)]

    def step(way, b, n):
        i, cut = pieces[n]
        src = lin_own.at[b, 1 - way, i, cut] if i < mine else win_own.at[b, 1 - way, cut]
        dst = lin_in.at[way, b, i, cut] if i < mine else win_in.at[way, b, cut]
        return remote(
            src, dst, r_send.at[0 if i < mine else 1], r_recv.at[way, b, n], sp=jnp.clip(s + 1 - 2 * way, 0, last)
        )

    def relay(way, b, n):
        i, cut = pieces[n]
        step(way, b, n).wait_recv()
        if i < mine:
            lin_own[b, 1 - way, i, cut] = (
                lin_own[b, 1 - way, i, cut].astype(F32) + lin_in[way, b, i, cut].astype(F32)
            ).astype(BF)
        else:
            win_own[b, 1 - way, cut] = (
                win_own[b, 1 - way, cut].astype(F32) + win_in[way, b, cut].astype(F32)
            ).astype(BF)
        step(way, b, n).start()

    for i in range(6):
        loads[i].wait()
    qw, kw = lane_of[0], lane_of[1]
    gain_here = gain[lax.div(s, per_half), :, pl.ds(pl.multiple_of(lax.rem(s, per_half) * width, width), width)]

    def send_sums(b):
        for n in range(len(pieces)):
            step(e, b, n).start()

    def project(k, carry):
        turned = lax.rem(s + k, sp)
        b = jnp.where(inside & (k > 1), jnp.where(k == 2, 0, sp + 1 - 2 * s), turned)

        @pl.when(inside & (k == last))
        def _():
            for n in range(EARLY):
                relay(e, 0, n)

        @pl.when(jnp.logical_or(jnp.logical_not(home), b != s))
        def _():
            forward(b).wait_recv()

        @pl.when(jnp.logical_and(home, b != s))
        def _():
            forward(b).start()

        @pl.when(jnp.logical_and(home, b == s))
        def _():
            keep(0).wait()

        @pl.when(k == 1)
        def _():
            squares_wait((sp - 1) * tp, 1)

        for i in reversed(range(per_half)):

            @pl.when((b == 0) & (s > 1) & (t * per_half + i > s))
            def _():
                slice_send(i).start()

        block = (blocks[b].astype(F32) * scale_of(b) * gain_here).astype(BF)

        def part(i, h):
            w = lane_of[i]
            return dot(block, weights[i][:, pl.ds(pl.multiple_of(h * w, w), w)]).astype(BF)

        for n in range(2):
            h = e if n else 1 - e
            query, key, value = part(3, h), part(4, h), part(5, h)
            for i in range(mine):
                lin_own[b, h, i, :, :lk] = query[:, i * lk : (i + 1) * lk]
                lin_own[b, h, i, :, lk : 2 * lk] = key[:, i * lk : (i + 1) * lk]
                lin_own[b, h, i, :, 2 * lk :] = value[:, i * DV : (i + 1) * DV]
            if n == 0:

                @pl.when((s == 0) & (t > 0) & (k == 0))
                def _():
                    slice_send(per_half - 1).wait_send()
                    pl.semaphore_signal(turn, inc=1, device_id={"tp": other}, device_id_type=MESH)

                @pl.when((s == 0) & (t == 0) & (k == 0))
                def _():
                    pl.semaphore_wait(turn, 1)
                    for i in range(1, per_half):
                        slice_send(i).start()

                for i in reversed(range(per_half)):

                    @pl.when((k == 0) & (s == 1) & (t * per_half + i > s))
                    def _():
                        slice_send(i).start()

                @pl.when(at_end & (k >= e))
                def _():
                    for m in range(mine * CUTS):
                        step(e, b, m).start()

            win_own[b, h, :, :qw] = part(0, h)
            win_own[b, h, :, qw : qw + kw] = part(1, h)
            win_own[b, h, :, qw + kw :] = part(2, h)
            if n == 0:

                @pl.when(at_end & (k >= e))
                def _():
                    for m in range(mine * CUTS, len(pieces)):
                        step(e, b, m).start()

        return carry

    lax.fori_loop(0, sp, project, 0)

    @pl.when(s == last)
    def _():
        send_sums(last)

    def gather(way, b, n):
        i, r = divmod(n, CUTS)
        ref = (held_n if i else held_g).at[b, way, slice(r * cut_rows, (r + 1) * cut_rows)]
        return remote(
            ref, ref, g_send.at[i], g_recv.at[way, b, n], sp=jnp.clip(s + 1 - 2 * way, 0, last)
        )

    part_rows = rows // tp
    cols_g, cols_n = held_g.shape[3], held_n.shape[3]

    def swap(b):
        return remote(term.at[b, other], away.at[b], t_send.at[b], t_recv.at[b], tp=other)

    columns = term.shape[3]

    def place_of(src):
        return pl.ds(pl.multiple_of(src * columns, columns), columns)

    def deliver(b):
        return remote(term.at[b, t], out.at[:, place_of(s)], o_send, o_recv, sp=b)

    def close(b):
        swap(b).wait()
        term[b, t] = (term[b, t].astype(F32) + away[b].astype(F32)).astype(BF)

        @pl.when(s != b)
        def _():
            deliver(b).start()

        @pl.when(s == b)
        def _():
            out[:, b * columns : (b + 1) * columns] = term[b, t]

    def multiply(b):
        total = None
        for src in range(2):
            piece = dot(held_g[b, src], weights[7][src * cols_g : (src + 1) * cols_g]) + dot(
                held_n[b, src], weights[6][src * cols_n : (src + 1) * cols_n]
            )
            total = piece if total is None else total + piece
        for h in range(tp):
            term[b, h] = total[h * part_rows : (h + 1) * part_rows].astype(BF)
        swap(b).start()

    def pass_on(way, b, i):
        gather(way, b, i).wait_recv()
        gather(way, b, i).start()

    @pl.when(inside)
    def _():
        loads[8].wait()
        items = [(relay, b, i) for b in range(sp) for i in range(len(pieces))]
        items += [(pass_on, b, i) for b in range(sp) for i in range(2 * CUTS)]
        for n in range(len(items) + LAG):
            if EARLY <= n < len(items):
                what, b, i = items[n]
                what(e, b, i)
            if n >= LAG:
                what, b, i = items[n - LAG]
                what(1 - e, b, i)
                if what is pass_on and i == 2 * CUTS - 1:
                    if b == 0:
                        loads[6].wait()
                        loads[7].wait()
                    if b == last:
                        for c in range(1, last):
                            close(c)
                    multiply(b)
        close(last)
        close(0)

    @pl.when(at_end)
    def _():
        loads[8].wait()
        others = note.at[pl.ds(0, sp * tp - 1)]
        remote(others, others, n_send, n_recv, tp=other).wait_recv()
        span = mine * lk
        lane = pl.ds(pl.multiple_of(e * span, span), span)
        up_own = jnp.concatenate([up[:, lane], jnp.zeros((rows - rank, span), BF)], axis=0)
        bias_own = bias[:, lane]
        row_at = lax.broadcasted_iota(jnp.int32, (rows, rows), 0)
        col_at = lax.broadcasted_iota(jnp.int32, (rows, rows), 1)
        span_low = jnp.logical_and(row_at >= col_at, row_at // SPAN == col_at // SPAN)
        ones_low = jnp.where(span_low, 1.0, 0.0).astype(BF)
        query_at = lax.broadcasted_iota(jnp.int32, (rows, 2 * rows), 0)
        key_at = lax.broadcasted_iota(jnp.int32, (rows, 2 * rows), 1)
        distance = query_at - key_at + rows
        near_by = jnp.logical_and(distance >= 0, distance < WINDOW)
        far = distance.astype(F32)
        heads = qw // HD // mine

        def linear(b, states):
            rank_rows = note[b * tp, :rank] + note[b * tp + 1, :rank]
            tall = jnp.concatenate(
                [rank_rows, note[b * tp + t, rank:], jnp.zeros((rows - noted, rows), F32)], axis=0
            ).T
            energies = dot(tall.astype(BF), up_own) + bias_own
            soft = jnp.minimum(energies, 0.0) - jnp.log1p(jnp.exp(-jnp.abs(energies)))
            soft = soft / FADING_SOFTNESS
            fading = []
            for i in range(mine):
                extra = jnp.sum(
                    jnp.where(col_at == rank + e * mine + i, tall, 0.0), axis=1, keepdims=True
                )
                fading.append(soft[:, i * lk : (i + 1) * lk] + extra)
            fading = jnp.concatenate(fading, axis=1)
            top = fading.astype(BF)
            rest = fading - top.astype(F32)
            middle = rest.astype(BF)
            bottom = (rest - middle.astype(F32)).astype(BF)
            summed = dot(ones_low, jnp.concatenate([top, middle, bottom], axis=1))
            running_all = summed[:, :span] + (summed[:, span : 2 * span] + summed[:, 2 * span :])
            new_states = []
            for i in range(mine):
                for r in range(CUTS):
                    step(1 - e, b, i * CUTS + r).wait_recv()
                here = (lin_own[b, e, i].astype(F32) + lin_in[1 - e, b, i].astype(F32)).astype(BF)
                running = running_all[:, i * lk : (i + 1) * lk]
                state = states[i]
                query = here[:, :lk].astype(F32) * lk ** (-0.5)
                key = here[:, lk : 2 * lk].astype(F32)
                value = here[:, 2 * lk :]
                decayed = (query * jnp.exp(running)).astype(BF)
                inner = columns_dot(decayed, (key * jnp.exp(-running)).astype(BF))
                inner = jnp.where(span_low, inner, 0.0).astype(BF)
                within = dot(inner, value)
                carried = []
                for j in range(rows // SPAN):
                    cut = slice(j * SPAN, (j + 1) * SPAN)
                    end = running[(j + 1) * SPAN - 1 : (j + 1) * SPAN]
                    ending = (key[cut] * jnp.exp(end - running[cut])).astype(BF)
                    carried.append(columns_dot(decayed[cut], state.astype(BF)))
                    state = state * jnp.exp(end) + lax.dot_general(
                        value[cut], ending, (((0,), (0,)), ((), ())), preferred_element_type=F32
                    )
                flat = within + jnp.concatenate(carried, axis=0)
                normal = (
                    flat
                    * lax.rsqrt(jnp.mean(flat * flat, axis=-1, keepdims=True) + EPS)
                    * head_gain[...]
                )
                held_g[b, e, :, i * DV : (i + 1) * DV] = normal.astype(BF)
                new_states.append(state)
            for r in range(CUTS):
                gather(e, b, r).start()
            return new_states

        def window(b):
            for r in range(CUTS):
                step(1 - e, b, mine * CUTS + r).wait_recv()
            win_own[b, e] = (win_own[b, e].astype(F32) + win_in[1 - e, b].astype(F32)).astype(BF)
            present = win_own[b, e]
            earlier = win_own[max(b - 1, 0), e]
            allowed = near_by if b else jnp.logical_and(near_by, key_at >= rows)
            for g in range(mine):
                ka, va = qw + g * HD, qw + kw + g * HD
                keys = jnp.concatenate([earlier[:, ka : ka + HD], present[:, ka : ka + HD]], axis=0)
                vals = jnp.concatenate([earlier[:, va : va + HD], present[:, va : va + HD]], axis=0)
                results = []
                for h in range(heads):
                    local = (e * mine + g) * heads + h
                    number = (t * (2 * mine * heads) + local + 1).astype(F32)
                    slope = jnp.exp2(jnp.full((rows, 1), -8.0 / QH, F32) * number)
                    at = (g * heads + h) * HD
                    score = (
                        columns_dot(present[:, at : at + HD], keys) * HD ** (-0.5) - slope * far
                    )
                    weight = jnp.where(allowed, jnp.exp(score), 0.0)
                    floor = jnp.exp(jnp.full((rows, 1), sink[local], F32))
                    probs = (weight / (jnp.sum(weight, axis=1, keepdims=True) + floor)).astype(BF)
                    results.append(dot(probs, vals))
                wide_to = heads * HD
                held_n[b, e, :, g * wide_to : (g + 1) * wide_to] = jnp.concatenate(
                    results, axis=1
                ).astype(BF)
            for r in range(CUTS):
                gather(e, b, CUTS + r).start()

        def collect(b):
            for i in range(2 * CUTS):
                gather(1 - e, b, i).wait_recv()

        states = [start[i].T for i in range(mine)]
        for b in range(sp):
            states = linear(b, states)
            window(b)
        loads[6].wait()
        loads[7].wait()
        for b in range(sp):
            collect(b)
            multiply(b)
            if b == last - 1:
                for c in (*range(1, last), 0):
                    close(c)
        close(last)

    def drain(ref, sem):
        remote(ref, ref, sem, l_sem, tp=other).wait_send()

    sent = ((lin_own, r_send.at[0]), (win_own, r_send.at[1]), (held_g, g_send.at[0]), (held_n, g_send.at[1]))

    @pl.when(inside)
    def _():
        for ref, sem in sent:
            drain(ref, sem)
        drain(note.at[pl.ds(0, 2 * tp)], n_send)

    @pl.when(at_end)
    def _():
        for ref, sem in sent:
            drain(ref.at[:, 0], sem)
        drain(note.at[pl.ds(0, 2 * tp - 1)], n_send)

    @pl.when(home)
    def _():
        drain(blocks, f_send)

    for i in range(per_half):

        @pl.when((t * per_half + i != s) & ((s > 0) | (t == 0) | (i < per_half - 1)))
        def _():
            slice_send(i).wait_send()

    drain(squares.at[pl.ds(0, sp * tp - 1)], sq_send)
    drain(term.at[pl.ds(0, last), 0], o_send)
    others = out.at[:, pl.ds(0, last * columns)]
    remote(others, others, o_send, o_recv, tp=other).wait_recv()


def stationary(
    activations,
    input_norm_gain,
    window_query_weight,
    window_key_weight,
    window_value_weight,
    linear_query_weight,
    linear_key_weight,
    linear_value_weight,
    decay_down_factor,
    decay_up_factor,
    decay_offset_bias,
    extra_fading_exponent,
    starting_state,
    head_sink_logit,
    linear_head_gain,
    window_output_weight,
    linear_output_weight,
):
    sp, tp = lax.axis_size("sp"), lax.axis_size("tp")
    rows, half = activations.shape
    matrices = (
        window_query_weight,
        window_key_weight,
        window_value_weight,
        linear_query_weight,
        linear_key_weight,
        linear_value_weight,
        window_output_weight,
        linear_output_weight,
    )
    rank = decay_down_factor.shape[1]
    heads_tp = extra_fading_exponent.shape[1]
    mine = heads_tp // 2
    noted = rank + heads_tp + -(rank + heads_tp) % 8
    columns = window_output_weight.shape[1]
    small = (
        input_norm_gain.reshape(tp, 1, half),
        decay_offset_bias.reshape(1, -1),
        head_sink_logit,
        linear_head_gain.reshape(1, -1),
        decay_up_factor,
        extra_fading_exponent.T,
    )
    vmem = pl.BlockSpec(memory_space=pltpu.VMEM)
    hbm = pl.BlockSpec(memory_space=pltpu.HBM)
    dma = pltpu.SemaphoreType.DMA
    slice_width = half * tp // sp
    lin_cols = sum(m.shape[1] for m in matrices[3:6]) // heads_tp
    win_cols = sum(m.shape[1] for m in matrices[:3]) // 2
    return pl.pallas_call(
        functools.partial(mixer_kernel, sp, tp),
        out_shape=pltpu.VMEM((rows // tp, columns * sp), BF),
        in_specs=[hbm] * 17,
        out_specs=vmem,
        scratch_shapes=[pltpu.VMEM(m.shape, BF) for m in matrices]
        + [
            pltpu.VMEM((mine,) + starting_state.shape[1:], F32),
            pltpu.VMEM((rank, half), BF),
            pltpu.VMEM((rows, half), BF),
            pltpu.VMEM((sp * tp, 8, rows), F32),
            pltpu.VMEM((sp, rows, slice_width), BF),
            pltpu.VMEM((sp * tp, noted, rows), F32),
            pltpu.VMEM((sp, tp, rows // tp, columns), BF),
            pltpu.VMEM((sp, rows // tp, columns), BF),
            pltpu.VMEM((sp, 2, mine, rows, lin_cols), BF),
            pltpu.VMEM((sp, 2, rows, win_cols), BF),
            pltpu.VMEM((2, sp, mine, rows, lin_cols), BF),
            pltpu.VMEM((2, sp, rows, win_cols), BF),
            pltpu.VMEM((sp, 2, rows, linear_output_weight.shape[0] // 2), BF),
            pltpu.VMEM((sp, 2, rows, window_output_weight.shape[0] // 2), BF),
            dma((11,)),
            dma,
            dma((2,)),
            dma((sp // tp,)),
            dma((sp,)),
            dma,
            dma,
            dma,
            dma,
            dma((2,)),
            dma((2, sp, (mine + 1) * CUTS)),
            dma((2,)),
            dma((2, sp, 2 * CUTS)),
            dma((sp,)),
            dma((sp,)),
            dma,
            dma,
            pltpu.SemaphoreType.REGULAR,
            dma((len(small),)),
        ]
        + [
            (pltpu.SMEM if a.ndim == 1 else pltpu.VMEM)(a.shape, a.dtype) for a in small
        ],
        compiler_params=pltpu.CompilerParams(
            collective_id=0, has_side_effects=True, vmem_limit_bytes=56 * 2**20
        ),
    )(
        *small,
        *matrices,
        starting_state,
        decay_down_factor.T,
        activations,
    )


def mixer(*arrays):
    sp, tp = lax.axis_size("sp"), lax.axis_size("tp")
    rows = arrays[0].shape[0]
    one_each = KVH == GATED_MIXERS == sp * tp and QH % KVH == 0
    if tp == 2 and sp == 2 * tp and one_each and rows == WINDOW and rows % SPAN == 0:
        return stationary(*arrays)
    return local(*arrays)


def solution(mesh):
    placed = (
        P(("fs", "sp"), "tp"),
        P(),
        P("sp", "tp"),
        P("sp", "tp"),
        P("sp", "tp"),
        P("sp", "tp"),
        P("sp", "tp"),
        P("sp", "tp"),
        P(),
        P(None, "tp"),
        P("tp"),
        P(("fs", "sp"), "tp"),
        P("tp", None, None),
        P("tp"),
        P(),
        P("tp", "sp"),
        P("tp", "sp"),
    )
    return jax.shard_map(
        mixer, mesh=mesh, in_specs=placed, out_specs=P(("fs", "sp", "tp"), None), check_vma=False
    )
```

```python
import functools

import jax
import jax.numpy as jnp
from jax import lax
from jax.experimental import pallas as pl
from jax.experimental.pallas import tpu as pltpu
from jax.sharding import PartitionSpec as P

QH = 32
HD = 64
WINDOW = 128
LOOKUP_FEATURES = 128
DV = 256
SPAN = 64
KVH = 8
GATED_MIXERS = 8


EPS = 1e-05
FADING_SOFTNESS = 16.0
HIGH_PRECISION = lax.Precision.HIGHEST


def passed_along(value, axis, steps):
    count = lax.axis_size(axis)
    leading, last = (max(0, -steps), min(count, count - steps))
    return lax.ppermute(value, axis, [(source, source + steps) for source in range(leading, last)])


def prefix(x, axis, combine, identity):
    peers, place = (lax.axis_size(axis), lax.axis_index(axis))
    everything = jax.tree.map(
        lambda part, kind: lax.all_gather(part.astype(kind), axis), x, (jnp.bfloat16, jnp.bfloat16)
    )
    start = jax.tree.map(
        lambda part, zero: jnp.broadcast_to(jnp.asarray(zero, part.dtype), part.shape), x, identity
    )

    def hop(k, before):
        reached = k < place
        new = combine(
            before, jax.tree.map(lambda part, own: part[k].astype(own.dtype), everything, x)
        )
        return jax.tree.map(lambda a, b: jnp.where(reached, a, b), new, before)

    return lax.fori_loop(0, peers, hop, start)


def window_attention(near_query, near_keys, near_values, head_sink_logit):
    stream_extent = near_query.shape[0]
    key_heads = near_keys.shape[1] // HD
    heads_here = near_query.shape[1] // HD
    groups = heads_here // key_heads
    blocks = stream_extent // WINDOW
    tail_rows = jnp.stack([near_keys, near_values])
    before = passed_along(tail_rows, "sp", 1)

    def banded(previous, current):
        extended = jnp.concatenate([previous, current], axis=0)
        earlier = extended[:stream_extent].reshape(blocks, WINDOW, key_heads, HD)
        present = extended[WINDOW:].reshape(blocks, WINDOW, key_heads, HD)
        return jnp.concatenate([earlier, present], axis=1)

    key_band = banded(before[0], near_keys)
    value_band = banded(before[1], near_values)
    queries = near_query.reshape(blocks, WINDOW, key_heads, groups, HD)
    scores = jnp.einsum(
        "nqhgd,nkhd->hgnqk", queries, key_band, preferred_element_type=jnp.float32
    ) * HD ** (-0.5)
    head_ids = lax.axis_index("tp") * heads_here + jnp.arange(heads_here, dtype=jnp.int32)
    slopes = jnp.exp2(-8.0 * (head_ids + 1).astype(jnp.float32) / QH).reshape(key_heads, groups)
    query_pos = jnp.arange(WINDOW, dtype=jnp.int32)
    key_pos = jnp.arange(2 * WINDOW, dtype=jnp.int32)
    distance = query_pos[:, None] - key_pos[None, :] + WINDOW
    start_pos = (
        lax.axis_index("sp") * stream_extent + (jnp.arange(blocks, dtype=jnp.int32) - 1) * WINDOW
    )
    absolute = start_pos[:, None] + key_pos[None, :]
    allowed = ((distance >= 0) & (distance < WINDOW))[None] & (absolute >= 0)[:, None, :]
    biased = scores - slopes[:, :, None, None, None] * distance.astype(jnp.float32)
    weights = jnp.where(allowed, jnp.exp(biased), 0.0)
    denominator = (
        jnp.sum(weights, axis=-1, keepdims=True)
        + jnp.exp(head_sink_logit.reshape(key_heads, groups))[:, :, None, None, None]
    )
    attention = (weights / denominator).astype(jnp.bfloat16)
    attended = jnp.einsum(
        "hgnqk,nkhd->nqhgd", attention, value_band, preferred_element_type=jnp.float32
    )
    return attended.reshape(stream_extent, heads_here * HD).astype(jnp.bfloat16)


def linear_attention(
    gated_query, gated_keys, gated_values, fading_exponent, linear_head_gain, starting_state
):
    stream_extent = gated_query.shape[0]
    head_total = gated_query.shape[1] // LOOKUP_FEATURES
    span_count = stream_extent // SPAN
    scaled_query = gated_query.astype(jnp.float32).reshape(
        span_count, SPAN, head_total, LOOKUP_FEATURES
    ) * LOOKUP_FEATURES ** (-0.5)
    keys_wide = gated_keys.astype(jnp.float32).reshape(
        span_count, SPAN, head_total, LOOKUP_FEATURES
    )
    values_wide = gated_values.astype(jnp.float32).reshape(span_count, SPAN, head_total, DV)
    running = jnp.cumsum(
        fading_exponent.reshape(span_count, SPAN, head_total, LOOKUP_FEATURES), axis=1
    )
    span_end = running[:, -1]
    query_with_decay = scaled_query * jnp.exp(running)
    inverse_keys = keys_wide * jnp.exp(-running)
    ending_keys = keys_wide * jnp.exp(span_end[:, None] - running)
    inner = jnp.einsum("nchk,nshk->nhcs", query_with_decay, inverse_keys, precision=HIGH_PRECISION)
    lower = jnp.tril(jnp.ones((SPAN, SPAN), dtype=bool))
    inner = jnp.where(lower, inner, 0.0)
    within = jnp.einsum("nhcs,nshv->nchv", inner, values_wide, precision=HIGH_PRECISION)

    def advance(running_state, inputs):
        query_portion, key_portion, value_portion, scale_factor = inputs
        layer_output = jnp.einsum(
            "fmy,mys->fms", query_portion, running_state, precision=HIGH_PRECISION
        )
        running_state = running_state * scale_factor[..., None] + jnp.einsum(
            "gxp,gxz->xpz", key_portion, value_portion, precision=HIGH_PRECISION
        )
        return (running_state, layer_output)

    start_state = jnp.zeros((head_total, LOOKUP_FEATURES, DV), jnp.float32)
    state_end, carried = lax.scan(
        advance, start_state, (query_with_decay, ending_keys, values_wide, jnp.exp(span_end))
    )
    device_decay = jnp.exp(jnp.sum(span_end, axis=0))
    prefix_sums = jnp.cumsum(span_end, axis=0) - span_end

    def combine(earlier, later):
        return (earlier[0] * later[0], later[0][..., None] * earlier[1] + later[1])

    decay_before, state_before = prefix(
        (device_decay, state_end),
        "sp",
        combine,
        (jnp.ones_like(device_decay), jnp.zeros_like(state_end)),
    )
    incoming_rows = state_before + decay_before[..., None] * starting_state
    crossing = jnp.einsum(
        "qwso,soz->qwsz",
        query_with_decay * jnp.exp(prefix_sums)[:, None],
        incoming_rows,
        precision=HIGH_PRECISION,
    )
    flat = (within + carried + crossing).reshape(stream_extent, head_total, DV)
    normal = (
        flat * lax.rsqrt(jnp.mean(flat * flat, axis=-1, keepdims=True) + EPS) * linear_head_gain
    )
    return normal.reshape(stream_extent, head_total * DV).astype(jnp.bfloat16)


def local(
    activations,
    input_norm_gain,
    window_query_weight,
    window_key_weight,
    window_value_weight,
    linear_query_weight,
    linear_key_weight,
    linear_value_weight,
    decay_down_factor,
    decay_up_factor,
    decay_offset_bias,
    extra_fading_exponent,
    starting_state,
    head_sink_logit,
    linear_head_gain,
    window_output_weight,
    linear_output_weight,
):
    gathered = lax.all_gather(activations, "tp", axis=1, tiled=True)
    widened = gathered.astype(jnp.float32)
    normed = (
        widened
        * lax.rsqrt(jnp.mean(widened * widened, axis=1, keepdims=True) + EPS)
        * input_norm_gain
    ).astype(jnp.bfloat16)
    row_total = normed.shape[0]
    matrices = (
        window_query_weight,
        window_key_weight,
        window_value_weight,
        linear_query_weight,
        linear_key_weight,
        linear_value_weight,
    )
    segments = (
        lax.all_gather(matrices[0], "sp", axis=0, tiled=True),
        lax.all_gather(matrices[1], "sp", axis=0, tiled=True),
        lax.all_gather(matrices[2], "sp", axis=0, tiled=True),
        lax.all_gather(matrices[3], "sp", axis=0, tiled=True),
        lax.all_gather(matrices[4], "sp", axis=0, tiled=True),
        lax.all_gather(matrices[5], "sp", axis=0, tiled=True),
    )
    projected = tuple(
        (jnp.dot(normed, segment, preferred_element_type=jnp.float32) for segment in segments)
    )
    near_query, near_keys, near_values, gated_query, gated_keys, gated_values = [
        product.astype(jnp.bfloat16) for product in projected
    ]
    low_rank = jnp.dot(normed, decay_down_factor, preferred_element_type=jnp.float32).astype(
        jnp.bfloat16
    )
    attention_energies = (
        jnp.dot(low_rank, decay_up_factor, preferred_element_type=jnp.float32) + decay_offset_bias
    )
    head_total = extra_fading_exponent.shape[1]
    fading_exponent = (jax.nn.log_sigmoid(attention_energies) / FADING_SOFTNESS).reshape(
        row_total, head_total, LOOKUP_FEATURES
    ) + extra_fading_exponent[:, :, None]
    near_out = window_attention(near_query, near_keys, near_values, head_sink_logit)
    gated_out = linear_attention(
        gated_query, gated_keys, gated_values, fading_exponent, linear_head_gain, starting_state
    )
    window_full, linear_full = (
        lax.all_gather(window_output_weight, "sp", axis=1, tiled=True),
        lax.all_gather(linear_output_weight, "sp", axis=1, tiled=True),
    )
    return lax.psum_scatter(
        (
            jnp.dot(near_out, window_full, preferred_element_type=jnp.float32)
            + jnp.dot(gated_out, linear_full, preferred_element_type=jnp.float32)
        ).astype(jnp.bfloat16),
        "tp",
        scatter_dimension=0,
        tiled=True,
    )


MESH = pl.DeviceIdType.MESH
BF = jnp.bfloat16
F32 = jnp.float32
LAG = 2
CUTS = 2
EARLY = 3


def dot(a, b):
    return jnp.dot(a, b, preferred_element_type=F32)


def remote(src, dst, send_sem, recv_sem, **where):
    return pltpu.make_async_remote_copy(
        src_ref=src,
        dst_ref=dst,
        send_sem=send_sem,
        recv_sem=recv_sem,
        device_id=where,
        device_id_type=MESH,
    )


def greet(sp, tp):
    s, t = lax.axis_index("sp"), lax.axis_index("tp")
    barrier = pltpu.get_barrier_semaphore()
    for ds in range(sp):
        for dt in range(tp):
            if ds or dt:
                where = {"sp": lax.rem(s + ds, sp), "tp": lax.rem(t + dt, tp)}
                pl.semaphore_signal(barrier, inc=1, device_id=where, device_id_type=MESH)


def greeted(sp, tp):
    pl.semaphore_wait(pltpu.get_barrier_semaphore(), sp * tp - 1)


def columns_dot(a, b):
    return lax.dot_general(a, b, (((1,), (1,)), ((), ())), preferred_element_type=F32)


def mixer_kernel(sp, tp, *refs):
    small_in, sources, state_in, down_in, x_in = refs[:6], refs[6:14], refs[14], refs[15], refs[16]
    out = refs[17]
    weights, start, down, x = refs[18:26], refs[26], refs[27], refs[28]
    gain, bias, sink, head_gain, up, fade = refs[58:64]
    squares, blocks, note, term, away = refs[29:34]
    lin_own, win_own, lin_in, win_in, held_g, held_n = refs[34:40]
    w_sem, sq_send, sq_recv, a_send, a_recv, f_send, l_sem, n_send, n_recv = refs[40:49]
    r_send, r_recv, g_send, g_recv, t_send, t_recv, o_send, o_recv, s_sem = refs[49:58]
    s, t = lax.axis_index("sp"), lax.axis_index("tp")
    other = 1 - t
    last = sp - 1
    e = jnp.where(s >= sp // 2, 1, 0)
    at_end = jnp.logical_or(s == 0, s == last)
    inside = jnp.logical_not(at_end)
    per_half = sp // tp
    rows, half = x.shape
    width = half // per_half
    rank = down.shape[0]
    lk = LOOKUP_FEATURES
    mine = lin_own.shape[2]
    lane_of = {i: weights[i].shape[1] // 2 for i in range(6)}
    greet(sp, tp)
    loads = [
        pltpu.make_async_copy(a, b, w_sem.at[i]) for i, (a, b) in enumerate(zip(sources, weights))
    ]
    loads.append(pltpu.make_async_copy(state_in.at[pl.ds(e * mine, mine)], start, w_sem.at[8]))
    loads.append(
        pltpu.make_async_copy(
            down_in.at[:, pl.ds(pl.multiple_of(t * half, half), half)], down, w_sem.at[9]
        )
    )
    loads.append(pltpu.make_async_copy(x_in, x, w_sem.at[10]))
    small = [
        pltpu.make_async_copy(a, b, s_sem.at[i]) for i, (a, b) in enumerate(zip(small_in, refs[58:64]))
    ]
    loads[10].start()
    for copy in small:
        copy.start()
    for i in (9, 3, 4, 5, 0, 1, 2, 8, 6, 7):
        loads[i].start()
    home = lax.div(s, per_half) == t

    def slice_send(i):
        src = x.at[:, i * width : (i + 1) * width]
        return remote(src, blocks.at[s], a_send.at[i], a_recv.at[s], sp=t * per_half + i)

    def forward(b):
        return remote(blocks.at[b], blocks.at[b], f_send, a_recv.at[b], tp=other)

    me = s * tp + t

    def squares_send(n):
        where = {"sp": lax.rem(s + n // tp, sp), "tp": lax.rem(t + n % tp, tp)}
        ref = squares.at[me]
        return remote(ref, ref, sq_send, sq_recv.at[0 if n // tp == 0 else 1], **where)

    def keep(i):
        return pltpu.make_async_copy(x.at[:, i * width : (i + 1) * width], blocks.at[s], l_sem)

    def share(i):
        src = x.at[:, i * width : (i + 1) * width]
        return remote(src, blocks.at[s], f_send, a_recv.at[s], tp=other)

    loads[10].wait()
    wide = x[...].astype(F32)
    own = jnp.sum(wide * wide, axis=1, keepdims=True)
    squares[me] = jnp.broadcast_to(own, (rows, rows)).T[:8]
    greeted(sp, tp)
    for n in range(1, sp * tp):
        squares_send(n).start()
    for i in reversed(range(per_half)):
        j = t * per_half + i

        @pl.when((j < s) | ((j > s) & (s == 0) & (t > 0)))
        def _():
            slice_send(i).start()

        @pl.when(j == s)
        def _():
            share(i).start()
            keep(i).start()

    def squares_wait(n, k):
        ref = squares.at[pl.ds(0, n)]
        remote(ref, ref, sq_send, sq_recv.at[k], tp=other).wait_recv()

    def scale_of(b):
        total = (squares[b * tp] + squares[b * tp + 1]) / (half * tp)
        tall = jnp.concatenate([lax.rsqrt(total + EPS), jnp.zeros((rows - 8, rows), F32)], axis=0)
        return tall.T[:, :1]

    for copy in small:
        copy.wait()
    squares_wait(tp - 1, 0)
    scale = scale_of(s)
    loads[9].wait()
    low = jnp.zeros((rank, rows), F32)
    for i in range(per_half):
        cols = slice(i * width, (i + 1) * width)
        shaped = (x[:, cols].astype(F32) * scale * gain[t, :, cols]).astype(BF)
        low += columns_dot(down[:, cols], shaped)
    fades = fade.shape[0]
    noted = note.shape[1]
    note[me] = jnp.concatenate(
        [low, fade[...], jnp.zeros((noted - rank - fades, rows), F32)], axis=0
    )

    def note_send(n):
        place, core = (0 if n < tp else last), lax.rem(t + n % tp, tp)
        ref = note.at[me]
        return remote(ref, ref, n_send, n_recv, sp=place, tp=core), (s != place) | (core != t)

    cut_rows = rows // CUTS
    pieces = [(i, slice(r * cut_rows, (r + 1) * cut_rows)) for i in range(mine + 1) for r in range(CUTS)]

    def step(way, b, n):
        i, cut = pieces[n]
        src = lin_own.at[b, 1 - way, i, cut] if i < mine else win_own.at[b, 1 - way, cut]
        dst = lin_in.at[way, b, i, cut] if i < mine else win_in.at[way, b, cut]
        return remote(
            src, dst, r_send.at[0 if i < mine else 1], r_recv.at[way, b, n], sp=jnp.clip(s + 1 - 2 * way, 0, last)
        )

    def relay(way, b, n):
        i, cut = pieces[n]
        step(way, b, n).wait_recv()
        if i < mine:
            lin_own[b, 1 - way, i, cut] = (
                lin_own[b, 1 - way, i, cut].astype(F32) + lin_in[way, b, i, cut].astype(F32)
            ).astype(BF)
        else:
            win_own[b, 1 - way, cut] = (
                win_own[b, 1 - way, cut].astype(F32) + win_in[way, b, cut].astype(F32)
            ).astype(BF)
        step(way, b, n).start()

    for i in range(6):
        loads[i].wait()
    qw, kw = lane_of[0], lane_of[1]
    gain_here = gain[lax.div(s, per_half), :, pl.ds(pl.multiple_of(lax.rem(s, per_half) * width, width), width)]

    def send_sums(b):
        for n in range(len(pieces)):
            step(e, b, n).start()

    def project(k, carry):
        turned = lax.rem(s + k, sp)
        b = jnp.where(inside & (k > 1), jnp.where(k == 2, 0, sp + 1 - 2 * s), turned)

        @pl.when(inside & (k == last))
        def _():
            for n in range(1, EARLY):
                relay(e, 0, n)

        @pl.when(jnp.logical_or(jnp.logical_not(home), b != s))
        def _():
            forward(b).wait_recv()

        @pl.when(jnp.logical_and(home, b != s))
        def _():
            forward(b).start()

        @pl.when(jnp.logical_and(home, b == s))
        def _():
            keep(0).wait()

        @pl.when(k == 1)
        def _():
            squares_wait((sp - 1) * tp, 1)

        for i in reversed(range(per_half)):

            @pl.when((b == 0) & (s > 1) & (t * per_half + i > s))
            def _():
                slice_send(i).start()

        block = (blocks[b].astype(F32) * scale_of(b) * gain_here).astype(BF)

        def part(i, h):
            w = lane_of[i]
            return dot(block, weights[i][:, pl.ds(pl.multiple_of(h * w, w), w)]).astype(BF)

        for n in range(2):
            h = e if n else 1 - e
            query, key, value = part(3, h), part(4, h), part(5, h)
            for i in range(mine):
                lin_own[b, h, i, :, :lk] = query[:, i * lk : (i + 1) * lk]
                lin_own[b, h, i, :, lk : 2 * lk] = key[:, i * lk : (i + 1) * lk]
                lin_own[b, h, i, :, 2 * lk :] = value[:, i * DV : (i + 1) * DV]
            if n == 0:

                @pl.when((s == 0) & (t == 0) & (k == 0))
                def _():
                    for i in range(1, per_half):
                        slice_send(i).start()

                for i in reversed(range(per_half)):

                    @pl.when((k == 0) & (s == 1) & (t * per_half + i > s))
                    def _():
                        slice_send(i).start()

                @pl.when(at_end & (k >= e))
                def _():
                    for m in range(mine * CUTS):
                        step(e, b, m).start()

            if n == 0:

                @pl.when(k == 0)
                def _():
                    for m in range(2 * tp):
                        send, away_from_here = note_send(m)

                        @pl.when(away_from_here)
                        def _():
                            send.start()

            win_own[b, h, :, :qw] = part(0, h)
            win_own[b, h, :, qw : qw + kw] = part(1, h)
            win_own[b, h, :, qw + kw :] = part(2, h)
            if n == 0:

                @pl.when(inside & (k == 2))
                def _():
                    relay(e, 0, 0)

                @pl.when(at_end & (k >= e))
                def _():
                    for m in range(mine * CUTS, len(pieces)):
                        step(e, b, m).start()

        return carry

    lax.fori_loop(0, sp, project, 0)

    @pl.when(s == last)
    def _():
        send_sums(last)

    def gather(way, b, n):
        i, r = divmod(n, CUTS)
        ref = (held_n if i else held_g).at[b, way, slice(r * cut_rows, (r + 1) * cut_rows)]
        return remote(
            ref, ref, g_send.at[i], g_recv.at[way, b, n], sp=jnp.clip(s + 1 - 2 * way, 0, last)
        )

    part_rows = rows // tp
    cols_g, cols_n = held_g.shape[3], held_n.shape[3]

    def swap(b):
        return remote(term.at[b, other], away.at[b], t_send.at[b], t_recv.at[b], tp=other)

    columns = term.shape[3]

    def place_of(src):
        return pl.ds(pl.multiple_of(src * columns, columns), columns)

    def deliver(b):
        return remote(term.at[b, t], out.at[:, place_of(s)], o_send, o_recv, sp=b)

    def close(b):
        swap(b).wait()
        term[b, t] = (term[b, t].astype(F32) + away[b].astype(F32)).astype(BF)

        @pl.when(s != b)
        def _():
            deliver(b).start()

        @pl.when(s == b)
        def _():
            out[:, b * columns : (b + 1) * columns] = term[b, t]

    def multiply(b):
        total = None
        for src in range(2):
            piece = dot(held_g[b, src], weights[7][src * cols_g : (src + 1) * cols_g]) + dot(
                held_n[b, src], weights[6][src * cols_n : (src + 1) * cols_n]
            )
            total = piece if total is None else total + piece
        for h in range(tp):
            term[b, h] = total[h * part_rows : (h + 1) * part_rows].astype(BF)
        swap(b).start()

    def pass_on(way, b, i):
        gather(way, b, i).wait_recv()
        gather(way, b, i).start()

    @pl.when(inside)
    def _():
        loads[8].wait()
        items = [(relay, b, i) for b in range(sp) for i in range(len(pieces))]
        items += [(pass_on, b, i) for b in range(sp) for i in range(2 * CUTS)]
        for n in range(len(items) + LAG):
            if EARLY <= n < len(items):
                what, b, i = items[n]
                what(e, b, i)
            if n >= LAG:
                what, b, i = items[n - LAG]
                what(1 - e, b, i)
                if what is pass_on and i == 2 * CUTS - 1:
                    if b == 0:
                        loads[6].wait()
                        loads[7].wait()
                    if b == last:
                        for c in range(1, last):
                            close(c)
                    multiply(b)
        close(last)
        close(0)

    @pl.when(at_end)
    def _():
        loads[8].wait()
        others = note.at[pl.ds(0, sp * tp - 1)]
        remote(others, others, n_send, n_recv, tp=other).wait_recv()
        span = mine * lk
        lane = pl.ds(pl.multiple_of(e * span, span), span)
        up_own = jnp.concatenate([up[:, lane], jnp.zeros((rows - rank, span), BF)], axis=0)
        bias_own = bias[:, lane]
        row_at = lax.broadcasted_iota(jnp.int32, (rows, rows), 0)
        col_at = lax.broadcasted_iota(jnp.int32, (rows, rows), 1)
        span_low = jnp.logical_and(row_at >= col_at, row_at // SPAN == col_at // SPAN)
        ones_low = jnp.where(span_low, 1.0, 0.0).astype(BF)
        query_at = lax.broadcasted_iota(jnp.int32, (rows, 2 * rows), 0)
        key_at = lax.broadcasted_iota(jnp.int32, (rows, 2 * rows), 1)
        distance = query_at - key_at + rows
        near_by = jnp.logical_and(distance >= 0, distance < WINDOW)
        far = distance.astype(F32)
        heads = qw // HD // mine

        def linear(b, states):
            rank_rows = note[b * tp, :rank] + note[b * tp + 1, :rank]
            tall = jnp.concatenate(
                [rank_rows, note[b * tp + t, rank:], jnp.zeros((rows - noted, rows), F32)], axis=0
            ).T
            energies = dot(tall.astype(BF), up_own) + bias_own
            soft = jnp.minimum(energies, 0.0) - jnp.log1p(jnp.exp(-jnp.abs(energies)))
            soft = soft / FADING_SOFTNESS
            fading = []
            for i in range(mine):
                extra = jnp.sum(
                    jnp.where(col_at == rank + e * mine + i, tall, 0.0), axis=1, keepdims=True
                )
                fading.append(soft[:, i * lk : (i + 1) * lk] + extra)
            fading = jnp.concatenate(fading, axis=1)
            top = fading.astype(BF)
            rest = fading - top.astype(F32)
            middle = rest.astype(BF)
            bottom = (rest - middle.astype(F32)).astype(BF)
            summed = dot(ones_low, jnp.concatenate([top, middle, bottom], axis=1))
            running_all = summed[:, :span] + (summed[:, span : 2 * span] + summed[:, 2 * span :])
            new_states = []
            for i in range(mine):
                for r in range(CUTS):
                    step(1 - e, b, i * CUTS + r).wait_recv()
                here = (lin_own[b, e, i].astype(F32) + lin_in[1 - e, b, i].astype(F32)).astype(BF)
                running = running_all[:, i * lk : (i + 1) * lk]
                state = states[i]
                query = here[:, :lk].astype(F32) * lk ** (-0.5)
                key = here[:, lk : 2 * lk].astype(F32)
                value = here[:, 2 * lk :]
                decayed = (query * jnp.exp(running)).astype(BF)
                inner = columns_dot(decayed, (key * jnp.exp(-running)).astype(BF))
                inner = jnp.where(span_low, inner, 0.0).astype(BF)
                within = dot(inner, value)
                carried = []
                for j in range(rows // SPAN):
                    cut = slice(j * SPAN, (j + 1) * SPAN)
                    end = running[(j + 1) * SPAN - 1 : (j + 1) * SPAN]
                    ending = (key[cut] * jnp.exp(end - running[cut])).astype(BF)
                    carried.append(columns_dot(decayed[cut], state.astype(BF)))
                    state = state * jnp.exp(end) + lax.dot_general(
                        value[cut], ending, (((0,), (0,)), ((), ())), preferred_element_type=F32
                    )
                flat = within + jnp.concatenate(carried, axis=0)
                normal = (
                    flat
                    * lax.rsqrt(jnp.mean(flat * flat, axis=-1, keepdims=True) + EPS)
                    * head_gain[...]
                )
                held_g[b, e, :, i * DV : (i + 1) * DV] = normal.astype(BF)
                new_states.append(state)
            for r in range(CUTS):
                gather(e, b, r).start()
            return new_states

        def window(b):
            for r in range(CUTS):
                step(1 - e, b, mine * CUTS + r).wait_recv()
            win_own[b, e] = (win_own[b, e].astype(F32) + win_in[1 - e, b].astype(F32)).astype(BF)
            present = win_own[b, e]
            earlier = win_own[max(b - 1, 0), e]
            allowed = near_by if b else jnp.logical_and(near_by, key_at >= rows)
            for g in range(mine):
                ka, va = qw + g * HD, qw + kw + g * HD
                keys = jnp.concatenate([earlier[:, ka : ka + HD], present[:, ka : ka + HD]], axis=0)
                vals = jnp.concatenate([earlier[:, va : va + HD], present[:, va : va + HD]], axis=0)
                results = []
                for h in range(heads):
                    local = (e * mine + g) * heads + h
                    number = (t * (2 * mine * heads) + local + 1).astype(F32)
                    slope = jnp.exp2(jnp.full((rows, 1), -8.0 / QH, F32) * number)
                    at = (g * heads + h) * HD
                    score = (
                        columns_dot(present[:, at : at + HD], keys) * HD ** (-0.5) - slope * far
                    )
                    weight = jnp.where(allowed, jnp.exp(score), 0.0)
                    floor = jnp.exp(jnp.full((rows, 1), sink[local], F32))
                    probs = (weight / (jnp.sum(weight, axis=1, keepdims=True) + floor)).astype(BF)
                    results.append(dot(probs, vals))
                wide_to = heads * HD
                held_n[b, e, :, g * wide_to : (g + 1) * wide_to] = jnp.concatenate(
                    results, axis=1
                ).astype(BF)
            for r in range(CUTS):
                gather(e, b, CUTS + r).start()

        def collect(b):
            for i in range(2 * CUTS):
                gather(1 - e, b, i).wait_recv()

        states = [start[i].T for i in range(mine)]
        for b in range(sp):
            states = linear(b, states)
            window(b)
        loads[6].wait()
        loads[7].wait()
        for b in range(sp):
            collect(b)
            multiply(b)
            if b == last - 1:
                for c in (*range(1, last), 0):
                    close(c)
        close(last)

    def drain(ref, sem):
        remote(ref, ref, sem, l_sem, tp=other).wait_send()

    sent = ((lin_own, r_send.at[0]), (win_own, r_send.at[1]), (held_g, g_send.at[0]), (held_n, g_send.at[1]))

    @pl.when(inside)
    def _():
        for ref, sem in sent:
            drain(ref, sem)
        drain(note.at[pl.ds(0, 2 * tp)], n_send)

    @pl.when(at_end)
    def _():
        for ref, sem in sent:
            drain(ref.at[:, 0], sem)
        drain(note.at[pl.ds(0, 2 * tp - 1)], n_send)

    @pl.when(home)
    def _():
        drain(blocks, f_send)

    for i in range(per_half):

        @pl.when(t * per_half + i != s)
        def _():
            slice_send(i).wait_send()

    drain(squares.at[pl.ds(0, sp * tp - 1)], sq_send)
    drain(term.at[pl.ds(0, last), 0], o_send)
    others = out.at[:, pl.ds(0, last * columns)]
    remote(others, others, o_send, o_recv, tp=other).wait_recv()


def stationary(
    activations,
    input_norm_gain,
    window_query_weight,
    window_key_weight,
    window_value_weight,
    linear_query_weight,
    linear_key_weight,
    linear_value_weight,
    decay_down_factor,
    decay_up_factor,
    decay_offset_bias,
    extra_fading_exponent,
    starting_state,
    head_sink_logit,
    linear_head_gain,
    window_output_weight,
    linear_output_weight,
):
    sp, tp = lax.axis_size("sp"), lax.axis_size("tp")
    rows, half = activations.shape
    matrices = (
        window_query_weight,
        window_key_weight,
        window_value_weight,
        linear_query_weight,
        linear_key_weight,
        linear_value_weight,
        window_output_weight,
        linear_output_weight,
    )
    rank = decay_down_factor.shape[1]
    heads_tp = extra_fading_exponent.shape[1]
    mine = heads_tp // 2
    noted = rank + heads_tp + -(rank + heads_tp) % 8
    columns = window_output_weight.shape[1]
    small = (
        input_norm_gain.reshape(tp, 1, half),
        decay_offset_bias.reshape(1, -1),
        head_sink_logit,
        linear_head_gain.reshape(1, -1),
        decay_up_factor,
        extra_fading_exponent.T,
    )
    vmem = pl.BlockSpec(memory_space=pltpu.VMEM)
    hbm = pl.BlockSpec(memory_space=pltpu.HBM)
    dma = pltpu.SemaphoreType.DMA
    slice_width = half * tp // sp
    lin_cols = sum(m.shape[1] for m in matrices[3:6]) // heads_tp
    win_cols = sum(m.shape[1] for m in matrices[:3]) // 2
    return pl.pallas_call(
        functools.partial(mixer_kernel, sp, tp),
        out_shape=pltpu.VMEM((rows // tp, columns * sp), BF),
        in_specs=[hbm] * 17,
        out_specs=vmem,
        scratch_shapes=[pltpu.VMEM(m.shape, BF) for m in matrices]
        + [
            pltpu.VMEM((mine,) + starting_state.shape[1:], F32),
            pltpu.VMEM((rank, half), BF),
            pltpu.VMEM((rows, half), BF),
            pltpu.VMEM((sp * tp, 8, rows), F32),
            pltpu.VMEM((sp, rows, slice_width), BF),
            pltpu.VMEM((sp * tp, noted, rows), F32),
            pltpu.VMEM((sp, tp, rows // tp, columns), BF),
            pltpu.VMEM((sp, rows // tp, columns), BF),
            pltpu.VMEM((sp, 2, mine, rows, lin_cols), BF),
            pltpu.VMEM((sp, 2, rows, win_cols), BF),
            pltpu.VMEM((2, sp, mine, rows, lin_cols), BF),
            pltpu.VMEM((2, sp, rows, win_cols), BF),
            pltpu.VMEM((sp, 2, rows, linear_output_weight.shape[0] // 2), BF),
            pltpu.VMEM((sp, 2, rows, window_output_weight.shape[0] // 2), BF),
            dma((11,)),
            dma,
            dma((2,)),
            dma((sp // tp,)),
            dma((sp,)),
            dma,
            dma,
            dma,
            dma,
            dma((2,)),
            dma((2, sp, (mine + 1) * CUTS)),
            dma((2,)),
            dma((2, sp, 2 * CUTS)),
            dma((sp,)),
            dma((sp,)),
            dma,
            dma,
            dma((len(small),)),
        ]
        + [
            (pltpu.SMEM if a.ndim == 1 else pltpu.VMEM)(a.shape, a.dtype) for a in small
        ],
        compiler_params=pltpu.CompilerParams(
            collective_id=0, has_side_effects=True, vmem_limit_bytes=56 * 2**20
        ),
    )(
        *small,
        *matrices,
        starting_state,
        decay_down_factor.T,
        activations,
    )


def mixer(*arrays):
    sp, tp = lax.axis_size("sp"), lax.axis_size("tp")
    rows = arrays[0].shape[0]
    one_each = KVH == GATED_MIXERS == sp * tp and QH % KVH == 0
    if tp == 2 and sp == 2 * tp and one_each and rows == WINDOW and rows % SPAN == 0:
        return stationary(*arrays)
    return local(*arrays)


def solution(mesh):
    placed = (
        P(("fs", "sp"), "tp"),
        P(),
        P("sp", "tp"),
        P("sp", "tp"),
        P("sp", "tp"),
        P("sp", "tp"),
        P("sp", "tp"),
        P("sp", "tp"),
        P(),
        P(None, "tp"),
        P("tp"),
        P(("fs", "sp"), "tp"),
        P("tp", None, None),
        P("tp"),
        P(),
        P("tp", "sp"),
        P("tp", "sp"),
    )
    return jax.shard_map(
        mixer, mesh=mesh, in_specs=placed, out_specs=P(("fs", "sp", "tp"), None), check_vma=False
    )
```

```python
import functools

import jax
import jax.numpy as jnp
from jax import lax
from jax.experimental import pallas as pl
from jax.experimental.pallas import tpu as pltpu
from jax.sharding import PartitionSpec as P

QH = 32
HD = 64
WINDOW = 128
LOOKUP_FEATURES = 128
DV = 256
SPAN = 64
KVH = 8
GATED_MIXERS = 8


EPS = 1e-05
FADING_SOFTNESS = 16.0
HIGH_PRECISION = lax.Precision.HIGHEST


def passed_along(value, axis, steps):
    count = lax.axis_size(axis)
    leading, last = (max(0, -steps), min(count, count - steps))
    return lax.ppermute(value, axis, [(source, source + steps) for source in range(leading, last)])


def prefix(x, axis, combine, identity):
    peers, place = (lax.axis_size(axis), lax.axis_index(axis))
    everything = jax.tree.map(
        lambda part, kind: lax.all_gather(part.astype(kind), axis), x, (jnp.bfloat16, jnp.bfloat16)
    )
    start = jax.tree.map(
        lambda part, zero: jnp.broadcast_to(jnp.asarray(zero, part.dtype), part.shape), x, identity
    )

    def hop(k, before):
        reached = k < place
        new = combine(
            before, jax.tree.map(lambda part, own: part[k].astype(own.dtype), everything, x)
        )
        return jax.tree.map(lambda a, b: jnp.where(reached, a, b), new, before)

    return lax.fori_loop(0, peers, hop, start)


def window_attention(near_query, near_keys, near_values, head_sink_logit):
    stream_extent = near_query.shape[0]
    key_heads = near_keys.shape[1] // HD
    heads_here = near_query.shape[1] // HD
    groups = heads_here // key_heads
    blocks = stream_extent // WINDOW
    tail_rows = jnp.stack([near_keys, near_values])
    before = passed_along(tail_rows, "sp", 1)

    def banded(previous, current):
        extended = jnp.concatenate([previous, current], axis=0)
        earlier = extended[:stream_extent].reshape(blocks, WINDOW, key_heads, HD)
        present = extended[WINDOW:].reshape(blocks, WINDOW, key_heads, HD)
        return jnp.concatenate([earlier, present], axis=1)

    key_band = banded(before[0], near_keys)
    value_band = banded(before[1], near_values)
    queries = near_query.reshape(blocks, WINDOW, key_heads, groups, HD)
    scores = jnp.einsum(
        "nqhgd,nkhd->hgnqk", queries, key_band, preferred_element_type=jnp.float32
    ) * HD ** (-0.5)
    head_ids = lax.axis_index("tp") * heads_here + jnp.arange(heads_here, dtype=jnp.int32)
    slopes = jnp.exp2(-8.0 * (head_ids + 1).astype(jnp.float32) / QH).reshape(key_heads, groups)
    query_pos = jnp.arange(WINDOW, dtype=jnp.int32)
    key_pos = jnp.arange(2 * WINDOW, dtype=jnp.int32)
    distance = query_pos[:, None] - key_pos[None, :] + WINDOW
    start_pos = (
        lax.axis_index("sp") * stream_extent + (jnp.arange(blocks, dtype=jnp.int32) - 1) * WINDOW
    )
    absolute = start_pos[:, None] + key_pos[None, :]
    allowed = ((distance >= 0) & (distance < WINDOW))[None] & (absolute >= 0)[:, None, :]
    biased = scores - slopes[:, :, None, None, None] * distance.astype(jnp.float32)
    weights = jnp.where(allowed, jnp.exp(biased), 0.0)
    denominator = (
        jnp.sum(weights, axis=-1, keepdims=True)
        + jnp.exp(head_sink_logit.reshape(key_heads, groups))[:, :, None, None, None]
    )
    attention = (weights / denominator).astype(jnp.bfloat16)
    attended = jnp.einsum(
        "hgnqk,nkhd->nqhgd", attention, value_band, preferred_element_type=jnp.float32
    )
    return attended.reshape(stream_extent, heads_here * HD).astype(jnp.bfloat16)


def linear_attention(
    gated_query, gated_keys, gated_values, fading_exponent, linear_head_gain, starting_state
):
    stream_extent = gated_query.shape[0]
    head_total = gated_query.shape[1] // LOOKUP_FEATURES
    span_count = stream_extent // SPAN
    scaled_query = gated_query.astype(jnp.float32).reshape(
        span_count, SPAN, head_total, LOOKUP_FEATURES
    ) * LOOKUP_FEATURES ** (-0.5)
    keys_wide = gated_keys.astype(jnp.float32).reshape(
        span_count, SPAN, head_total, LOOKUP_FEATURES
    )
    values_wide = gated_values.astype(jnp.float32).reshape(span_count, SPAN, head_total, DV)
    running = jnp.cumsum(
        fading_exponent.reshape(span_count, SPAN, head_total, LOOKUP_FEATURES), axis=1
    )
    span_end = running[:, -1]
    query_with_decay = scaled_query * jnp.exp(running)
    inverse_keys = keys_wide * jnp.exp(-running)
    ending_keys = keys_wide * jnp.exp(span_end[:, None] - running)
    inner = jnp.einsum("nchk,nshk->nhcs", query_with_decay, inverse_keys, precision=HIGH_PRECISION)
    lower = jnp.tril(jnp.ones((SPAN, SPAN), dtype=bool))
    inner = jnp.where(lower, inner, 0.0)
    within = jnp.einsum("nhcs,nshv->nchv", inner, values_wide, precision=HIGH_PRECISION)

    def advance(running_state, inputs):
        query_portion, key_portion, value_portion, scale_factor = inputs
        layer_output = jnp.einsum(
            "fmy,mys->fms", query_portion, running_state, precision=HIGH_PRECISION
        )
        running_state = running_state * scale_factor[..., None] + jnp.einsum(
            "gxp,gxz->xpz", key_portion, value_portion, precision=HIGH_PRECISION
        )
        return (running_state, layer_output)

    start_state = jnp.zeros((head_total, LOOKUP_FEATURES, DV), jnp.float32)
    state_end, carried = lax.scan(
        advance, start_state, (query_with_decay, ending_keys, values_wide, jnp.exp(span_end))
    )
    device_decay = jnp.exp(jnp.sum(span_end, axis=0))
    prefix_sums = jnp.cumsum(span_end, axis=0) - span_end

    def combine(earlier, later):
        return (earlier[0] * later[0], later[0][..., None] * earlier[1] + later[1])

    decay_before, state_before = prefix(
        (device_decay, state_end),
        "sp",
        combine,
        (jnp.ones_like(device_decay), jnp.zeros_like(state_end)),
    )
    incoming_rows = state_before + decay_before[..., None] * starting_state
    crossing = jnp.einsum(
        "qwso,soz->qwsz",
        query_with_decay * jnp.exp(prefix_sums)[:, None],
        incoming_rows,
        precision=HIGH_PRECISION,
    )
    flat = (within + carried + crossing).reshape(stream_extent, head_total, DV)
    normal = (
        flat * lax.rsqrt(jnp.mean(flat * flat, axis=-1, keepdims=True) + EPS) * linear_head_gain
    )
    return normal.reshape(stream_extent, head_total * DV).astype(jnp.bfloat16)


def local(
    activations,
    input_norm_gain,
    window_query_weight,
    window_key_weight,
    window_value_weight,
    linear_query_weight,
    linear_key_weight,
    linear_value_weight,
    decay_down_factor,
    decay_up_factor,
    decay_offset_bias,
    extra_fading_exponent,
    starting_state,
    head_sink_logit,
    linear_head_gain,
    window_output_weight,
    linear_output_weight,
):
    gathered = lax.all_gather(activations, "tp", axis=1, tiled=True)
    widened = gathered.astype(jnp.float32)
    normed = (
        widened
        * lax.rsqrt(jnp.mean(widened * widened, axis=1, keepdims=True) + EPS)
        * input_norm_gain
    ).astype(jnp.bfloat16)
    row_total = normed.shape[0]
    matrices = (
        window_query_weight,
        window_key_weight,
        window_value_weight,
        linear_query_weight,
        linear_key_weight,
        linear_value_weight,
    )
    segments = (
        lax.all_gather(matrices[0], "sp", axis=0, tiled=True),
        lax.all_gather(matrices[1], "sp", axis=0, tiled=True),
        lax.all_gather(matrices[2], "sp", axis=0, tiled=True),
        lax.all_gather(matrices[3], "sp", axis=0, tiled=True),
        lax.all_gather(matrices[4], "sp", axis=0, tiled=True),
        lax.all_gather(matrices[5], "sp", axis=0, tiled=True),
    )
    projected = tuple(
        (jnp.dot(normed, segment, preferred_element_type=jnp.float32) for segment in segments)
    )
    near_query, near_keys, near_values, gated_query, gated_keys, gated_values = [
        product.astype(jnp.bfloat16) for product in projected
    ]
    low_rank = jnp.dot(normed, decay_down_factor, preferred_element_type=jnp.float32).astype(
        jnp.bfloat16
    )
    attention_energies = (
        jnp.dot(low_rank, decay_up_factor, preferred_element_type=jnp.float32) + decay_offset_bias
    )
    head_total = extra_fading_exponent.shape[1]
    fading_exponent = (jax.nn.log_sigmoid(attention_energies) / FADING_SOFTNESS).reshape(
        row_total, head_total, LOOKUP_FEATURES
    ) + extra_fading_exponent[:, :, None]
    near_out = window_attention(near_query, near_keys, near_values, head_sink_logit)
    gated_out = linear_attention(
        gated_query, gated_keys, gated_values, fading_exponent, linear_head_gain, starting_state
    )
    window_full, linear_full = (
        lax.all_gather(window_output_weight, "sp", axis=1, tiled=True),
        lax.all_gather(linear_output_weight, "sp", axis=1, tiled=True),
    )
    return lax.psum_scatter(
        (
            jnp.dot(near_out, window_full, preferred_element_type=jnp.float32)
            + jnp.dot(gated_out, linear_full, preferred_element_type=jnp.float32)
        ).astype(jnp.bfloat16),
        "tp",
        scatter_dimension=0,
        tiled=True,
    )


MESH = pl.DeviceIdType.MESH
BF = jnp.bfloat16
F32 = jnp.float32
LAG = 2
CUTS = 2
EARLY = 3


def dot(a, b):
    return jnp.dot(a, b, preferred_element_type=F32)


def remote(src, dst, send_sem, recv_sem, **where):
    return pltpu.make_async_remote_copy(
        src_ref=src,
        dst_ref=dst,
        send_sem=send_sem,
        recv_sem=recv_sem,
        device_id=where,
        device_id_type=MESH,
    )


def greet(sp, tp):
    s, t = lax.axis_index("sp"), lax.axis_index("tp")
    barrier = pltpu.get_barrier_semaphore()
    for ds in range(sp):
        for dt in range(tp):
            if ds or dt:
                where = {"sp": lax.rem(s + ds, sp), "tp": lax.rem(t + dt, tp)}
                pl.semaphore_signal(barrier, inc=1, device_id=where, device_id_type=MESH)


def greeted(sp, tp):
    pl.semaphore_wait(pltpu.get_barrier_semaphore(), sp * tp - 1)


def columns_dot(a, b):
    return lax.dot_general(a, b, (((1,), (1,)), ((), ())), preferred_element_type=F32)


def mixer_kernel(sp, tp, *refs):
    small_in, sources, state_in, down_in, x_in = refs[:6], refs[6:14], refs[14], refs[15], refs[16]
    out = refs[17]
    weights, start, down, x = refs[18:26], refs[26], refs[27], refs[28]
    gain, bias, sink, head_gain, up, fade = refs[58:64]
    squares, blocks, note, term, away = refs[29:34]
    lin_own, win_own, lin_in, win_in, held_g, held_n = refs[34:40]
    w_sem, sq_send, sq_recv, a_send, a_recv, f_send, l_sem, n_send, n_recv = refs[40:49]
    r_send, r_recv, g_send, g_recv, t_send, t_recv, o_send, o_recv, s_sem = refs[49:58]
    s, t = lax.axis_index("sp"), lax.axis_index("tp")
    other = 1 - t
    last = sp - 1
    e = jnp.where(s >= sp // 2, 1, 0)
    at_end = jnp.logical_or(s == 0, s == last)
    inside = jnp.logical_not(at_end)
    per_half = sp // tp
    rows, half = x.shape
    width = half // per_half
    rank = down.shape[0]
    lk = LOOKUP_FEATURES
    mine = lin_own.shape[2]
    lane_of = {i: weights[i].shape[1] // 2 for i in range(6)}
    greet(sp, tp)
    loads = [
        pltpu.make_async_copy(a, b, w_sem.at[i]) for i, (a, b) in enumerate(zip(sources, weights))
    ]
    loads.append(pltpu.make_async_copy(state_in.at[pl.ds(e * mine, mine)], start, w_sem.at[8]))
    loads.append(
        pltpu.make_async_copy(
            down_in.at[:, pl.ds(pl.multiple_of(t * half, half), half)], down, w_sem.at[9]
        )
    )
    loads.append(pltpu.make_async_copy(x_in, x, w_sem.at[10]))
    small = [
        pltpu.make_async_copy(a, b, s_sem.at[i]) for i, (a, b) in enumerate(zip(small_in, refs[58:64]))
    ]
    loads[10].start()
    for copy in small:
        copy.start()
    for i in (9, 3, 4, 5, 0, 1, 2, 8, 6, 7):
        loads[i].start()
    home = lax.div(s, per_half) == t

    def slice_send(i):
        src = x.at[:, i * width : (i + 1) * width]
        return remote(src, blocks.at[s], a_send.at[i], a_recv.at[s], sp=t * per_half + i)

    def forward(b):
        return remote(blocks.at[b], blocks.at[b], f_send, a_recv.at[b], tp=other)

    me = s * tp + t

    def squares_send(n):
        where = {"sp": lax.rem(s + n // tp, sp), "tp": lax.rem(t + n % tp, tp)}
        ref = squares.at[me]
        return remote(ref, ref, sq_send, sq_recv.at[0 if n // tp == 0 else 1], **where)

    def keep(i):
        return pltpu.make_async_copy(x.at[:, i * width : (i + 1) * width], blocks.at[s], l_sem)

    def share(i):
        src = x.at[:, i * width : (i + 1) * width]
        return remote(src, blocks.at[s], f_send, a_recv.at[s], tp=other)

    loads[10].wait()
    wide = x[...].astype(F32)
    own = jnp.sum(wide * wide, axis=1, keepdims=True)
    squares[me] = jnp.broadcast_to(own, (rows, rows)).T[:8]
    greeted(sp, tp)
    for n in range(1, sp * tp):
        squares_send(n).start()
    for i in reversed(range(per_half)):
        j = t * per_half + i

        @pl.when(((j < s) & ((s < last) | (t == 0))) | ((j > s) & (s == 0) & (t > 0)))
        def _():
            slice_send(i).start()

        @pl.when(j == s)
        def _():
            share(i).start()
            keep(i).start()

    def squares_wait(n, k):
        ref = squares.at[pl.ds(0, n)]
        remote(ref, ref, sq_send, sq_recv.at[k], tp=other).wait_recv()

    def scale_of(b):
        total = (squares[b * tp] + squares[b * tp + 1]) / (half * tp)
        tall = jnp.concatenate([lax.rsqrt(total + EPS), jnp.zeros((rows - 8, rows), F32)], axis=0)
        return tall.T[:, :1]

    for copy in small:
        copy.wait()
    squares_wait(tp - 1, 0)
    scale = scale_of(s)
    loads[9].wait()
    low = jnp.zeros((rank, rows), F32)
    for i in range(per_half):
        cols = slice(i * width, (i + 1) * width)
        shaped = (x[:, cols].astype(F32) * scale * gain[t, :, cols]).astype(BF)
        low += columns_dot(down[:, cols], shaped)
    fades = fade.shape[0]
    noted = note.shape[1]
    note[me] = jnp.concatenate(
        [low, fade[...], jnp.zeros((noted - rank - fades, rows), F32)], axis=0
    )

    def note_send(n):
        place, core = (0 if n < tp else last), lax.rem(t + n % tp, tp)
        ref = note.at[me]
        return remote(ref, ref, n_send, n_recv, sp=place, tp=core), (s != place) | (core != t)

    cut_rows = rows // CUTS
    pieces = [(i, slice(r * cut_rows, (r + 1) * cut_rows)) for i in range(mine + 1) for r in range(CUTS)]

    def step(way, b, n):
        i, cut = pieces[n]
        src = lin_own.at[b, 1 - way, i, cut] if i < mine else win_own.at[b, 1 - way, cut]
        dst = lin_in.at[way, b, i, cut] if i < mine else win_in.at[way, b, cut]
        return remote(
            src, dst, r_send.at[0 if i < mine else 1], r_recv.at[way, b, n], sp=jnp.clip(s + 1 - 2 * way, 0, last)
        )

    def relay(way, b, n):
        i, cut = pieces[n]
        step(way, b, n).wait_recv()
        if i < mine:
            lin_own[b, 1 - way, i, cut] = (
                lin_own[b, 1 - way, i, cut].astype(F32) + lin_in[way, b, i, cut].astype(F32)
            ).astype(BF)
        else:
            win_own[b, 1 - way, cut] = (
                win_own[b, 1 - way, cut].astype(F32) + win_in[way, b, cut].astype(F32)
            ).astype(BF)
        step(way, b, n).start()

    for i in range(6):
        loads[i].wait()
    qw, kw = lane_of[0], lane_of[1]
    gain_here = gain[lax.div(s, per_half), :, pl.ds(pl.multiple_of(lax.rem(s, per_half) * width, width), width)]

    def send_sums(b):
        for n in range(len(pieces)):
            step(e, b, n).start()

    def project(k, carry):
        turned = lax.rem(s + k, sp)
        b = jnp.where(inside & (k > 1), jnp.where(k == 2, 0, sp + 1 - 2 * s), turned)

        @pl.when(inside & (k == last))
        def _():
            for n in range(1, EARLY):
                relay(e, 0, n)

        @pl.when(jnp.logical_or(jnp.logical_not(home), b != s))
        def _():
            forward(b).wait_recv()

        @pl.when(jnp.logical_and(home, b != s))
        def _():
            forward(b).start()

        @pl.when(jnp.logical_and(home, b == s))
        def _():
            keep(0).wait()

        @pl.when(k == 1)
        def _():
            squares_wait((sp - 1) * tp, 1)

        for i in reversed(range(per_half)):

            @pl.when((b == 0) & (s > 1) & (t * per_half + i > s))
            def _():
                slice_send(i).start()

        block = (blocks[b].astype(F32) * scale_of(b) * gain_here).astype(BF)

        def part(i, h):
            w = lane_of[i]
            return dot(block, weights[i][:, pl.ds(pl.multiple_of(h * w, w), w)]).astype(BF)

        for n in range(2):
            h = e if n else 1 - e
            query, key, value = part(3, h), part(4, h), part(5, h)
            for i in range(mine):
                lin_own[b, h, i, :, :lk] = query[:, i * lk : (i + 1) * lk]
                lin_own[b, h, i, :, lk : 2 * lk] = key[:, i * lk : (i + 1) * lk]
                lin_own[b, h, i, :, 2 * lk :] = value[:, i * DV : (i + 1) * DV]
            if n == 0:

                @pl.when((s == last) & (t > 0) & (k == 0))
                def _():
                    for i in range(per_half - 1):
                        slice_send(i).start()

                @pl.when((s == 0) & (t == 0) & (k == 0))
                def _():
                    for i in range(1, per_half):
                        slice_send(i).start()

                for i in reversed(range(per_half)):

                    @pl.when((k == 0) & (s == 1) & (t * per_half + i > s))
                    def _():
                        slice_send(i).start()

                @pl.when(at_end & (k >= e))
                def _():
                    for m in range(mine * CUTS):
                        step(e, b, m).start()

            if n == 0:

                @pl.when(k == 0)
                def _():
                    for m in range(2 * tp):
                        send, away_from_here = note_send(m)

                        @pl.when(away_from_here)
                        def _():
                            send.start()

            win_own[b, h, :, :qw] = part(0, h)
            win_own[b, h, :, qw : qw + kw] = part(1, h)
            win_own[b, h, :, qw + kw :] = part(2, h)
            if n == 0:

                @pl.when(inside & (k == 2))
                def _():
                    relay(e, 0, 0)

                @pl.when(at_end & (k >= e))
                def _():
                    for m in range(mine * CUTS, len(pieces)):
                        step(e, b, m).start()

        return carry

    lax.fori_loop(0, sp, project, 0)

    @pl.when(s == last)
    def _():
        send_sums(last)

    def gather(way, b, n):
        i, r = divmod(n, CUTS)
        ref = (held_n if i else held_g).at[b, way, slice(r * cut_rows, (r + 1) * cut_rows)]
        return remote(
            ref, ref, g_send.at[i], g_recv.at[way, b, n], sp=jnp.clip(s + 1 - 2 * way, 0, last)
        )

    part_rows = rows // tp
    cols_g, cols_n = held_g.shape[3], held_n.shape[3]

    def swap(b):
        return remote(term.at[b, other], away.at[b], t_send.at[b], t_recv.at[b], tp=other)

    columns = term.shape[3]

    def place_of(src):
        return pl.ds(pl.multiple_of(src * columns, columns), columns)

    def deliver(b):
        return remote(term.at[b, t], out.at[:, place_of(s)], o_send, o_recv, sp=b)

    def close(b):
        swap(b).wait()
        term[b, t] = (term[b, t].astype(F32) + away[b].astype(F32)).astype(BF)

        @pl.when(s != b)
        def _():
            deliver(b).start()

        @pl.when(s == b)
        def _():
            out[:, b * columns : (b + 1) * columns] = term[b, t]

    def multiply(b):
        total = None
        for src in range(2):
            piece = dot(held_g[b, src], weights[7][src * cols_g : (src + 1) * cols_g]) + dot(
                held_n[b, src], weights[6][src * cols_n : (src + 1) * cols_n]
            )
            total = piece if total is None else total + piece
        for h in range(tp):
            term[b, h] = total[h * part_rows : (h + 1) * part_rows].astype(BF)
        swap(b).start()

    def pass_on(way, b, i):
        gather(way, b, i).wait_recv()
        gather(way, b, i).start()

    @pl.when(inside)
    def _():
        loads[8].wait()
        items = [(relay, b, i) for b in range(sp) for i in range(len(pieces))]
        items += [(pass_on, b, i) for b in range(sp) for i in range(2 * CUTS)]
        for n in range(len(items) + LAG):
            if EARLY <= n < len(items):
                what, b, i = items[n]
                what(e, b, i)
            if n >= LAG:
                what, b, i = items[n - LAG]
                what(1 - e, b, i)
                if what is pass_on and i == 2 * CUTS - 1:
                    if b == 0:
                        loads[6].wait()
                        loads[7].wait()
                    if b == last:
                        for c in range(1, last):
                            close(c)

                        @pl.when(s == 1)
                        def _():
                            close(0)

                    multiply(b)
        close(last)

        @pl.when(s > 1)
        def _():
            close(0)


    @pl.when(at_end)
    def _():
        loads[8].wait()
        others = note.at[pl.ds(0, sp * tp - 1)]
        remote(others, others, n_send, n_recv, tp=other).wait_recv()
        span = mine * lk
        lane = pl.ds(pl.multiple_of(e * span, span), span)
        up_own = jnp.concatenate([up[:, lane], jnp.zeros((rows - rank, span), BF)], axis=0)
        bias_own = bias[:, lane]
        row_at = lax.broadcasted_iota(jnp.int32, (rows, rows), 0)
        col_at = lax.broadcasted_iota(jnp.int32, (rows, rows), 1)
        span_low = jnp.logical_and(row_at >= col_at, row_at // SPAN == col_at // SPAN)
        ones_low = jnp.where(span_low, 1.0, 0.0).astype(BF)
        query_at = lax.broadcasted_iota(jnp.int32, (rows, 2 * rows), 0)
        key_at = lax.broadcasted_iota(jnp.int32, (rows, 2 * rows), 1)
        distance = query_at - key_at + rows
        near_by = jnp.logical_and(distance >= 0, distance < WINDOW)
        far = distance.astype(F32)
        heads = qw // HD // mine

        def linear(b, states):
            rank_rows = note[b * tp, :rank] + note[b * tp + 1, :rank]
            tall = jnp.concatenate(
                [rank_rows, note[b * tp + t, rank:], jnp.zeros((rows - noted, rows), F32)], axis=0
            ).T
            energies = dot(tall.astype(BF), up_own) + bias_own
            soft = jnp.minimum(energies, 0.0) - jnp.log1p(jnp.exp(-jnp.abs(energies)))
            soft = soft / FADING_SOFTNESS
            fading = []
            for i in range(mine):
                extra = jnp.sum(
                    jnp.where(col_at == rank + e * mine + i, tall, 0.0), axis=1, keepdims=True
                )
                fading.append(soft[:, i * lk : (i + 1) * lk] + extra)
            fading = jnp.concatenate(fading, axis=1)
            top = fading.astype(BF)
            rest = fading - top.astype(F32)
            middle = rest.astype(BF)
            bottom = (rest - middle.astype(F32)).astype(BF)
            summed = dot(ones_low, jnp.concatenate([top, middle, bottom], axis=1))
            running_all = summed[:, :span] + (summed[:, span : 2 * span] + summed[:, 2 * span :])
            new_states = []
            for i in range(mine):
                for r in range(CUTS):
                    step(1 - e, b, i * CUTS + r).wait_recv()
                here = (lin_own[b, e, i].astype(F32) + lin_in[1 - e, b, i].astype(F32)).astype(BF)
                running = running_all[:, i * lk : (i + 1) * lk]
                state = states[i]
                query = here[:, :lk].astype(F32) * lk ** (-0.5)
                key = here[:, lk : 2 * lk].astype(F32)
                value = here[:, 2 * lk :]
                decayed = (query * jnp.exp(running)).astype(BF)
                inner = columns_dot(decayed, (key * jnp.exp(-running)).astype(BF))
                inner = jnp.where(span_low, inner, 0.0).astype(BF)
                within = dot(inner, value)
                carried = []
                for j in range(rows // SPAN):
                    cut = slice(j * SPAN, (j + 1) * SPAN)
                    end = running[(j + 1) * SPAN - 1 : (j + 1) * SPAN]
                    ending = (key[cut] * jnp.exp(end - running[cut])).astype(BF)
                    carried.append(columns_dot(decayed[cut], state.astype(BF)))
                    state = state * jnp.exp(end) + lax.dot_general(
                        value[cut], ending, (((0,), (0,)), ((), ())), preferred_element_type=F32
                    )
                flat = within + jnp.concatenate(carried, axis=0)
                normal = (
                    flat
                    * lax.rsqrt(jnp.mean(flat * flat, axis=-1, keepdims=True) + EPS)
                    * head_gain[...]
                )
                held_g[b, e, :, i * DV : (i + 1) * DV] = normal.astype(BF)
                new_states.append(state)
            for r in range(CUTS):
                gather(e, b, r).start()
            return new_states

        def window(b):
            for r in range(CUTS):
                step(1 - e, b, mine * CUTS + r).wait_recv()
            win_own[b, e] = (win_own[b, e].astype(F32) + win_in[1 - e, b].astype(F32)).astype(BF)
            present = win_own[b, e]
            earlier = win_own[max(b - 1, 0), e]
            allowed = near_by if b else jnp.logical_and(near_by, key_at >= rows)
            for g in range(mine):
                ka, va = qw + g * HD, qw + kw + g * HD
                keys = jnp.concatenate([earlier[:, ka : ka + HD], present[:, ka : ka + HD]], axis=0)
                vals = jnp.concatenate([earlier[:, va : va + HD], present[:, va : va + HD]], axis=0)
                results = []
                for h in range(heads):
                    local = (e * mine + g) * heads + h
                    number = (t * (2 * mine * heads) + local + 1).astype(F32)
                    slope = jnp.exp2(jnp.full((rows, 1), -8.0 / QH, F32) * number)
                    at = (g * heads + h) * HD
                    score = (
                        columns_dot(present[:, at : at + HD], keys) * HD ** (-0.5) - slope * far
                    )
                    weight = jnp.where(allowed, jnp.exp(score), 0.0)
                    floor = jnp.exp(jnp.full((rows, 1), sink[local], F32))
                    probs = (weight / (jnp.sum(weight, axis=1, keepdims=True) + floor)).astype(BF)
                    results.append(dot(probs, vals))
                wide_to = heads * HD
                held_n[b, e, :, g * wide_to : (g + 1) * wide_to] = jnp.concatenate(
                    results, axis=1
                ).astype(BF)
            for r in range(CUTS):
                gather(e, b, CUTS + r).start()

        def collect(b):
            for i in range(2 * CUTS):
                gather(1 - e, b, i).wait_recv()

        states = [start[i].T for i in range(mine)]
        for b in range(sp):
            states = linear(b, states)
            window(b)
        loads[6].wait()
        loads[7].wait()
        for b in range(sp):
            collect(b)
            multiply(b)
            if b == last - 1:
                for c in (*range(1, last), 0):
                    close(c)
        close(last)

    def drain(ref, sem):
        remote(ref, ref, sem, l_sem, tp=other).wait_send()

    sent = ((lin_own, r_send.at[0]), (win_own, r_send.at[1]), (held_g, g_send.at[0]), (held_n, g_send.at[1]))

    @pl.when(inside)
    def _():
        for ref, sem in sent:
            drain(ref, sem)
        drain(note.at[pl.ds(0, 2 * tp)], n_send)

    @pl.when(at_end)
    def _():
        for ref, sem in sent:
            drain(ref.at[:, 0], sem)
        drain(note.at[pl.ds(0, 2 * tp - 1)], n_send)

    @pl.when(home)
    def _():
        drain(blocks, f_send)

    for i in range(per_half):

        @pl.when(t * per_half + i != s)
        def _():
            slice_send(i).wait_send()

    drain(squares.at[pl.ds(0, sp * tp - 1)], sq_send)
    drain(term.at[pl.ds(0, last), 0], o_send)
    others = out.at[:, pl.ds(0, last * columns)]
    remote(others, others, o_send, o_recv, tp=other).wait_recv()


def stationary(
    activations,
    input_norm_gain,
    window_query_weight,
    window_key_weight,
    window_value_weight,
    linear_query_weight,
    linear_key_weight,
    linear_value_weight,
    decay_down_factor,
    decay_up_factor,
    decay_offset_bias,
    extra_fading_exponent,
    starting_state,
    head_sink_logit,
    linear_head_gain,
    window_output_weight,
    linear_output_weight,
):
    sp, tp = lax.axis_size("sp"), lax.axis_size("tp")
    rows, half = activations.shape
    matrices = (
        window_query_weight,
        window_key_weight,
        window_value_weight,
        linear_query_weight,
        linear_key_weight,
        linear_value_weight,
        window_output_weight,
        linear_output_weight,
    )
    rank = decay_down_factor.shape[1]
    heads_tp = extra_fading_exponent.shape[1]
    mine = heads_tp // 2
    noted = rank + heads_tp + -(rank + heads_tp) % 8
    columns = window_output_weight.shape[1]
    small = (
        input_norm_gain.reshape(tp, 1, half),
        decay_offset_bias.reshape(1, -1),
        head_sink_logit,
        linear_head_gain.reshape(1, -1),
        decay_up_factor,
        extra_fading_exponent.T,
    )
    vmem = pl.BlockSpec(memory_space=pltpu.VMEM)
    hbm = pl.BlockSpec(memory_space=pltpu.HBM)
    dma = pltpu.SemaphoreType.DMA
    slice_width = half * tp // sp
    lin_cols = sum(m.shape[1] for m in matrices[3:6]) // heads_tp
    win_cols = sum(m.shape[1] for m in matrices[:3]) // 2
    return pl.pallas_call(
        functools.partial(mixer_kernel, sp, tp),
        out_shape=pltpu.VMEM((rows // tp, columns * sp), BF),
        in_specs=[hbm] * 17,
        out_specs=vmem,
        scratch_shapes=[pltpu.VMEM(m.shape, BF) for m in matrices]
        + [
            pltpu.VMEM((mine,) + starting_state.shape[1:], F32),
            pltpu.VMEM((rank, half), BF),
            pltpu.VMEM((rows, half), BF),
            pltpu.VMEM((sp * tp, 8, rows), F32),
            pltpu.VMEM((sp, rows, slice_width), BF),
            pltpu.VMEM((sp * tp, noted, rows), F32),
            pltpu.VMEM((sp, tp, rows // tp, columns), BF),
            pltpu.VMEM((sp, rows // tp, columns), BF),
            pltpu.VMEM((sp, 2, mine, rows, lin_cols), BF),
            pltpu.VMEM((sp, 2, rows, win_cols), BF),
            pltpu.VMEM((2, sp, mine, rows, lin_cols), BF),
            pltpu.VMEM((2, sp, rows, win_cols), BF),
            pltpu.VMEM((sp, 2, rows, linear_output_weight.shape[0] // 2), BF),
            pltpu.VMEM((sp, 2, rows, window_output_weight.shape[0] // 2), BF),
            dma((11,)),
            dma,
            dma((2,)),
            dma((sp // tp,)),
            dma((sp,)),
            dma,
            dma,
            dma,
            dma,
            dma((2,)),
            dma((2, sp, (mine + 1) * CUTS)),
            dma((2,)),
            dma((2, sp, 2 * CUTS)),
            dma((sp,)),
            dma((sp,)),
            dma,
            dma,
            dma((len(small),)),
        ]
        + [
            (pltpu.SMEM if a.ndim == 1 else pltpu.VMEM)(a.shape, a.dtype) for a in small
        ],
        compiler_params=pltpu.CompilerParams(
            collective_id=0, has_side_effects=True, vmem_limit_bytes=56 * 2**20
        ),
    )(
        *small,
        *matrices,
        starting_state,
        decay_down_factor.T,
        activations,
    )


def mixer(*arrays):
    sp, tp = lax.axis_size("sp"), lax.axis_size("tp")
    rows = arrays[0].shape[0]
    one_each = KVH == GATED_MIXERS == sp * tp and QH % KVH == 0
    if tp == 2 and sp == 2 * tp and one_each and rows == WINDOW and rows % SPAN == 0:
        return stationary(*arrays)
    return local(*arrays)


def solution(mesh):
    placed = (
        P(("fs", "sp"), "tp"),
        P(),
        P("sp", "tp"),
        P("sp", "tp"),
        P("sp", "tp"),
        P("sp", "tp"),
        P("sp", "tp"),
        P("sp", "tp"),
        P(),
        P(None, "tp"),
        P("tp"),
        P(("fs", "sp"), "tp"),
        P("tp", None, None),
        P("tp"),
        P(),
        P("tp", "sp"),
        P("tp", "sp"),
    )
    return jax.shard_map(
        mixer, mesh=mesh, in_specs=placed, out_specs=P(("fs", "sp", "tp"), None), check_vma=False
    )
```
